32 devices in a mesh: grp: 2 (over y), ep: 4 (over z), tp: 4 (over x, core).
Axes of the slice: x: 2, y: 2, z: 4, core: 2. Of those that a mesh axis runs over, the one named last changes fastest.
Arguments:
- queries: bfloat16 [1024, 2048], P(('grp', 'ep'), 'tp'), parts along dimension 0, may hold values from -6 to 6
- keys: bfloat16 [1024, 2048], P(('grp', 'ep'), 'tp'), parts along dimension 0, may hold values from -6 to 6
- values: bfloat16 [1024, 2048], P(('grp', 'ep'), 'tp'), parts along dimension 0, may hold values from -6 to 6
- stop_bias: bfloat16 [1024, 32], P(('grp', 'ep'), 'tp'), parts along dimension 0, may hold values from -20 to 0
- out_weight: bfloat16 [2048, 2048], P('tp'), may hold values from -0.125 to 0.125
- mix_gain: float32 [2048], replicated, may hold values from 0.1 to 1.9
- moe_input: bfloat16 [4096, 2048], P(('grp', 'ep', 'tp')), parts along dimension 0, may hold values from -6 to 6
- ffn_gain: float32 [2048], replicated, may hold values from 0.1 to 1.9
- expert_ids: int32 [4096, 2], P(('grp', 'ep', 'tp')), parts along dimension 0, may hold values from 0 to 3, all different within a row; in each aligned block of 128 rows (0 to 127, 128 to 255, ...) at most 96 rows name the same one
- expert_scores: float32 [4096, 2], P(('grp', 'ep', 'tp')), parts along dimension 0, may hold values from 0.05 to 1
- gate_weight: bfloat16 [4, 2048, 1024], P('ep', None, 'tp'), may hold values from -0.125 to 0.125
- up_weight: bfloat16 [4, 2048, 1024], P('ep', None, 'tp'), may hold values from -0.125 to 0.125
- down_weight: bfloat16 [4, 1024, 2048], P('ep', 'tp'), may hold values from -0.1875 to 0.1875
Outputs:
- mixed: bfloat16 [1024, 2048], P(('grp', 'ep', 'tp')), parts along dimension 0
- experts_mixed: bfloat16 [4096, 2048], P(('grp', 'ep', 'tp')), parts along dimension 0
The draws below stay inside these ranges and needn't reach their ends.
There are 2 independent parts, one for each index of `grp`. The reference program is written for one: setup_inputs(seed, part) draws one part's arguments, and reference() takes and returns one part's arrays. A program takes and returns all parts, laid end to end along the dimension named above; an argument that names none is the same for every part. Nothing has to cross between parts.
Inputs may be any that keep to these rules, and one draw needn't show every extreme that they name: `expert_ids`: each token names 2 different experts. Among the 128 tokens of one device, no expert is named by more than 96 tokens, and in some device's tokens some expert is named by exactly 96.
All inputs are finite; a program needn't handle non-finite values.
Results may differ from the reference program's by a relative error of at most 0.012.
Values may be sent and summed in bfloat16 or wider, within the bound.
No kernel may reach another device: no remote copies, remote signals or barrier semaphores. Data moves between devices by JAX's collectives and lax.ppermute only.
A program may use at most 128 MiB of HBM per device.

```python
import math
import jax
import jax.numpy as jnp
import numpy as np
from jax import lax

D = 2048
HEADS = 32
HEAD = 64
FF = 1024
TOP_K = 2
SEQ_DEV = 128
TOK_DEV = 128
CONTEXT_LENGTH = 512
TOKENS = 2048
EXPERTS = 4
CAP = 96
N_EP = 4
N_TP = 4


def draw_stop_bias(key, part):
    streams = jax.random.split(key, 7)
    fast = jax.random.uniform(streams[0], (HEADS,)) < 0.5
    slow_rate = jax.random.uniform(streams[1], (HEADS,), minval=0.1, maxval=0.4) / CONTEXT_LENGTH
    fast_rate = jax.random.uniform(streams[2], (HEADS,), minval=1.0 / 150.0, maxval=1.0 / 60.0)
    starting_level = jnp.log(jnp.where(fast, fast_rate, slow_rate))
    displacement_delta = jax.random.uniform(streams[3], (CONTEXT_LENGTH // SEQ_DEV, 1), minval=-0.7, maxval=0.7)
    displacement_delta = jnp.repeat(displacement_delta, SEQ_DEV, axis=0)
    approximate_guess = jax.random.uniform(streams[4], (CONTEXT_LENGTH, HEADS), minval=-2.0, maxval=2.0)
    location_number = jax.random.randint(streams[5], (4,), 0, CONTEXT_LENGTH)
    spike_height = jnp.any(jnp.arange(CONTEXT_LENGTH)[:, None] == location_number[None, :], axis=1)
    intensity_multiplier = jax.random.uniform(streams[6], (CONTEXT_LENGTH, HEADS), minval=0.25, maxval=0.4)
    closing_answer = jnp.where(spike_height[:, None], jnp.log(intensity_multiplier / (1.0 - intensity_multiplier)), starting_level[None, :] + displacement_delta + approximate_guess)
    return closing_answer.astype(jnp.bfloat16)


def level_of(key, extent, cuts, low, largest):
    def one(position, blocks):
        heights = jax.random.uniform(jax.random.fold_in(jax.random.fold_in(key, 6), position), (blocks,), jnp.float32, low / len(cuts), largest / len(cuts))
        return jnp.repeat(jnp.exp(heights), extent[position] // blocks).reshape((-1,) + (1,) * (len(extent) - position - 1))

    loudness = one(*cuts[0])
    for cut in cuts[1:]:
        loudness = loudness * one(*cut)
    return loudness


def routed_block(stream_key, own, number, rows, amount, top, limit, slope):
    sequence = jax.random.permutation(stream_key, amount)
    heavy_load, usual = shares(amount, rows * top, limit, slope, True), shares(amount, rows * top, limit, slope, False)
    places = jnp.arange(amount)

    def named(tallies, turn):
        used = int((tallies > 0).sum())
        fixed = max(1, used // 4)
        shifted = fixed + (places - fixed + turn * (used - fixed)) % max(1, amount - fixed)
        return jnp.zeros((amount,), jnp.int32).at[sequence[jnp.where(places < fixed, places, shifted)]].set(jnp.asarray(tallies, jnp.int32))

    tallies = jnp.where(number % 4 == 0, named(heavy_load, number // 4), named(usual, number - number // 4 - 1))
    mixed = jax.random.permutation(jax.random.fold_in(own, 3), amount)
    giver, sink = mixed[0:amount // 2 * 2:2], mixed[1:amount // 2 * 2:2]
    margin = jnp.minimum(tallies[giver] - 1, limit - tallies[sink]) // 2
    margin = jnp.where((giver == sequence[0]) | (sink == sequence[0]) | (tallies[sink] == 0), 0, jnp.maximum(margin, 0))
    shifted = jax.random.randint(jax.random.fold_in(own, 4), (amount // 2,), 0, 1 << 20) % (margin + 1)
    tallies = tallies.at[giver].add(-shifted).at[sink].add(shifted)
    members = jnp.searchsorted(jnp.cumsum(tallies), jnp.arange(rows * top), side="right").astype(jnp.int32)
    table = members.reshape(top, rows).T
    table = table[jax.random.permutation(jax.random.fold_in(own, 1), rows)]
    turn = jax.random.randint(jax.random.fold_in(own, 2), (rows, 1), 0, top)
    return jnp.take_along_axis(table, (jnp.arange(top)[None, :] + turn) % top, axis=1)


def shares(number_of, total, bound, skew, full):
    loads = [(1 << 20) // math.isqrt(standing ** skew) + 1 for standing in range(1, number_of + 1)]
    largest = bound if full else min(bound, max(-(-total // number_of), total * loads[0] // sum(loads)))
    least = 1 if total - largest >= number_of - 1 else 0
    counts, spare = [largest] + [least] * (number_of - 1), total - largest - least * (number_of - 1)
    while spare > 0:
        candidates = [i for i in range(1, number_of) if counts[i] < largest] or [i for i in range(1, number_of) if counts[i] < bound]
        mass, remaining = sum([loads[i] for i in candidates]), spare
        for i in candidates:
            addition = min(bound - counts[i], max(1, remaining * loads[i] // mass), spare)
            counts[i] = counts[i] + addition
            spare = spare - addition
    return np.array(counts)


def scatter_about(own_key, shape, scale, bound, cuts=(), held_as=jnp.bfloat16):
    values = jax.random.normal(own_key, shape, jnp.float32) * scale
    if len(cuts) > 0:
        values = level_of(own_key, shape, cuts, -0.22, 0.18) * values
    return jnp.clip(values, min=-bound, max=bound).astype(held_as)


def setup_inputs(seed: int = 0, part: int = 0) -> dict:
    key_of = jax.random.split(jax.random.key(seed), 14)
    own_keys = jax.random.split(jax.random.fold_in(key_of[13], part), 14)
    queries = scatter_about(own_keys[0], (CONTEXT_LENGTH, HEADS * HEAD), 1.0, 6.0, ((0, 4), (1, 4)))
    keys = scatter_about(own_keys[1], (CONTEXT_LENGTH, HEADS * HEAD), 1.0, 6.0, ((0, 4), (1, 4)))
    values = scatter_about(own_keys[2], (CONTEXT_LENGTH, HEADS * HEAD), 1.0, 6.0, ((0, 4), (1, 4)))
    stop_bias = draw_stop_bias(jax.random.fold_in(jax.random.fold_in(key_of[13], part), 71), part)
    out_weight = scatter_about(key_of[4], (HEADS * HEAD, D), (HEADS * HEAD) ** -0.5, 0.125, ((0, 4),))
    mix_gain = jnp.clip(1.0 + 0.18 * jax.random.normal(key_of[5], (D,), jnp.float32), 0.1, 1.9)
    moe_input = scatter_about(own_keys[6], (TOKENS, D), 1.0, 6.0, ((0, 16),))
    ffn_gain = jnp.clip(1.0 + 0.18 * jax.random.normal(key_of[7], (D,), jnp.float32), 0.1, 1.9)
    expert_ids_keys = jax.random.split(jax.random.fold_in(own_keys[8], 1), TOKENS // TOK_DEV)
    expert_ids_turns = jax.random.permutation(jax.random.fold_in(own_keys[8], 3), TOKENS // TOK_DEV)
    expert_ids = jax.vmap(lambda own, number: routed_block(jax.random.fold_in(own_keys[8], 2), own, number, TOK_DEV, EXPERTS, TOP_K, CAP, 2))(expert_ids_keys, expert_ids_turns).reshape((TOKENS, TOP_K))
    expert_scores = jnp.clip(jnp.exp(math.log(1.0) - 2.9957323 * jax.random.uniform(own_keys[9], (TOKENS, TOP_K), jnp.float32) ** level_of(own_keys[9], (TOKENS, TOP_K), ((0, 16),), -0.2, 0.2)), 0.05, 1.0)
    gate_weight = scatter_about(key_of[10], (EXPERTS, D, FF), D ** -0.5, 0.125, ((0, 4), (2, 4)))
    up_weight = scatter_about(key_of[11], (EXPERTS, D, FF), D ** -0.5, 0.125, ((0, 4), (2, 4)))
    down_weight = scatter_about(key_of[12], (EXPERTS, FF, D), FF ** -0.5, 0.1875, ((0, 4), (1, 4)))
    return dict(queries=queries, keys=keys, values=values, stop_bias=stop_bias, out_weight=out_weight, mix_gain=mix_gain, moe_input=moe_input, ffn_gain=ffn_gain, expert_ids=expert_ids, expert_scores=expert_scores, gate_weight=gate_weight, up_weight=up_weight, down_weight=down_weight)


def norm_rows(values, gain):
    values = values.astype(jnp.float32)
    scale = lax.rsqrt(lax.optimization_barrier(jnp.mean(values * values, axis=-1, keepdims=True)) + 1e-06)
    return values * scale * gain

def settle(term):
    return lax.optimization_barrier(term.astype(jnp.bfloat16)).astype(jnp.float32)

def stick_head(inputs):
    query, key, value, bias = inputs
    length = query.shape[0]
    count = length // SEQ_DEV
    scores = jnp.dot(query, key.T, preferred_element_type=jnp.float32) * HEAD ** (-0.5)
    scores = scores + bias.astype(jnp.float32)[None, :]
    place = jnp.arange(length)
    past = place[None, :] < place[:, None]
    rest = jnp.where(past, jax.nn.log_sigmoid(-scores), 0.0)
    rest_blocks = rest.reshape(length, count, SEQ_DEV)
    later = lax.cumsum(rest_blocks, axis=2, reverse=True)
    within = (later - rest_blocks).reshape(length, length)
    totals = later[:, :, 0]
    local = jnp.where(past, jnp.exp(jax.nn.log_sigmoid(scores) + within), 0.0).astype(jnp.bfloat16)
    parts = jnp.einsum('tbs,bsd->tbd', local.reshape(length, count, SEQ_DEV).astype(jnp.float32), value.reshape(count, SEQ_DEV, HEAD).astype(jnp.float32), precision=lax.Precision.HIGHEST)
    carried = lax.cumsum(totals, axis=1, reverse=True) - totals
    return lax.optimization_barrier(jnp.sum(jnp.exp(carried)[:, :, None] * parts, axis=1))

def reference(queries, keys, values, stop_bias, out_weight, mix_gain, moe_input, ffn_gain, expert_ids, expert_scores, gate_weight, up_weight, down_weight):
    length = queries.shape[0]

    def by_head(array):
        return array.reshape(length, HEADS, HEAD).transpose(1, 0, 2)
    attended = lax.map(stick_head, (by_head(queries), by_head(keys), by_head(values), stop_bias.T))
    attended = attended.transpose(1, 0, 2).reshape(length, HEADS * HEAD).astype(jnp.bfloat16)
    group = HEADS * HEAD // N_TP
    projected = jnp.zeros((length, D), jnp.float32)
    for quarter in range(N_TP):
        term = jnp.dot(attended[:, quarter * group:(quarter + 1) * group], out_weight[quarter * group:(quarter + 1) * group], preferred_element_type=jnp.float32)
        projected = projected + settle(term)
    mixed = norm_rows(projected, mix_gain).astype(jnp.bfloat16)
    normed = norm_rows(moe_input, ffn_gain).astype(jnp.bfloat16)
    weights = expert_scores / lax.optimization_barrier(jnp.sum(expert_scores, axis=1, keepdims=True))
    load = N_EP * N_TP * CAP
    share = FF // N_TP

    def one_expert(total, expert):
        named = expert_ids == expert
        present = jnp.any(named, axis=1)
        weight = lax.optimization_barrier(jnp.sum(jnp.where(named, weights, 0.0), axis=1))
        chosen = jnp.nonzero(present, size=load, fill_value=0)[0].astype(jnp.int32)
        valid = jnp.arange(load) < jnp.sum(present.astype(jnp.int32))
        rows = normed[chosen]
        gate = jnp.dot(rows, gate_weight[expert], preferred_element_type=jnp.float32)
        upward = jnp.dot(rows, up_weight[expert], preferred_element_type=jnp.float32)
        hidden = (jax.nn.silu(gate) * upward).astype(jnp.bfloat16)
        lowering = down_weight[expert]
        summed = jnp.zeros((load, D), jnp.float32)
        for quarter in range(N_TP):
            term = jnp.dot(hidden[:, quarter * share:(quarter + 1) * share], lowering[quarter * share:(quarter + 1) * share], preferred_element_type=jnp.float32)
            summed = summed + settle(term)
        output = settle(summed)
        contribution = jnp.where(valid[:, None], weight[chosen][:, None] * output, 0.0)
        return (total.at[chosen].add(contribution), None)
    total, _ = lax.scan(one_expert, jnp.zeros((TOKENS, D), jnp.float32), jnp.arange(EXPERTS, dtype=jnp.int32))
    return (mixed, total.astype(jnp.bfloat16))
```

```python
import jax
import jax.numpy as jnp
from jax import lax
from jax.experimental import pallas as pl
from jax.experimental.pallas import tpu as pltpu
from jax.sharding import PartitionSpec as P


def norm_rows(values, gain):
    values = values.astype(jnp.float32)
    scale = lax.rsqrt(jnp.mean(values * values, axis=-1, keepdims=True) + 1e-06)
    return values * scale * gain


def break_terms(query_heads, query_place, key_block, bias_block, first):
    span = key_block.shape[0]
    heads = query_heads.shape[1]
    key_heads = key_block.reshape(span, heads, -1)
    scores = jnp.einsum("qhd,khd->hqk", query_heads, key_heads, preferred_element_type=jnp.float32)
    scores = scores * query_heads.shape[2] ** (-0.5) + bias_block.astype(jnp.float32).T[:, None, :]
    key_place = first + jnp.arange(span)
    past = (key_place[None, :] < query_place[:, None])[None]
    rest = jnp.where(past, jax.nn.log_sigmoid(-scores), 0.0)
    later = lax.cumsum(rest, axis=2, reverse=True)
    return (scores, past, rest, later)


def block_part(scores, past, rest, later, value_block, heads):
    within = later - rest
    local = jnp.where(past, jnp.exp(jax.nn.log_sigmoid(scores) + within), 0.0).astype(jnp.bfloat16)
    span = value_block.shape[0]
    value_heads = value_block.reshape(span, heads, -1)
    part = jnp.einsum("hqk,khd->qhd", local, value_heads, preferred_element_type=jnp.float32)
    return part.reshape(part.shape[0], -1)


def keep(state):
    return state


def dispatch_plan(normed, expert_ids, experts, capacity):
    rows, top = expert_ids.shape
    flat_ids = expert_ids.reshape(rows * top)
    onehot = (flat_ids[:, None] == jnp.arange(experts)[None, :]).astype(jnp.int32)
    earlier = jnp.cumsum(onehot, axis=0) - onehot
    place = jnp.sum(earlier * onehot, axis=1)
    target = flat_ids * capacity + place
    source = (
        jnp.zeros((experts * capacity,), jnp.int32)
        .at[target]
        .set(jnp.arange(rows * top, dtype=jnp.int32) // top + 1)
    )
    padded = jnp.concatenate([jnp.zeros((1, normed.shape[1]), normed.dtype), normed], axis=0)
    return (padded[source].reshape(experts, capacity, normed.shape[1]), target)


def expert_hidden(piece, gate_weight, up_weight):
    flat = piece.reshape(-1, piece.shape[-1])
    gate = jnp.dot(flat, gate_weight[0], preferred_element_type=jnp.float32)
    upward = jnp.dot(flat, up_weight[0], preferred_element_type=jnp.float32)
    hidden = (jax.nn.silu(gate) * upward).astype(jnp.bfloat16)
    return hidden.reshape(piece.shape[0], piece.shape[1], -1)


def send_back(summed):
    return lax.all_to_all(
        summed.astype(jnp.bfloat16), "ep", split_axis=0, concat_axis=0, tiled=True
    )


def return_rows(hidden_all, down_weight, sources):
    flat = hidden_all.reshape(-1, hidden_all.shape[2])
    product = jnp.dot(flat, down_weight[0], preferred_element_type=jnp.float32)
    return send_back(
        lax.psum_scatter(
            product.reshape(sources * lax.axis_size("tp"), hidden_all.shape[1], -1).astype(
                jnp.bfloat16
            ),
            "tp",
            scatter_dimension=0,
            tiled=True,
        ).astype(jnp.float32)
    )


def per_device_wide(
    queries,
    keys,
    values,
    stop_bias,
    out_weight,
    mix_gain,
    moe_input,
    ffn_gain,
    expert_ids,
    expert_scores,
    gate_weight,
    up_weight,
    down_weight,
):
    span = queries.shape[0]
    heads = stop_bias.shape[1]
    width_heads = queries.shape[1]
    blocks = lax.axis_size("ep")
    own_first = lax.axis_index("ep") * span
    query_heads = queries.reshape(span, heads, -1)
    query_place = own_first + jnp.arange(span)

    def piece_rows(piece, index):
        return tuple((lax.dynamic_slice_in_dim(member, index * span, span, 0) for member in piece))

    start_state = (
        jnp.zeros((blocks, heads, span), jnp.float32),
        jnp.zeros((blocks, span, width_heads), jnp.float32),
    )
    piece = (
        lax.all_gather(keys, "ep", axis=0, tiled=True),
        lax.all_gather(values, "ep", axis=0, tiled=True),
        lax.all_gather(stop_bias, "ep", axis=0, tiled=True),
    )

    def one_block(index, state):
        key_block, value_block, bias_block = piece_rows(piece, index)
        first = index * span

        def compute(inner_state):
            totals, parts = inner_state
            scores, past, rest, later = break_terms(
                query_heads, query_place, key_block, bias_block, first
            )
            part = block_part(scores, past, rest, later, value_block, heads)
            number = first // span
            totals = lax.dynamic_update_index_in_dim(totals, later[:, :, 0], number, 0)
            parts = lax.dynamic_update_index_in_dim(parts, part, number, 0)
            return (totals, parts)

        return lax.cond(first <= own_first, compute, keep, state)

    totals, parts = lax.fori_loop(0, piece[0].shape[0] // span, one_block, start_state)
    carried = lax.cumsum(totals, axis=0, reverse=True) - totals
    factor = jnp.exp(carried).transpose(0, 2, 1)[:, :, :, None]
    attended = jnp.sum(factor * parts.reshape(blocks, span, heads, -1), axis=0).reshape(
        span, width_heads
    )
    attended = attended.astype(jnp.bfloat16)
    projected = lax.psum_scatter(
        jnp.dot(attended, out_weight, preferred_element_type=jnp.float32).astype(jnp.bfloat16),
        "tp",
        scatter_dimension=0,
        tiled=True,
    ).astype(jnp.float32)
    mixed = norm_rows(projected, mix_gain).astype(jnp.bfloat16)
    normed = norm_rows(moe_input, ffn_gain).astype(jnp.bfloat16)
    rows, top = expert_ids.shape
    experts = lax.axis_size("ep")
    capacity = 3 * rows * top // (2 * experts)
    weights = expert_scores / jnp.sum(expert_scores, axis=1, keepdims=True)
    outbound, target = dispatch_plan(normed, expert_ids, experts, capacity)
    arrived = lax.all_to_all(outbound, "ep", split_axis=0, concat_axis=0, tiled=True)
    hidden_all = expert_hidden(
        lax.all_gather(arrived, "tp", axis=0, tiled=True), gate_weight, up_weight
    )
    returned = return_rows(hidden_all, down_weight, arrived.shape[0])
    picked = returned.reshape(experts * capacity, -1)[target].reshape(rows, top, -1)
    experts_mixed = jnp.sum(picked.astype(jnp.float32) * weights[:, :, None], axis=1).astype(
        jnp.bfloat16
    )
    return (mixed, experts_mixed)


VMEM = pl.BlockSpec(memory_space=pltpu.VMEM)
SMEM = pl.BlockSpec(memory_space=pltpu.SMEM)
ANY = pl.BlockSpec(memory_space=pl.ANY)


def shape_of(shape, dtype=jnp.bfloat16):
    return jax.ShapeDtypeStruct(shape, dtype)


def call(body, outs, ins, name, scratch=(), flops=0):
    return pl.pallas_call(
        body,
        out_shape=outs,
        in_specs=ins,
        out_specs=jax.tree.map(lambda _: VMEM, outs),
        scratch_shapes=scratch,
        name=name,
        compiler_params=pltpu.CompilerParams(vmem_limit_bytes=60 * 1024 * 1024),
        cost_estimate=pl.CostEstimate(flops=flops, transcendentals=0, bytes_accessed=0),
    )


def selections(place_ref, ids_ref, experts, capacity):
    rows, top = ids_ref.shape
    ids = ids_ref[...]
    lane = lax.broadcasted_iota(jnp.int32, (rows, 128), 1)
    expert = (place_ref[0] + lane) % experts
    chosen = jnp.zeros((rows, 128), jnp.float32)
    for k in range(top):
        chosen = chosen + jnp.where(ids[:, k : k + 1] == expert, 1.0, 0.0)
    chosen = jnp.where(lane < experts, chosen, 0.0)
    below = lax.broadcasted_iota(jnp.int32, (rows, rows), 1) < lax.broadcasted_iota(
        jnp.int32, (rows, rows), 0
    )
    rank = jnp.dot(
        below.astype(jnp.bfloat16), chosen.astype(jnp.bfloat16), preferred_element_type=jnp.float32
    )
    slot = lax.broadcasted_iota(jnp.int32, (rows, capacity), 1).astype(jnp.float32)
    picks = []
    for d in range(experts):
        hit = (rank[:, d : d + 1] == slot) & (chosen[:, d : d + 1] > 0.5)
        picks.append(jnp.where(hit, 1.0, 0.0).astype(jnp.bfloat16))
    return ids, expert, picks


def route_rows(place, moe_input, ffn_gain, expert_ids, experts, capacity):
    rows, width = moe_input.shape

    def body(place_ref, input_ref, gain_ref, ids_ref, *outs):
        normed = norm_rows(input_ref[...], gain_ref[...]).astype(jnp.bfloat16)
        _, _, picks = selections(place_ref, ids_ref, experts, capacity)
        for d in range(experts):
            outs[d][...] = lax.dot_general(
                picks[d], normed, (((0,), (0,)), ((), ())), preferred_element_type=jnp.float32
            ).astype(jnp.bfloat16)

    outs = [shape_of((capacity, width))] * experts
    return call(body, outs, [SMEM, VMEM, VMEM, VMEM], "route_rows", flops=4 * capacity * rows * width * 2)(
        place, moe_input, ffn_gain.reshape(1, width), expert_ids
    )


def combine_rows(place, expert_ids, expert_scores, returned):
    rows = expert_ids.shape[0]
    experts = len(returned)
    capacity, width = returned[0].shape

    def body(place_ref, ids_ref, scores_ref, *refs):
        ids, expert, picks = selections(place_ref, ids_ref, experts, capacity)
        scores = scores_ref[...]
        weights = scores / jnp.sum(scores, axis=1, keepdims=True)
        total = jnp.zeros((rows, width), jnp.float32)
        for d in range(experts):
            weight = jnp.zeros((rows, 1), jnp.float32)
            for k in range(ids.shape[1]):
                weight = weight + jnp.where(
                    ids[:, k : k + 1] == expert[:, d : d + 1], weights[:, k : k + 1], 0.0
                )
            total = total + weight * jnp.dot(
                picks[d], refs[d][...], preferred_element_type=jnp.float32
            )
        refs[-1][...] = total.astype(jnp.bfloat16)

    return call(
        body, shape_of((rows, width)), [SMEM, VMEM, VMEM] + [VMEM] * experts, "combine_rows",
        flops=4 * capacity * rows * width * 2,
    )(place, expert_ids, expert_scores, *returned)


def expert_part(rows_in, pieces, carried, last, name):
    capacity, width = rows_in[0].shape
    count = len(rows_in)
    hidden = sum(piece[0].shape[1] for piece in pieces)
    flat = [array for piece in pieces for array in piece]
    starts = []
    at = 0
    for piece in pieces:
        starts.append((at, piece[0].shape[1]))
        at += piece[0].shape[1]

    def body(*refs):
        row_refs = refs[:count]
        weight_refs = refs[count : count + len(flat)]
        rest = refs[count + len(flat) :]
        if carried is not None:
            acc_ref, rest = rest[0], rest[1:]
        outs = rest[: count if last else 1]
        gate_v, up_v, down_v, rows_v, sems = rest[len(outs) :]
        copies = []
        for kind, target in enumerate((gate_v, up_v, down_v)):
            for p, (begin, size) in enumerate(starts):
                number = kind * len(pieces) + p
                place = target.at[pl.ds(begin, size), :] if kind == 2 else target.at[:, pl.ds(begin, size)]
                copy = pltpu.make_async_copy(weight_refs[3 * p + kind], place, sems.at[number])
                copy.start()
                copies.append(copy)
        for d in range(count):
            rows_v[d * capacity : (d + 1) * capacity, :] = row_refs[d][...]
        for copy in copies[: len(pieces)]:
            copy.wait()
        rows = rows_v[...]
        gate = jnp.dot(rows, gate_v[...], preferred_element_type=jnp.float32)
        for copy in copies[len(pieces) : 2 * len(pieces)]:
            copy.wait()
        upward = jnp.dot(rows, up_v[...], preferred_element_type=jnp.float32)
        inner = (gate / (1.0 + jnp.exp(-gate)) * upward).astype(jnp.bfloat16)
        for copy in copies[2 * len(pieces) :]:
            copy.wait()
        out = jnp.dot(inner, down_v[...], preferred_element_type=jnp.float32)
        if carried is not None:
            out = out + acc_ref[...]
        if last:
            for d in range(count):
                outs[d][...] = out[d * capacity : (d + 1) * capacity].astype(jnp.bfloat16)
        else:
            outs[0][...] = out

    outs = (
        [shape_of((capacity, width))] * count
        if last
        else [shape_of((count * capacity, width), jnp.float32)]
    )
    extra = [] if carried is None else [carried]
    return call(
        body,
        outs,
        [VMEM] * count + [ANY] * len(flat) + [VMEM] * len(extra),
        name,
        scratch=(
            pltpu.VMEM((width, hidden), jnp.bfloat16),
            pltpu.VMEM((width, hidden), jnp.bfloat16),
            pltpu.VMEM((hidden, width), jnp.bfloat16),
            pltpu.VMEM((count * capacity, width), jnp.bfloat16),
            pltpu.SemaphoreType.DMA((3 * len(pieces),)),
        ),
        flops=6 * count * capacity * width * hidden,
    )(*rows_in, *flat, *extra)


def attend_project(place, queries, own, passed, out_weight, heads, quarters):
    span, width_heads = queries.shape
    size = width_heads // heads
    pair = 2 * size
    width = out_weight.shape[1]
    share = span // quarters
    blocks = 1 + len(passed)
    half = quarters // 2

    def body(place_ref, q_ref, own_ref, *refs):
        kv_refs = (own_ref,) + refs[: len(passed)]
        weight_ref, send_ref, keep_ref, acc, carry, att, proj = refs[len(passed) :]
        row = lax.broadcasted_iota(jnp.int32, (span, span), 0)
        column = lax.broadcasted_iota(jnp.int32, (span, span), 1)
        earlier = column < row
        after = jnp.where(row > column, 1.0, 0.0)
        sums = jnp.concatenate([after, jnp.ones((span, span), jnp.float32)], axis=1)
        sums = jnp.concatenate([sums, sums], axis=0).astype(jnp.bfloat16)
        low = lax.broadcasted_iota(jnp.int32, (span, pair), 1) < size

        def one_block(d):
            for h in range(heads):
                lanes = slice((h // 2) * pair, (h // 2 + 1) * pair)
                query = jnp.where(low if h % 2 == 0 else ~low, q_ref[:, lanes], 0.0).astype(jnp.bfloat16)
                key = kv_refs[d][:span, lanes]
                bias = kv_refs[d][span + h : span + h + 1, :span].astype(jnp.float32)
                z = lax.dot_general(
                    query, key, (((1,), (1,)), ((), ())), preferred_element_type=jnp.float32
                ) * size ** (-0.5) + bias
                rest = -(jnp.maximum(z, 0.0) + jnp.log1p(jnp.exp(-jnp.abs(z))))
                masked = jnp.where(earlier, rest, 0.0) if d == 0 else rest
                top = masked.astype(jnp.bfloat16)
                bottom = (masked - top.astype(jnp.float32)).astype(jnp.bfloat16)
                both = jnp.dot(
                    jnp.concatenate([top, bottom], axis=1), sums, preferred_element_type=jnp.float32
                )
                local = jnp.exp(z + rest + both[:, :span])
                if d == 0:
                    local = jnp.where(earlier, local, 0.0)
                value = kv_refs[d][:span, width_heads + lanes.start : width_heads + lanes.stop]
                part = jnp.dot(local.astype(jnp.bfloat16), value, preferred_element_type=jnp.float32)
                if d == 0:
                    carry[h] = both[:, span:]
                    total = part
                else:
                    before = carry[h]
                    total = jnp.exp(before) * part
                    carry[h] = before + both[:, span:]
                mine = low if h % 2 == 0 else ~low
                if d == 0 and h % 2 == 0:
                    acc[h // 2] = total
                elif d == 0:
                    acc[h // 2] = jnp.where(mine, total, acc[h // 2])
                else:
                    acc[h // 2] = acc[h // 2] + jnp.where(mine, total, 0.0)

        one_block(0)
        for d in range(1, blocks):
            pl.when(place_ref[0] >= d)(lambda d=d: one_block(d))
        for p in range(heads // 2):
            att[:, p * pair : (p + 1) * pair] = acc[p].astype(jnp.bfloat16)
        proj[...] = jnp.dot(att[...], weight_ref[...], preferred_element_type=jnp.float32)
        core = place_ref[1]
        for k in range(half):
            send_ref[k * share : (k + 1) * share, :] = proj[
                pl.ds((2 * k + 1 - core) * share, share), :
            ].astype(jnp.bfloat16)
            keep_ref[k * share : (k + 1) * share, :] = proj[pl.ds((2 * k + core) * share, share), :]

    return call(
        body,
        [shape_of((half * share, width)), shape_of((half * share, width), jnp.float32)],
        [SMEM, VMEM, VMEM] + [VMEM] * len(passed) + [VMEM],
        "attend_project",
        scratch=(
            pltpu.VMEM((heads // 2, span, pair), jnp.float32),
            pltpu.VMEM((heads, span, span), jnp.float32),
            pltpu.VMEM((span, width_heads), jnp.bfloat16),
            pltpu.VMEM((span, width), jnp.float32),
        ),
        flops=4 * blocks * span * span * width_heads + 2 * span * width_heads * width,
    )(place, queries, own, *passed, out_weight)


def per_device(
    queries,
    keys,
    values,
    stop_bias,
    out_weight,
    mix_gain,
    moe_input,
    ffn_gain,
    expert_ids,
    expert_scores,
    gate_weight,
    up_weight,
    down_weight,
):
    blocks = lax.axis_size("ep")
    shards = lax.axis_size("tp")
    group = lax.axis_index("grp")
    block = lax.axis_index("ep")
    shard = lax.axis_index("tp")
    place = jnp.stack([block, shard % 2]).astype(jnp.int32)
    heads = stop_bias.shape[1]
    span = queries.shape[0]

    def core(array):
        return lax.ppermute(array, "tp", [(i, i ^ 1) for i in range(shards)])

    def across(array):
        return lax.ppermute(array, "tp", [(i, i ^ 2) for i in range(shards)])

    def beside(array):
        return lax.ppermute(array, "grp", [(0, 1), (1, 0)])

    def turn(array, d):
        return lax.ppermute(array, "ep", [(i, (i + d) % blocks) for i in range(blocks)])

    def upward(array, d):
        return lax.ppermute(array, "ep", [(i, i + 1) for i in range(d - 1, blocks - 1)])

    rows, top = expert_ids.shape
    capacity = 3 * rows * top // (2 * blocks)
    outbound = route_rows(place, moe_input, ffn_gain, expert_ids, blocks, capacity)
    arrived = [outbound[0]] + [turn(outbound[d], d) for d in range(1, blocks)]

    mine = (gate_weight[0], up_weight[0], down_weight[0])
    part = mine[0].shape[1] // 2
    halves = (
        lax.dynamic_slice_in_dim(mine[0], group * part, part, 1),
        lax.dynamic_slice_in_dim(mine[1], group * part, part, 1),
        lax.dynamic_slice_in_dim(mine[2], group * part, part, 0),
    )
    far = tuple(across(array) for array in halves)
    near = tuple(core(array) for array in mine)
    other = tuple(beside(array) for array in far)
    far_near = tuple(core(array) for array in far)
    other_near = tuple(core(array) for array in other)

    own = jnp.concatenate(
        [
            jnp.concatenate([keys, values], axis=1),
            jnp.pad(stop_bias.T, ((0, 0), (0, 2 * keys.shape[1] - span))),
        ],
        axis=0,
    )
    passed = []
    for d in range(1, blocks):
        passed.append(upward(passed[-1] if passed else own, d))

    summed = expert_part(arrived, [mine, near], None, False, "expert_first")[0]
    produced = expert_part(arrived, [far, far_near, other, other_near], summed, True, "expert_last")
    returned = [produced[0]] + [turn(produced[d], -d) for d in range(1, blocks)]

    send, kept = attend_project(place, queries, own, passed, out_weight, heads, shards)
    chip = kept + core(send).astype(jnp.float32)
    share = span // shards
    first, second = chip[:share], chip[share:]
    outer = jnp.where(shard < 2, second, first).astype(jnp.bfloat16)
    inner = jnp.where(shard < 2, first, second)
    projected = inner + across(outer).astype(jnp.float32)
    mixed = norm_rows(projected, mix_gain).astype(jnp.bfloat16)

    experts_mixed = combine_rows(place, expert_ids, expert_scores, returned)
    return (mixed, experts_mixed)


def solution(mesh):
    sizes = mesh.shape
    paired = sizes["grp"] == 2 and sizes["tp"] == 4 and sizes["ep"] <= sizes["tp"]
    return jax.shard_map(
        per_device if paired else per_device_wide,
        mesh=mesh,
        in_specs=(
            P(("grp", "ep"), "tp"),
            P(("grp", "ep"), "tp"),
            P(("grp", "ep"), "tp"),
            P(("grp", "ep"), "tp"),
            P("tp", None),
            P(),
            P(("grp", "ep", "tp"), None),
            P(),
            P(("grp", "ep", "tp"), None),
            P(("grp", "ep", "tp"), None),
            P("ep", None, "tp"),
            P("ep", None, "tp"),
            P("ep", "tp", None),
        ),
        out_specs=(P(("grp", "ep", "tp"), None), P(("grp", "ep", "tp"), None)),
        check_vma=False,
    )
```

```python
import jax
import jax.numpy as jnp
from jax import lax
from jax.experimental import pallas as pl
from jax.experimental.pallas import tpu as pltpu
from jax.sharding import PartitionSpec as P


def norm_rows(values, gain):
    values = values.astype(jnp.float32)
    scale = lax.rsqrt(jnp.mean(values * values, axis=-1, keepdims=True) + 1e-06)
    return values * scale * gain


def break_terms(query_heads, query_place, key_block, bias_block, first):
    span = key_block.shape[0]
    heads = query_heads.shape[1]
    key_heads = key_block.reshape(span, heads, -1)
    scores = jnp.einsum("qhd,khd->hqk", query_heads, key_heads, preferred_element_type=jnp.float32)
    scores = scores * query_heads.shape[2] ** (-0.5) + bias_block.astype(jnp.float32).T[:, None, :]
    key_place = first + jnp.arange(span)
    past = (key_place[None, :] < query_place[:, None])[None]
    rest = jnp.where(past, jax.nn.log_sigmoid(-scores), 0.0)
    later = lax.cumsum(rest, axis=2, reverse=True)
    return (scores, past, rest, later)


def block_part(scores, past, rest, later, value_block, heads):
    within = later - rest
    local = jnp.where(past, jnp.exp(jax.nn.log_sigmoid(scores) + within), 0.0).astype(jnp.bfloat16)
    span = value_block.shape[0]
    value_heads = value_block.reshape(span, heads, -1)
    part = jnp.einsum("hqk,khd->qhd", local, value_heads, preferred_element_type=jnp.float32)
    return part.reshape(part.shape[0], -1)


def keep(state):
    return state


def dispatch_plan(normed, expert_ids, experts, capacity):
    rows, top = expert_ids.shape
    flat_ids = expert_ids.reshape(rows * top)
    onehot = (flat_ids[:, None] == jnp.arange(experts)[None, :]).astype(jnp.int32)
    earlier = jnp.cumsum(onehot, axis=0) - onehot
    place = jnp.sum(earlier * onehot, axis=1)
    target = flat_ids * capacity + place
    source = (
        jnp.zeros((experts * capacity,), jnp.int32)
        .at[target]
        .set(jnp.arange(rows * top, dtype=jnp.int32) // top + 1)
    )
    padded = jnp.concatenate([jnp.zeros((1, normed.shape[1]), normed.dtype), normed], axis=0)
    return (padded[source].reshape(experts, capacity, normed.shape[1]), target)


def expert_hidden(piece, gate_weight, up_weight):
    flat = piece.reshape(-1, piece.shape[-1])
    gate = jnp.dot(flat, gate_weight[0], preferred_element_type=jnp.float32)
    upward = jnp.dot(flat, up_weight[0], preferred_element_type=jnp.float32)
    hidden = (jax.nn.silu(gate) * upward).astype(jnp.bfloat16)
    return hidden.reshape(piece.shape[0], piece.shape[1], -1)


def send_back(summed):
    return lax.all_to_all(
        summed.astype(jnp.bfloat16), "ep", split_axis=0, concat_axis=0, tiled=True
    )


def return_rows(hidden_all, down_weight, sources):
    flat = hidden_all.reshape(-1, hidden_all.shape[2])
    product = jnp.dot(flat, down_weight[0], preferred_element_type=jnp.float32)
    return send_back(
        lax.psum_scatter(
            product.reshape(sources * lax.axis_size("tp"), hidden_all.shape[1], -1).astype(
                jnp.bfloat16
            ),
            "tp",
            scatter_dimension=0,
            tiled=True,
        ).astype(jnp.float32)
    )


def per_device_wide(
    queries,
    keys,
    values,
    stop_bias,
    out_weight,
    mix_gain,
    moe_input,
    ffn_gain,
    expert_ids,
    expert_scores,
    gate_weight,
    up_weight,
    down_weight,
):
    span = queries.shape[0]
    heads = stop_bias.shape[1]
    width_heads = queries.shape[1]
    blocks = lax.axis_size("ep")
    own_first = lax.axis_index("ep") * span
    query_heads = queries.reshape(span, heads, -1)
    query_place = own_first + jnp.arange(span)

    def piece_rows(piece, index):
        return tuple((lax.dynamic_slice_in_dim(member, index * span, span, 0) for member in piece))

    start_state = (
        jnp.zeros((blocks, heads, span), jnp.float32),
        jnp.zeros((blocks, span, width_heads), jnp.float32),
    )
    piece = (
        lax.all_gather(keys, "ep", axis=0, tiled=True),
        lax.all_gather(values, "ep", axis=0, tiled=True),
        lax.all_gather(stop_bias, "ep", axis=0, tiled=True),
    )

    def one_block(index, state):
        key_block, value_block, bias_block = piece_rows(piece, index)
        first = index * span

        def compute(inner_state):
            totals, parts = inner_state
            scores, past, rest, later = break_terms(
                query_heads, query_place, key_block, bias_block, first
            )
            part = block_part(scores, past, rest, later, value_block, heads)
            number = first // span
            totals = lax.dynamic_update_index_in_dim(totals, later[:, :, 0], number, 0)
            parts = lax.dynamic_update_index_in_dim(parts, part, number, 0)
            return (totals, parts)

        return lax.cond(first <= own_first, compute, keep, state)

    totals, parts = lax.fori_loop(0, piece[0].shape[0] // span, one_block, start_state)
    carried = lax.cumsum(totals, axis=0, reverse=True) - totals
    factor = jnp.exp(carried).transpose(0, 2, 1)[:, :, :, None]
    attended = jnp.sum(factor * parts.reshape(blocks, span, heads, -1), axis=0).reshape(
        span, width_heads
    )
    attended = attended.astype(jnp.bfloat16)
    projected = lax.psum_scatter(
        jnp.dot(attended, out_weight, preferred_element_type=jnp.float32).astype(jnp.bfloat16),
        "tp",
        scatter_dimension=0,
        tiled=True,
    ).astype(jnp.float32)
    mixed = norm_rows(projected, mix_gain).astype(jnp.bfloat16)
    normed = norm_rows(moe_input, ffn_gain).astype(jnp.bfloat16)
    rows, top = expert_ids.shape
    experts = lax.axis_size("ep")
    capacity = 3 * rows * top // (2 * experts)
    weights = expert_scores / jnp.sum(expert_scores, axis=1, keepdims=True)
    outbound, target = dispatch_plan(normed, expert_ids, experts, capacity)
    arrived = lax.all_to_all(outbound, "ep", split_axis=0, concat_axis=0, tiled=True)
    hidden_all = expert_hidden(
        lax.all_gather(arrived, "tp", axis=0, tiled=True), gate_weight, up_weight
    )
    returned = return_rows(hidden_all, down_weight, arrived.shape[0])
    picked = returned.reshape(experts * capacity, -1)[target].reshape(rows, top, -1)
    experts_mixed = jnp.sum(picked.astype(jnp.float32) * weights[:, :, None], axis=1).astype(
        jnp.bfloat16
    )
    return (mixed, experts_mixed)


VMEM = pl.BlockSpec(memory_space=pltpu.VMEM)
SMEM = pl.BlockSpec(memory_space=pltpu.SMEM)
ANY = pl.BlockSpec(memory_space=pl.ANY)


def shape_of(shape, dtype=jnp.bfloat16):
    return jax.ShapeDtypeStruct(shape, dtype)


def call(body, outs, ins, scratch=(), flops=0, limit=24):
    return pl.pallas_call(
        body,
        out_shape=outs,
        in_specs=ins,
        out_specs=jax.tree.map(lambda _: VMEM, outs),
        scratch_shapes=scratch,
        compiler_params=pltpu.CompilerParams(vmem_limit_bytes=limit * 1024 * 1024),
        cost_estimate=pl.CostEstimate(flops=flops, transcendentals=0, bytes_accessed=0),
    )


def selections(place_ref, ids_ref, experts, capacity):
    rows, top = ids_ref.shape
    ids = ids_ref[...]
    lane = lax.broadcasted_iota(jnp.int32, (rows, 128), 1)
    expert = (place_ref[0] + lane) % experts
    chosen = jnp.zeros((rows, 128), jnp.float32)
    for k in range(top):
        chosen = chosen + jnp.where(ids[:, k : k + 1] == expert, 1.0, 0.0)
    chosen = jnp.where(lane < experts, chosen, 0.0)
    below = lax.broadcasted_iota(jnp.int32, (rows, rows), 1) < lax.broadcasted_iota(
        jnp.int32, (rows, rows), 0
    )
    rank = jnp.dot(
        below.astype(jnp.bfloat16), chosen.astype(jnp.bfloat16), preferred_element_type=jnp.float32
    )
    slot = lax.broadcasted_iota(jnp.int32, (rows, capacity), 1).astype(jnp.float32)
    picks = []
    for d in range(experts):
        hit = (rank[:, d : d + 1] == slot) & (chosen[:, d : d + 1] > 0.5)
        picks.append(jnp.where(hit, 1.0, 0.0).astype(jnp.bfloat16))
    return ids, expert, picks


def route_rows(place, moe_input, ffn_gain, expert_ids, experts, capacity):
    rows, width = moe_input.shape

    def body(place_ref, input_ref, gain_ref, ids_ref, *outs):
        normed = norm_rows(input_ref[...], gain_ref[...]).astype(jnp.bfloat16)
        _, _, picks = selections(place_ref, ids_ref, experts, capacity)
        for d in range(experts):
            outs[d][...] = lax.dot_general(
                picks[d], normed, (((0,), (0,)), ((), ())), preferred_element_type=jnp.float32
            ).astype(jnp.bfloat16)

    outs = [shape_of((capacity, width))] * experts
    return call(body, outs, [SMEM, VMEM, VMEM, VMEM], flops=4 * capacity * rows * width * 2)(
        place, moe_input, ffn_gain.reshape(1, width), expert_ids
    )


def combine_rows(place, expert_ids, expert_scores, returned):
    rows = expert_ids.shape[0]
    experts = len(returned)
    capacity, width = returned[0].shape

    def body(place_ref, ids_ref, scores_ref, *refs):
        ids, expert, picks = selections(place_ref, ids_ref, experts, capacity)
        scores = scores_ref[...]
        weights = scores / jnp.sum(scores, axis=1, keepdims=True)
        total = jnp.zeros((rows, width), jnp.float32)
        for d in range(experts):
            weight = jnp.zeros((rows, 1), jnp.float32)
            for k in range(ids.shape[1]):
                weight = weight + jnp.where(
                    ids[:, k : k + 1] == expert[:, d : d + 1], weights[:, k : k + 1], 0.0
                )
            total = total + weight * jnp.dot(
                picks[d], refs[d][...], preferred_element_type=jnp.float32
            )
        refs[-1][...] = total.astype(jnp.bfloat16)

    return call(
        body, shape_of((rows, width)), [SMEM, VMEM, VMEM] + [VMEM] * experts,
        flops=4 * capacity * rows * width * 2,
    )(place, expert_ids, expert_scores, *returned)


def expert_part(rows_in, pieces, carried, last):
    capacity, width = rows_in[0].shape
    count = len(rows_in)
    hidden = sum(piece[0].shape[1] for piece in pieces)
    flat = [array for piece in pieces for array in piece]

    def body(*refs):
        row_refs = refs[:count]
        weight_refs = refs[count : count + len(flat)]
        rest = refs[count + len(flat) :]
        if carried is not None:
            acc_ref, rest = rest[0], rest[1:]
        rows = jnp.concatenate([ref[...] for ref in row_refs], axis=0)
        inner = []
        for p in range(len(pieces)):
            size = weight_refs[3 * p].shape[1]
            both = jnp.concatenate([weight_refs[3 * p][...], weight_refs[3 * p + 1][...]], axis=1)
            product = jnp.dot(rows, both, preferred_element_type=jnp.float32)
            gate, upward = product[:, :size], product[:, size:]
            inner.append((gate / (1.0 + jnp.exp(-gate)) * upward).astype(jnp.bfloat16))
        inner = jnp.concatenate(inner, axis=1)
        down = jnp.concatenate([weight_refs[3 * p + 2][...] for p in range(len(pieces))], axis=0)
        if last:
            for d in range(count):
                some = slice(d * capacity, (d + 1) * capacity)
                out = jnp.dot(inner[some], down, preferred_element_type=jnp.float32)
                rest[d][...] = (out + acc_ref[some]).astype(jnp.bfloat16)
        else:
            out = jnp.dot(inner, down, preferred_element_type=jnp.float32)
            rest[0][...] = out if carried is None else out + acc_ref[...]

    outs = (
        [shape_of((capacity, width))] * count
        if last
        else [shape_of((count * capacity, width), jnp.float32)]
    )
    extra = [] if carried is None else [carried]
    return call(
        body,
        outs,
        [VMEM] * (count + len(flat) + len(extra)),
        flops=6 * count * capacity * width * hidden,
    )(*rows_in, *flat, *extra)


def attend_project(place, queries, own, passed, out_weight, heads, quarters):
    span, width_heads = queries.shape
    size = width_heads // heads
    pair = 2 * size
    width = out_weight.shape[1]
    share = span // quarters
    blocks = 1 + len(passed)
    half = quarters // 2

    def body(place_ref, q_ref, own_ref, *refs):
        kv_refs = (own_ref,) + refs[: len(passed)]
        weight_ref, send_ref, keep_ref, acc, carry, att, proj = refs[len(passed) :]
        row = lax.broadcasted_iota(jnp.int32, (span, span), 0)
        column = lax.broadcasted_iota(jnp.int32, (span, span), 1)
        earlier = column < row
        after = jnp.where(row > column, 1.0, 0.0)
        sums = jnp.concatenate([after, jnp.ones((span, span), jnp.float32)], axis=1)
        sums = jnp.concatenate([sums, sums], axis=0).astype(jnp.bfloat16)
        low = lax.broadcasted_iota(jnp.int32, (span, pair), 1) < size

        def one_block(d):
            for h in range(heads):
                lanes = slice((h // 2) * pair, (h // 2 + 1) * pair)
                query = jnp.where(low if h % 2 == 0 else ~low, q_ref[:, lanes], 0.0).astype(jnp.bfloat16)
                key = kv_refs[d][:span, lanes]
                bias = kv_refs[d][span + h : span + h + 1, :span].astype(jnp.float32)
                z = lax.dot_general(
                    query, key, (((1,), (1,)), ((), ())), preferred_element_type=jnp.float32
                ) * size ** (-0.5) + bias
                rest = -(jnp.maximum(z, 0.0) + jnp.log1p(jnp.exp(-jnp.abs(z))))
                masked = jnp.where(earlier, rest, 0.0) if d == 0 else rest
                top = masked.astype(jnp.bfloat16)
                bottom = (masked - top.astype(jnp.float32)).astype(jnp.bfloat16)
                both = jnp.dot(
                    jnp.concatenate([top, bottom], axis=1), sums, preferred_element_type=jnp.float32
                )
                local = jnp.exp(z + rest + both[:, :span])
                if d == 0:
                    local = jnp.where(earlier, local, 0.0)
                value = kv_refs[d][:span, width_heads + lanes.start : width_heads + lanes.stop]
                part = jnp.dot(local.astype(jnp.bfloat16), value, preferred_element_type=jnp.float32)
                if d == 0:
                    carry[h] = both[:, span:]
                    total = part
                else:
                    before = carry[h]
                    total = jnp.exp(before) * part
                    carry[h] = before + both[:, span:]
                mine = low if h % 2 == 0 else ~low
                if d == 0 and h % 2 == 0:
                    acc[h // 2] = total
                elif d == 0:
                    acc[h // 2] = jnp.where(mine, total, acc[h // 2])
                else:
                    acc[h // 2] = acc[h // 2] + jnp.where(mine, total, 0.0)

        one_block(0)
        for d in range(1, blocks):
            pl.when(place_ref[0] >= d)(lambda d=d: one_block(d))
        for p in range(heads // 2):
            att[:, p * pair : (p + 1) * pair] = acc[p].astype(jnp.bfloat16)
        proj[...] = jnp.dot(att[...], weight_ref[...], preferred_element_type=jnp.float32)
        core = place_ref[1]
        for k in range(half):
            send_ref[k * share : (k + 1) * share, :] = proj[
                pl.ds((2 * k + 1 - core) * share, share), :
            ].astype(jnp.bfloat16)
            keep_ref[k * share : (k + 1) * share, :] = proj[pl.ds((2 * k + core) * share, share), :]

    return call(
        body,
        [shape_of((half * share, width)), shape_of((half * share, width), jnp.float32)],
        [SMEM, VMEM, VMEM] + [VMEM] * len(passed) + [VMEM],
        scratch=(
            pltpu.VMEM((heads // 2, span, pair), jnp.float32),
            pltpu.VMEM((heads, span, span), jnp.float32),
            pltpu.VMEM((span, width_heads), jnp.bfloat16),
            pltpu.VMEM((span, width), jnp.float32),
        ),
        flops=4 * blocks * span * span * width_heads + 2 * span * width_heads * width,
    )(place, queries, own, *passed, out_weight)


def per_device(*arrays):
    return paired_step(*arrays)


def paired_step(
    queries,
    keys,
    values,
    stop_bias,
    out_weight,
    mix_gain,
    moe_input,
    ffn_gain,
    expert_ids,
    expert_scores,
    gate_weight,
    up_weight,
    down_weight,
):
    blocks = lax.axis_size("ep")
    shards = lax.axis_size("tp")
    group = lax.axis_index("grp")
    block = lax.axis_index("ep")
    shard = lax.axis_index("tp")
    place = jnp.stack([block, shard % 2]).astype(jnp.int32)
    heads = stop_bias.shape[1]
    span = queries.shape[0]

    def core(array):
        return lax.ppermute(array, "tp", [(i, i ^ 1) for i in range(shards)])

    def across(array):
        return lax.ppermute(array, "tp", [(i, i ^ 2) for i in range(shards)])

    def beside(array):
        return lax.ppermute(array, "grp", [(0, 1), (1, 0)])

    def turn(array, d):
        return lax.ppermute(array, "ep", [(i, (i + d) % blocks) for i in range(blocks)])

    def upward(array, d):
        return lax.ppermute(array, "ep", [(i, i + 1) for i in range(d - 1, blocks - 1)])

    mine = (gate_weight[0], up_weight[0], down_weight[0])
    part = mine[0].shape[1] // 2
    gate_half = lax.dynamic_slice_in_dim(mine[0], group * part, part, 1)

    rows, top = expert_ids.shape
    capacity = 3 * rows * top // (2 * blocks)
    outbound = route_rows(place, moe_input, ffn_gain, expert_ids, blocks, capacity)
    arrived = [outbound[0]] + [turn(outbound[d], d) for d in range(1, blocks)]

    halves = (
        gate_half,
        lax.dynamic_slice_in_dim(mine[1], group * part, part, 1),
        lax.dynamic_slice_in_dim(mine[2], group * part, part, 0),
    )
    far = tuple(across(array) for array in halves)
    near = tuple(core(array) for array in mine)
    other = tuple(beside(array) for array in far)
    far_near = tuple(core(array) for array in far)
    other_near = tuple(core(array) for array in other)

    own = jnp.concatenate(
        [
            jnp.concatenate([keys, values], axis=1),
            jnp.pad(stop_bias.T, ((0, 0), (0, 2 * keys.shape[1] - span))),
        ],
        axis=0,
    )
    passed = []
    for d in range(1, blocks):
        passed.append(upward(passed[-1] if passed else own, d))

    summed = expert_part(arrived, [mine, near], None, False)[0]
    summed = expert_part(arrived, [far, far_near], summed, False)[0]
    produced = expert_part(arrived, [other, other_near], summed, True)
    returned = [produced[0]] + [turn(produced[d], -d) for d in range(1, blocks)]

    send, kept = attend_project(place, queries, own, passed, out_weight, heads, shards)
    chip = kept + core(send).astype(jnp.float32)
    share = span // shards
    first, second = chip[:share], chip[share:]
    outer = jnp.where(shard < 2, second, first).astype(jnp.bfloat16)
    inner = jnp.where(shard < 2, first, second)
    projected = inner + across(outer).astype(jnp.float32)
    mixed = norm_rows(projected, mix_gain).astype(jnp.bfloat16)

    experts_mixed = combine_rows(place, expert_ids, expert_scores, returned)
    return (mixed, experts_mixed)


def solution(mesh):
    sizes = mesh.shape
    paired = sizes["grp"] == 2 and sizes["tp"] == 4 and sizes["ep"] <= sizes["tp"]
    return jax.shard_map(
        per_device if paired else per_device_wide,
        mesh=mesh,
        in_specs=(
            P(("grp", "ep"), "tp"),
            P(("grp", "ep"), "tp"),
            P(("grp", "ep"), "tp"),
            P(("grp", "ep"), "tp"),
            P("tp", None),
            P(),
            P(("grp", "ep", "tp"), None),
            P(),
            P(("grp", "ep", "tp"), None),
            P(("grp", "ep", "tp"), None),
            P("ep", None, "tp"),
            P("ep", None, "tp"),
            P("ep", "tp", None),
        ),
        out_specs=(P(("grp", "ep", "tp"), None), P(("grp", "ep", "tp"), None)),
        check_vma=False,
    )
```

```python
import jax
import jax.numpy as jnp
from jax import lax
from jax.experimental import pallas as pl
from jax.experimental.pallas import tpu as pltpu
from jax.sharding import PartitionSpec as P


def norm_rows(values, gain):
    values = values.astype(jnp.float32)
    scale = lax.rsqrt(jnp.mean(values * values, axis=-1, keepdims=True) + 1e-06)
    return values * scale * gain


def break_terms(query_heads, query_place, key_block, bias_block, first):
    span = key_block.shape[0]
    heads = query_heads.shape[1]
    key_heads = key_block.reshape(span, heads, -1)
    scores = jnp.einsum("qhd,khd->hqk", query_heads, key_heads, preferred_element_type=jnp.float32)
    scores = scores * query_heads.shape[2] ** (-0.5) + bias_block.astype(jnp.float32).T[:, None, :]
    key_place = first + jnp.arange(span)
    past = (key_place[None, :] < query_place[:, None])[None]
    rest = jnp.where(past, jax.nn.log_sigmoid(-scores), 0.0)
    later = lax.cumsum(rest, axis=2, reverse=True)
    return (scores, past, rest, later)


def block_part(scores, past, rest, later, value_block, heads):
    within = later - rest
    local = jnp.where(past, jnp.exp(jax.nn.log_sigmoid(scores) + within), 0.0).astype(jnp.bfloat16)
    span = value_block.shape[0]
    value_heads = value_block.reshape(span, heads, -1)
    part = jnp.einsum("hqk,khd->qhd", local, value_heads, preferred_element_type=jnp.float32)
    return part.reshape(part.shape[0], -1)


def keep(state):
    return state


def dispatch_plan(normed, expert_ids, experts, capacity):
    rows, top = expert_ids.shape
    flat_ids = expert_ids.reshape(rows * top)
    onehot = (flat_ids[:, None] == jnp.arange(experts)[None, :]).astype(jnp.int32)
    earlier = jnp.cumsum(onehot, axis=0) - onehot
    place = jnp.sum(earlier * onehot, axis=1)
    target = flat_ids * capacity + place
    source = (
        jnp.zeros((experts * capacity,), jnp.int32)
        .at[target]
        .set(jnp.arange(rows * top, dtype=jnp.int32) // top + 1)
    )
    padded = jnp.concatenate([jnp.zeros((1, normed.shape[1]), normed.dtype), normed], axis=0)
    return (padded[source].reshape(experts, capacity, normed.shape[1]), target)


def expert_hidden(piece, gate_weight, up_weight):
    flat = piece.reshape(-1, piece.shape[-1])
    gate = jnp.dot(flat, gate_weight[0], preferred_element_type=jnp.float32)
    upward = jnp.dot(flat, up_weight[0], preferred_element_type=jnp.float32)
    hidden = (jax.nn.silu(gate) * upward).astype(jnp.bfloat16)
    return hidden.reshape(piece.shape[0], piece.shape[1], -1)


def send_back(summed):
    return lax.all_to_all(
        summed.astype(jnp.bfloat16), "ep", split_axis=0, concat_axis=0, tiled=True
    )


def return_rows(hidden_all, down_weight, sources):
    flat = hidden_all.reshape(-1, hidden_all.shape[2])
    product = jnp.dot(flat, down_weight[0], preferred_element_type=jnp.float32)
    return send_back(
        lax.psum_scatter(
            product.reshape(sources * lax.axis_size("tp"), hidden_all.shape[1], -1).astype(
                jnp.bfloat16
            ),
            "tp",
            scatter_dimension=0,
            tiled=True,
        ).astype(jnp.float32)
    )


def per_device_wide(
    queries,
    keys,
    values,
    stop_bias,
    out_weight,
    mix_gain,
    moe_input,
    ffn_gain,
    expert_ids,
    expert_scores,
    gate_weight,
    up_weight,
    down_weight,
):
    span = queries.shape[0]
    heads = stop_bias.shape[1]
    width_heads = queries.shape[1]
    blocks = lax.axis_size("ep")
    own_first = lax.axis_index("ep") * span
    query_heads = queries.reshape(span, heads, -1)
    query_place = own_first + jnp.arange(span)

    def piece_rows(piece, index):
        return tuple((lax.dynamic_slice_in_dim(member, index * span, span, 0) for member in piece))

    start_state = (
        jnp.zeros((blocks, heads, span), jnp.float32),
        jnp.zeros((blocks, span, width_heads), jnp.float32),
    )
    piece = (
        lax.all_gather(keys, "ep", axis=0, tiled=True),
        lax.all_gather(values, "ep", axis=0, tiled=True),
        lax.all_gather(stop_bias, "ep", axis=0, tiled=True),
    )

    def one_block(index, state):
        key_block, value_block, bias_block = piece_rows(piece, index)
        first = index * span

        def compute(inner_state):
            totals, parts = inner_state
            scores, past, rest, later = break_terms(
                query_heads, query_place, key_block, bias_block, first
            )
            part = block_part(scores, past, rest, later, value_block, heads)
            number = first // span
            totals = lax.dynamic_update_index_in_dim(totals, later[:, :, 0], number, 0)
            parts = lax.dynamic_update_index_in_dim(parts, part, number, 0)
            return (totals, parts)

        return lax.cond(first <= own_first, compute, keep, state)

    totals, parts = lax.fori_loop(0, piece[0].shape[0] // span, one_block, start_state)
    carried = lax.cumsum(totals, axis=0, reverse=True) - totals
    factor = jnp.exp(carried).transpose(0, 2, 1)[:, :, :, None]
    attended = jnp.sum(factor * parts.reshape(blocks, span, heads, -1), axis=0).reshape(
        span, width_heads
    )
    attended = attended.astype(jnp.bfloat16)
    projected = lax.psum_scatter(
        jnp.dot(attended, out_weight, preferred_element_type=jnp.float32).astype(jnp.bfloat16),
        "tp",
        scatter_dimension=0,
        tiled=True,
    ).astype(jnp.float32)
    mixed = norm_rows(projected, mix_gain).astype(jnp.bfloat16)
    normed = norm_rows(moe_input, ffn_gain).astype(jnp.bfloat16)
    rows, top = expert_ids.shape
    experts = lax.axis_size("ep")
    capacity = 3 * rows * top // (2 * experts)
    weights = expert_scores / jnp.sum(expert_scores, axis=1, keepdims=True)
    outbound, target = dispatch_plan(normed, expert_ids, experts, capacity)
    arrived = lax.all_to_all(outbound, "ep", split_axis=0, concat_axis=0, tiled=True)
    hidden_all = expert_hidden(
        lax.all_gather(arrived, "tp", axis=0, tiled=True), gate_weight, up_weight
    )
    returned = return_rows(hidden_all, down_weight, arrived.shape[0])
    picked = returned.reshape(experts * capacity, -1)[target].reshape(rows, top, -1)
    experts_mixed = jnp.sum(picked.astype(jnp.float32) * weights[:, :, None], axis=1).astype(
        jnp.bfloat16
    )
    return (mixed, experts_mixed)


VMEM = pl.BlockSpec(memory_space=pltpu.VMEM)
SMEM = pl.BlockSpec(memory_space=pltpu.SMEM)
HBM = pl.BlockSpec(memory_space=pltpu.HBM)


def shape_of(shape, dtype=jnp.bfloat16):
    return jax.ShapeDtypeStruct(shape, dtype)


def call(body, outs, ins, scratch=(), flops=0, limit=24):
    return pl.pallas_call(
        body,
        out_shape=outs,
        in_specs=ins,
        out_specs=jax.tree.map(lambda _: VMEM, outs),
        scratch_shapes=scratch,
        compiler_params=pltpu.CompilerParams(vmem_limit_bytes=limit * 1024 * 1024),
        cost_estimate=pl.CostEstimate(flops=flops, transcendentals=0, bytes_accessed=0),
    )


def selections(place_ref, ids_ref, experts, capacity):
    top, rows = ids_ref.shape
    distance = lax.broadcasted_iota(jnp.int32, (8, rows), 0)
    expert = (place_ref[0] + distance) % experts
    hits = [ids_ref[k : k + 1, :] == expert for k in range(top)]
    chosen = jnp.zeros((8, rows), jnp.float32)
    for hit in hits:
        chosen = chosen + jnp.where(hit & (distance < experts), 1.0, 0.0)
    below = lax.broadcasted_iota(jnp.int32, (rows, rows), 0) < lax.broadcasted_iota(
        jnp.int32, (rows, rows), 1
    )
    rank = jnp.dot(
        chosen.astype(jnp.bfloat16),
        jnp.where(below, 1.0, 0.0).astype(jnp.bfloat16),
        preferred_element_type=jnp.float32,
    )
    slot = lax.broadcasted_iota(jnp.int32, (capacity, rows), 0).astype(jnp.float32)
    picks = []
    for d in range(experts):
        pick = (rank[d : d + 1, :] == slot) & (chosen[d : d + 1, :] > 0.5)
        picks.append(jnp.where(pick, 1.0, 0.0).astype(jnp.bfloat16))
    return hits, picks


def prepare(place, moe_input, ffn_gain, ids, keys, values, bias, weights, experts, capacity):
    rows, width = moe_input.shape
    span, heads_width = keys.shape
    heads = bias.shape[0]
    gate, upward, down = weights
    part = gate.shape[1] // 2
    deep = gate.shape[0] // 2
    thin = part // 2

    def body(place_ref, gain_hbm, ids_hbm, bias_hbm, input_hbm, keys_hbm, values_hbm, *refs):
        gate_hbm, up_hbm, down_hbm = refs[:3]
        outs = refs[3 : 3 + experts]
        own_ref, gate_a, gate_b, up_a, up_b, down_a, down_b = refs[3 + experts : 10 + experts]
        input_v, gain_v, ids_v, bias_v, sems = refs[10 + experts :]
        begin = pl.multiple_of(place_ref[2] * part, part)
        columns = pl.ds(begin, part)
        moves = [
            (ids_hbm, ids_v),
            (input_hbm, input_v),
            (gain_hbm, gain_v),
            (bias_hbm, bias_v),
            (gate_hbm.at[pl.ds(0, deep), columns], gate_a),
            (gate_hbm.at[pl.ds(deep, deep), columns], gate_b),
            (keys_hbm, own_ref.at[pl.ds(0, span), pl.ds(0, heads_width)]),
            (values_hbm, own_ref.at[pl.ds(0, span), pl.ds(heads_width, heads_width)]),
            (up_hbm.at[pl.ds(0, deep), columns], up_a),
            (up_hbm.at[pl.ds(deep, deep), columns], up_b),
            (down_hbm.at[pl.ds(begin, thin), :], down_a),
            (down_hbm.at[pl.ds(pl.multiple_of(begin + thin, thin), thin), :], down_b),
        ]
        copies = [
            pltpu.make_async_copy(source, target, sems.at[k])
            for k, (source, target) in enumerate(moves)
        ]
        for copy in copies:
            copy.start()
        own_ref[span:, :] = jnp.zeros((heads, 2 * heads_width), jnp.bfloat16)
        copies[0].wait()
        _, picks = selections(place_ref, ids_v, experts, capacity)
        copies[1].wait()
        copies[2].wait()
        normed = norm_rows(input_v[...], gain_v[...]).astype(jnp.bfloat16)
        for d in range(experts):
            outs[d][...] = jnp.dot(
                picks[d], normed, preferred_element_type=jnp.float32
            ).astype(jnp.bfloat16)
        copies[3].wait()
        own_ref[span:, :span] = bias_v[...]
        for copy in copies[4:]:
            copy.wait()

    outs = [shape_of((capacity, width))] * experts + [
        shape_of((span + heads, 2 * heads_width)),
        shape_of((deep, part)),
        shape_of((deep, part)),
        shape_of((deep, part)),
        shape_of((deep, part)),
        shape_of((thin, width)),
        shape_of((thin, width)),
    ]
    return call(
        body,
        outs,
        [SMEM] + [HBM] * 9,
        scratch=(
            pltpu.VMEM((rows, width), jnp.bfloat16),
            pltpu.VMEM((1, width), jnp.float32),
            pltpu.VMEM(ids.shape, jnp.int32),
            pltpu.VMEM(bias.shape, jnp.bfloat16),
            pltpu.SemaphoreType.DMA((12,)),
        ),
        flops=2 * experts * capacity * rows * width,
    )(
        place,
        *(
            pltpu.with_memory_space_constraint(array, pltpu.HBM)
            for array in (
                ffn_gain.reshape(1, width),
                ids,
                bias,
                moe_input,
                keys,
                values,
                gate,
                upward,
                down,
            )
        ),
    )


def combine_rows(place, ids, scores, returned):
    rows = ids.shape[1]
    experts = len(returned)
    capacity, width = returned[0].shape

    def body(place_ref, ids_ref, scores_ref, *refs):
        hits, picks = selections(place_ref, ids_ref, experts, capacity)
        shares = scores_ref[...]
        shares = shares / jnp.sum(shares, axis=0, keepdims=True)
        weight = jnp.zeros((8, rows), jnp.float32)
        for k, hit in enumerate(hits):
            weight = weight + jnp.where(hit, shares[k : k + 1, :], 0.0)
        weight = weight.T
        total = jnp.zeros((rows, width), jnp.float32)
        for d in range(experts):
            total = total + weight[:, d : d + 1] * lax.dot_general(
                picks[d], refs[d][...], (((0,), (0,)), ((), ())), preferred_element_type=jnp.float32
            )
        refs[-1][...] = total.astype(jnp.bfloat16)

    return call(
        body, shape_of((rows, width)), [SMEM, VMEM, VMEM] + [VMEM] * experts,
        flops=2 * experts * capacity * rows * width,
    )(place, ids, scores, *returned)


def expert_part(rows_in, pieces, carried, last):
    capacity, width = rows_in[0].shape
    count = len(rows_in)
    hidden = sum(piece[0][0].shape[1] for piece in pieces)
    flat = [array for piece in pieces for kind in piece for array in kind]

    def body(*refs):
        row_refs = refs[:count]
        weight_refs = refs[count : count + len(flat)]
        rest = refs[count + len(flat) :]
        if carried is not None:
            acc_ref, rest = rest[0], rest[1:]
        rows = jnp.concatenate([ref[...] for ref in row_refs], axis=0)
        inner, down = [], []
        at = 0
        for piece in pieces:
            kinds = []
            for kind in piece:
                chunk = [ref[...] for ref in weight_refs[at : at + len(kind)]]
                kinds.append(chunk[0] if len(chunk) == 1 else jnp.concatenate(chunk, axis=0))
                at += len(kind)
            size = kinds[0].shape[1]
            both = jnp.concatenate(kinds[:2], axis=1)
            down.append(kinds[2])
            product = jnp.dot(rows, both, preferred_element_type=jnp.float32)
            gate, upward = product[:, :size], product[:, size:]
            inner.append((gate / (1.0 + jnp.exp(-gate)) * upward).astype(jnp.bfloat16))
        inner = jnp.concatenate(inner, axis=1)
        down = jnp.concatenate(down, axis=0)
        if last:
            for d in range(count):
                some = slice(d * capacity, (d + 1) * capacity)
                out = jnp.dot(inner[some], down, preferred_element_type=jnp.float32)
                rest[d][...] = (out + acc_ref[some]).astype(jnp.bfloat16)
        else:
            out = jnp.dot(inner, down, preferred_element_type=jnp.float32)
            rest[0][...] = out if carried is None else out + acc_ref[...]

    outs = (
        [shape_of((capacity, width))] * count
        if last
        else [shape_of((count * capacity, width), jnp.float32)]
    )
    extra = [] if carried is None else [carried]
    return call(
        body,
        outs,
        [VMEM] * (count + len(flat) + len(extra)),
        flops=6 * count * capacity * width * hidden,
    )(*rows_in, *flat, *extra)


def pair_sum(place, kept, received):
    share = kept.shape[0] // 2

    def body(place_ref, kept_ref, received_ref, outer_ref, inner_ref):
        mine = place_ref[3]
        for out, half in ((outer_ref, 1 - mine), (inner_ref, mine)):
            some = pl.ds(pl.multiple_of(half * share, share), share)
            out[...] = (kept_ref[some, :] + received_ref[some, :].astype(jnp.float32)).astype(out.dtype)

    outs = [shape_of((share, kept.shape[1])), shape_of((share, kept.shape[1]), jnp.float32)]
    return call(body, outs, [SMEM, VMEM, VMEM])(place, kept, received)


def finish(inner, received, gain):
    def body(inner_ref, received_ref, gain_ref, out_ref):
        projected = inner_ref[...] + received_ref[...].astype(jnp.float32)
        out_ref[...] = norm_rows(projected, gain_ref[...]).astype(jnp.bfloat16)

    return call(body, shape_of(inner.shape), [VMEM] * 3)(inner, received, gain.reshape(1, -1))


def attend_project(place, queries, own, passed, out_weight, heads, quarters):
    span, width_heads = queries.shape
    size = width_heads // heads
    pair = 2 * size
    width = out_weight.shape[1]
    share = span // quarters
    blocks = 1 + len(passed)
    half = quarters // 2

    def body(place_ref, q_ref, own_ref, *refs):
        kv_refs = (own_ref,) + refs[: len(passed)]
        weight_ref, send_ref, keep_ref, acc, carry, att, proj = refs[len(passed) :]
        row = lax.broadcasted_iota(jnp.int32, (span, span), 0)
        column = lax.broadcasted_iota(jnp.int32, (span, span), 1)
        earlier = column < row
        after = jnp.where(row > column, 1.0, 0.0)
        sums = jnp.concatenate([after, jnp.ones((span, span), jnp.float32)], axis=1)
        sums = jnp.concatenate([sums, sums], axis=0).astype(jnp.bfloat16)
        low = lax.broadcasted_iota(jnp.int32, (span, pair), 1) < size

        def one_block(d):
            for h in range(heads):
                lanes = slice((h // 2) * pair, (h // 2 + 1) * pair)
                query = jnp.where(low if h % 2 == 0 else ~low, q_ref[:, lanes], 0.0).astype(jnp.bfloat16)
                key = kv_refs[d][:span, lanes]
                bias = kv_refs[d][span + h : span + h + 1, :span].astype(jnp.float32)
                z = lax.dot_general(
                    query, key, (((1,), (1,)), ((), ())), preferred_element_type=jnp.float32
                ) * size ** (-0.5) + bias
                rest = -(jnp.maximum(z, 0.0) + jnp.log1p(jnp.exp(-jnp.abs(z))))
                masked = jnp.where(earlier, rest, 0.0) if d == 0 else rest
                top = masked.astype(jnp.bfloat16)
                bottom = (masked - top.astype(jnp.float32)).astype(jnp.bfloat16)
                both = jnp.dot(
                    jnp.concatenate([top, bottom], axis=1), sums, preferred_element_type=jnp.float32
                )
                local = jnp.exp(z + rest + both[:, :span])
                if d == 0:
                    local = jnp.where(earlier, local, 0.0)
                value = kv_refs[d][:span, width_heads + lanes.start : width_heads + lanes.stop]
                part = jnp.dot(local.astype(jnp.bfloat16), value, preferred_element_type=jnp.float32)
                if d == 0:
                    carry[h] = both[:, span:]
                    total = part
                else:
                    before = carry[h]
                    total = jnp.exp(before) * part
                    carry[h] = before + both[:, span:]
                mine = low if h % 2 == 0 else ~low
                if d == 0 and h % 2 == 0:
                    acc[h // 2] = total
                elif d == 0:
                    acc[h // 2] = jnp.where(mine, total, acc[h // 2])
                else:
                    acc[h // 2] = acc[h // 2] + jnp.where(mine, total, 0.0)

        one_block(0)
        for d in range(1, blocks):
            pl.when(place_ref[0] >= d)(lambda d=d: one_block(d))
        for p in range(heads // 2):
            att[:, p * pair : (p + 1) * pair] = acc[p].astype(jnp.bfloat16)
        proj[...] = jnp.dot(att[...], weight_ref[...], preferred_element_type=jnp.float32)
        core = place_ref[1]
        for k in range(half):
            send_ref[k * share : (k + 1) * share, :] = proj[
                pl.ds((2 * k + 1 - core) * share, share), :
            ].astype(jnp.bfloat16)
            keep_ref[k * share : (k + 1) * share, :] = proj[pl.ds((2 * k + core) * share, share), :]

    return call(
        body,
        [shape_of((half * share, width)), shape_of((half * share, width), jnp.float32)],
        [SMEM, VMEM, VMEM] + [VMEM] * len(passed) + [VMEM],
        scratch=(
            pltpu.VMEM((heads // 2, span, pair), jnp.float32),
            pltpu.VMEM((heads, span, span), jnp.float32),
            pltpu.VMEM((span, width_heads), jnp.bfloat16),
            pltpu.VMEM((span, width), jnp.float32),
        ),
        flops=4 * blocks * span * span * width_heads + 2 * span * width_heads * width,
    )(place, queries, own, *passed, out_weight)


def per_device(*arrays):
    return paired_step(*arrays)


def paired_step(
    queries,
    keys,
    values,
    stop_bias,
    out_weight,
    mix_gain,
    moe_input,
    ffn_gain,
    expert_ids,
    expert_scores,
    gate_weight,
    up_weight,
    down_weight,
):
    blocks = lax.axis_size("ep")
    shards = lax.axis_size("tp")
    group = lax.axis_index("grp")
    block = lax.axis_index("ep")
    shard = lax.axis_index("tp")
    place = jnp.stack([block, shard % 2, group, shard // 2]).astype(jnp.int32)
    heads = stop_bias.shape[1]

    def core(array):
        return lax.ppermute(array, "tp", [(i, i ^ 1) for i in range(shards)])

    def across(array):
        return lax.ppermute(array, "tp", [(i, i ^ 2) for i in range(shards)])

    def beside(array):
        return lax.ppermute(array, "grp", [(0, 1), (1, 0)])

    def turn(array, d):
        return lax.ppermute(array, "ep", [(i, (i + d) % blocks) for i in range(blocks)])

    def upward(array, d):
        return lax.ppermute(array, "ep", [(i, i + 1) for i in range(d - 1, blocks - 1)])

    rows, top = expert_ids.shape
    capacity = 3 * rows * top // (2 * blocks)
    mine = (gate_weight[0], up_weight[0], down_weight[0])
    prepared = prepare(
        place, moe_input, ffn_gain, expert_ids.T, keys, values, stop_bias.T, mine, blocks, capacity
    )
    outbound, own, halves = prepared[:blocks], prepared[blocks], prepared[blocks + 1 :]

    arrived = [outbound[0]] + [turn(outbound[d], d) for d in range(1, blocks)]

    far = tuple(across(array) for array in halves)
    near = tuple(core(array) for array in mine)
    other = tuple(beside(array) for array in far)
    far_near = tuple(core(array) for array in far)
    other_near = tuple(core(array) for array in other)

    passed = []
    for d in range(1, blocks):
        passed.append(upward(passed[-1] if passed else own, d))

    def whole(arrays):
        return [[array] for array in arrays]

    def chunked(arrays):
        return [arrays[0:2], arrays[2:4], arrays[4:6]]

    summed = expert_part(arrived, [whole(mine), whole(near)], None, False)[0]
    summed = expert_part(arrived, [chunked(far), chunked(far_near)], summed, False)[0]
    produced = expert_part(arrived, [chunked(other), chunked(other_near)], summed, True)
    returned = [produced[0]] + [turn(produced[d], -d) for d in range(1, blocks)]

    send, kept = attend_project(place, queries, own, passed, out_weight, heads, shards)
    outer, inner = pair_sum(place, kept, core(send))
    mixed = finish(inner, across(outer), mix_gain)
    experts_mixed = combine_rows(place, expert_ids.T, expert_scores.T, returned)
    return (mixed, experts_mixed)


def solution(mesh):
    sizes = mesh.shape
    paired = sizes["grp"] == 2 and sizes["tp"] == 4 and sizes["ep"] <= sizes["tp"]
    return jax.shard_map(
        per_device if paired else per_device_wide,
        mesh=mesh,
        in_specs=(
            P(("grp", "ep"), "tp"),
            P(("grp", "ep"), "tp"),
            P(("grp", "ep"), "tp"),
            P(("grp", "ep"), "tp"),
            P("tp", None),
            P(),
            P(("grp", "ep", "tp"), None),
            P(),
            P(("grp", "ep", "tp"), None),
            P(("grp", "ep", "tp"), None),
            P("ep", None, "tp"),
            P("ep", None, "tp"),
            P("ep", "tp", None),
        ),
        out_specs=(P(("grp", "ep", "tp"), None), P(("grp", "ep", "tp"), None)),
        check_vma=False,
    )
```

```python
import jax
import jax.numpy as jnp
from jax import lax
from jax.experimental import pallas as pl
from jax.experimental.pallas import tpu as pltpu
from jax.sharding import PartitionSpec as P


def norm_rows(values, gain):
    values = values.astype(jnp.float32)
    scale = lax.rsqrt(jnp.mean(values * values, axis=-1, keepdims=True) + 1e-06)
    return values * scale * gain


def break_terms(query_heads, query_place, key_block, bias_block, first):
    span = key_block.shape[0]
    heads = query_heads.shape[1]
    key_heads = key_block.reshape(span, heads, -1)
    scores = jnp.einsum("qhd,khd->hqk", query_heads, key_heads, preferred_element_type=jnp.float32)
    scores = scores * query_heads.shape[2] ** (-0.5) + bias_block.astype(jnp.float32).T[:, None, :]
    key_place = first + jnp.arange(span)
    past = (key_place[None, :] < query_place[:, None])[None]
    rest = jnp.where(past, jax.nn.log_sigmoid(-scores), 0.0)
    later = lax.cumsum(rest, axis=2, reverse=True)
    return (scores, past, rest, later)


def block_part(scores, past, rest, later, value_block, heads):
    within = later - rest
    local = jnp.where(past, jnp.exp(jax.nn.log_sigmoid(scores) + within), 0.0).astype(jnp.bfloat16)
    span = value_block.shape[0]
    value_heads = value_block.reshape(span, heads, -1)
    part = jnp.einsum("hqk,khd->qhd", local, value_heads, preferred_element_type=jnp.float32)
    return part.reshape(part.shape[0], -1)


def keep(state):
    return state


def dispatch_plan(normed, expert_ids, experts, capacity):
    rows, top = expert_ids.shape
    flat_ids = expert_ids.reshape(rows * top)
    onehot = (flat_ids[:, None] == jnp.arange(experts)[None, :]).astype(jnp.int32)
    earlier = jnp.cumsum(onehot, axis=0) - onehot
    place = jnp.sum(earlier * onehot, axis=1)
    target = flat_ids * capacity + place
    source = (
        jnp.zeros((experts * capacity,), jnp.int32)
        .at[target]
        .set(jnp.arange(rows * top, dtype=jnp.int32) // top + 1)
    )
    padded = jnp.concatenate([jnp.zeros((1, normed.shape[1]), normed.dtype), normed], axis=0)
    return (padded[source].reshape(experts, capacity, normed.shape[1]), target)


def expert_hidden(piece, gate_weight, up_weight):
    flat = piece.reshape(-1, piece.shape[-1])
    gate = jnp.dot(flat, gate_weight[0], preferred_element_type=jnp.float32)
    upward = jnp.dot(flat, up_weight[0], preferred_element_type=jnp.float32)
    hidden = (jax.nn.silu(gate) * upward).astype(jnp.bfloat16)
    return hidden.reshape(piece.shape[0], piece.shape[1], -1)


def send_back(summed):
    return lax.all_to_all(
        summed.astype(jnp.bfloat16), "ep", split_axis=0, concat_axis=0, tiled=True
    )


def return_rows(hidden_all, down_weight, sources):
    flat = hidden_all.reshape(-1, hidden_all.shape[2])
    product = jnp.dot(flat, down_weight[0], preferred_element_type=jnp.float32)
    return send_back(
        lax.psum_scatter(
            product.reshape(sources * lax.axis_size("tp"), hidden_all.shape[1], -1).astype(
                jnp.bfloat16
            ),
            "tp",
            scatter_dimension=0,
            tiled=True,
        ).astype(jnp.float32)
    )


def per_device_wide(
    queries,
    keys,
    values,
    stop_bias,
    out_weight,
    mix_gain,
    moe_input,
    ffn_gain,
    expert_ids,
    expert_scores,
    gate_weight,
    up_weight,
    down_weight,
):
    span = queries.shape[0]
    heads = stop_bias.shape[1]
    width_heads = queries.shape[1]
    blocks = lax.axis_size("ep")
    own_first = lax.axis_index("ep") * span
    query_heads = queries.reshape(span, heads, -1)
    query_place = own_first + jnp.arange(span)

    def piece_rows(piece, index):
        return tuple((lax.dynamic_slice_in_dim(member, index * span, span, 0) for member in piece))

    start_state = (
        jnp.zeros((blocks, heads, span), jnp.float32),
        jnp.zeros((blocks, span, width_heads), jnp.float32),
    )
    piece = (
        lax.all_gather(keys, "ep", axis=0, tiled=True),
        lax.all_gather(values, "ep", axis=0, tiled=True),
        lax.all_gather(stop_bias, "ep", axis=0, tiled=True),
    )

    def one_block(index, state):
        key_block, value_block, bias_block = piece_rows(piece, index)
        first = index * span

        def compute(inner_state):
            totals, parts = inner_state
            scores, past, rest, later = break_terms(
                query_heads, query_place, key_block, bias_block, first
            )
            part = block_part(scores, past, rest, later, value_block, heads)
            number = first // span
            totals = lax.dynamic_update_index_in_dim(totals, later[:, :, 0], number, 0)
            parts = lax.dynamic_update_index_in_dim(parts, part, number, 0)
            return (totals, parts)

        return lax.cond(first <= own_first, compute, keep, state)

    totals, parts = lax.fori_loop(0, piece[0].shape[0] // span, one_block, start_state)
    carried = lax.cumsum(totals, axis=0, reverse=True) - totals
    factor = jnp.exp(carried).transpose(0, 2, 1)[:, :, :, None]
    attended = jnp.sum(factor * parts.reshape(blocks, span, heads, -1), axis=0).reshape(
        span, width_heads
    )
    attended = attended.astype(jnp.bfloat16)
    projected = lax.psum_scatter(
        jnp.dot(attended, out_weight, preferred_element_type=jnp.float32).astype(jnp.bfloat16),
        "tp",
        scatter_dimension=0,
        tiled=True,
    ).astype(jnp.float32)
    mixed = norm_rows(projected, mix_gain).astype(jnp.bfloat16)
    normed = norm_rows(moe_input, ffn_gain).astype(jnp.bfloat16)
    rows, top = expert_ids.shape
    experts = lax.axis_size("ep")
    capacity = 3 * rows * top // (2 * experts)
    weights = expert_scores / jnp.sum(expert_scores, axis=1, keepdims=True)
    outbound, target = dispatch_plan(normed, expert_ids, experts, capacity)
    arrived = lax.all_to_all(outbound, "ep", split_axis=0, concat_axis=0, tiled=True)
    hidden_all = expert_hidden(
        lax.all_gather(arrived, "tp", axis=0, tiled=True), gate_weight, up_weight
    )
    returned = return_rows(hidden_all, down_weight, arrived.shape[0])
    picked = returned.reshape(experts * capacity, -1)[target].reshape(rows, top, -1)
    experts_mixed = jnp.sum(picked.astype(jnp.float32) * weights[:, :, None], axis=1).astype(
        jnp.bfloat16
    )
    return (mixed, experts_mixed)


VMEM = pl.BlockSpec(memory_space=pltpu.VMEM)
SMEM = pl.BlockSpec(memory_space=pltpu.SMEM)
HBM = pl.BlockSpec(memory_space=pltpu.HBM)


def shape_of(shape, dtype=jnp.bfloat16):
    return jax.ShapeDtypeStruct(shape, dtype)


def call(body, outs, ins, scratch=(), flops=0, limit=24):
    return pl.pallas_call(
        body,
        out_shape=outs,
        in_specs=ins,
        out_specs=jax.tree.map(lambda _: VMEM, outs),
        scratch_shapes=scratch,
        compiler_params=pltpu.CompilerParams(vmem_limit_bytes=limit * 1024 * 1024),
        cost_estimate=pl.CostEstimate(flops=flops, transcendentals=0, bytes_accessed=0),
    )


def selections(place_ref, ids_ref, experts, capacity):
    top, rows = ids_ref.shape
    distance = lax.broadcasted_iota(jnp.int32, (8, rows), 0)
    expert = (place_ref[0] + distance) % experts
    hits = [ids_ref[k : k + 1, :] == expert for k in range(top)]
    chosen = jnp.zeros((8, rows), jnp.float32)
    for hit in hits:
        chosen = chosen + jnp.where(hit & (distance < experts), 1.0, 0.0)
    below = lax.broadcasted_iota(jnp.int32, (rows, rows), 0) < lax.broadcasted_iota(
        jnp.int32, (rows, rows), 1
    )
    rank = jnp.dot(
        chosen.astype(jnp.bfloat16),
        jnp.where(below, 1.0, 0.0).astype(jnp.bfloat16),
        preferred_element_type=jnp.float32,
    )
    slot = lax.broadcasted_iota(jnp.int32, (capacity, rows), 0).astype(jnp.float32)
    picks = []
    for d in range(experts):
        pick = (rank[d : d + 1, :] == slot) & (chosen[d : d + 1, :] > 0.5)
        picks.append(jnp.where(pick, 1.0, 0.0).astype(jnp.bfloat16))
    return hits, picks


def prepare(place, moe_input, ffn_gain, ids, keys, values, bias, weights, experts, capacity):
    rows, width = moe_input.shape
    span, heads_width = keys.shape
    heads = bias.shape[0]
    gate, upward, down = weights
    part = gate.shape[1] // 2
    deep = gate.shape[0] // 2
    thin = part // 2

    def body(place_ref, gain_hbm, ids_hbm, bias_hbm, input_hbm, keys_hbm, values_hbm, *refs):
        gate_hbm, up_hbm, down_hbm = refs[:3]
        outs = refs[3 : 3 + experts]
        own_ref, gate_a, gate_b, up_a, up_b, down_a, down_b = refs[3 + experts : 10 + experts]
        input_v, gain_v, ids_v, bias_v, sems = refs[10 + experts :]
        begin = pl.multiple_of(place_ref[2] * part, part)
        columns = pl.ds(begin, part)
        moves = [
            (ids_hbm, ids_v),
            (input_hbm, input_v),
            (gain_hbm, gain_v),
            (bias_hbm, bias_v),
            (gate_hbm.at[pl.ds(0, deep), columns], gate_a),
            (gate_hbm.at[pl.ds(deep, deep), columns], gate_b),
            (keys_hbm, own_ref.at[pl.ds(0, span), pl.ds(0, heads_width)]),
            (values_hbm, own_ref.at[pl.ds(0, span), pl.ds(heads_width, heads_width)]),
            (up_hbm.at[pl.ds(0, deep), columns], up_a),
            (up_hbm.at[pl.ds(deep, deep), columns], up_b),
            (down_hbm.at[pl.ds(begin, thin), :], down_a),
            (down_hbm.at[pl.ds(pl.multiple_of(begin + thin, thin), thin), :], down_b),
        ]
        copies = [
            pltpu.make_async_copy(source, target, sems.at[k])
            for k, (source, target) in enumerate(moves)
        ]
        for copy in copies:
            copy.start()
        own_ref[span:, :] = jnp.zeros((heads, 2 * heads_width), jnp.bfloat16)
        copies[0].wait()
        _, picks = selections(place_ref, ids_v, experts, capacity)
        copies[1].wait()
        copies[2].wait()
        normed = norm_rows(input_v[...], gain_v[...]).astype(jnp.bfloat16)
        for d in range(experts):
            outs[d][...] = jnp.dot(
                picks[d], normed, preferred_element_type=jnp.float32
            ).astype(jnp.bfloat16)
        copies[3].wait()
        own_ref[span:, :span] = bias_v[...]
        for copy in copies[4:]:
            copy.wait()

    outs = [shape_of((capacity, width))] * experts + [
        shape_of((span + heads, 2 * heads_width)),
        shape_of((deep, part)),
        shape_of((deep, part)),
        shape_of((deep, part)),
        shape_of((deep, part)),
        shape_of((thin, width)),
        shape_of((thin, width)),
    ]
    return call(
        body,
        outs,
        [SMEM] + [HBM] * 9,
        scratch=(
            pltpu.VMEM((rows, width), jnp.bfloat16),
            pltpu.VMEM((1, width), jnp.float32),
            pltpu.VMEM(ids.shape, jnp.int32),
            pltpu.VMEM(bias.shape, jnp.bfloat16),
            pltpu.SemaphoreType.DMA((12,)),
        ),
        flops=2 * experts * capacity * rows * width,
    )(
        place,
        *(
            pltpu.with_memory_space_constraint(array, pltpu.HBM)
            for array in (
                ffn_gain.reshape(1, width),
                ids,
                bias,
                moe_input,
                keys,
                values,
                gate,
                upward,
                down,
            )
        ),
    )


def combine_rows(place, ids, scores, returned):
    rows = ids.shape[1]
    experts = len(returned)
    capacity, width = returned[0].shape

    def body(place_ref, ids_ref, scores_ref, *refs):
        hits, picks = selections(place_ref, ids_ref, experts, capacity)
        shares = scores_ref[...]
        shares = shares / jnp.sum(shares, axis=0, keepdims=True)
        weight = jnp.zeros((8, rows), jnp.float32)
        for k, hit in enumerate(hits):
            weight = weight + jnp.where(hit, shares[k : k + 1, :], 0.0)
        weight = weight.T
        total = jnp.zeros((rows, width), jnp.float32)
        for d in range(experts):
            total = total + weight[:, d : d + 1] * lax.dot_general(
                picks[d], refs[d][...], (((0,), (0,)), ((), ())), preferred_element_type=jnp.float32
            )
        refs[-1][...] = total.astype(jnp.bfloat16)

    return call(
        body, shape_of((rows, width)), [SMEM, VMEM, VMEM] + [VMEM] * experts,
        flops=2 * experts * capacity * rows * width,
    )(place, ids, scores, *returned)


def expert_part(rows_in, pieces, carried, last):
    capacity, width = rows_in[0].shape
    count = len(rows_in)
    hidden = sum(piece[0][0].shape[1] for piece in pieces)
    flat = [array for piece in pieces for kind in piece for array in kind]

    def body(*refs):
        row_refs = refs[:count]
        weight_refs = refs[count : count + len(flat)]
        rest = refs[count + len(flat) :]
        if carried is not None:
            acc_ref, rest = rest[0], rest[1:]
        rows = jnp.concatenate([ref[...] for ref in row_refs], axis=0)
        inner, down = [], []
        at = 0
        for piece in pieces:
            kinds = []
            for kind in piece:
                chunk = [ref[...] for ref in weight_refs[at : at + len(kind)]]
                kinds.append(chunk[0] if len(chunk) == 1 else jnp.concatenate(chunk, axis=0))
                at += len(kind)
            size = kinds[0].shape[1]
            both = jnp.concatenate(kinds[:2], axis=1)
            down.append(kinds[2])
            product = jnp.dot(rows, both, preferred_element_type=jnp.float32)
            gate, upward = product[:, :size], product[:, size:]
            inner.append((gate / (1.0 + jnp.exp(-gate)) * upward).astype(jnp.bfloat16))
        inner = jnp.concatenate(inner, axis=1)
        down = jnp.concatenate(down, axis=0)
        if last:
            for d in range(count):
                some = slice(d * capacity, (d + 1) * capacity)
                out = jnp.dot(inner[some], down, preferred_element_type=jnp.float32)
                if carried is not None:
                    out = out + acc_ref[some]
                rest[d][...] = out.astype(jnp.bfloat16)
        else:
            out = jnp.dot(inner, down, preferred_element_type=jnp.float32)
            rest[0][...] = out if carried is None else out + acc_ref[...]

    outs = (
        [shape_of((capacity, width))] * count
        if last
        else [shape_of((count * capacity, width), jnp.float32)]
    )
    extra = [] if carried is None else [carried]
    return call(
        body,
        outs,
        [VMEM] * (count + len(flat) + len(extra)),
        flops=6 * count * capacity * width * hidden,
    )(*rows_in, *flat, *extra)


def pair_sum(place, kept, received):
    share = kept.shape[0] // 2

    def body(place_ref, kept_ref, received_ref, outer_ref, inner_ref):
        mine = place_ref[3]
        for out, half in ((outer_ref, 1 - mine), (inner_ref, mine)):
            some = pl.ds(pl.multiple_of(half * share, share), share)
            out[...] = (kept_ref[some, :] + received_ref[some, :].astype(jnp.float32)).astype(out.dtype)

    outs = [shape_of((share, kept.shape[1])), shape_of((share, kept.shape[1]), jnp.float32)]
    return call(body, outs, [SMEM, VMEM, VMEM])(place, kept, received)


def finish(inner, received, gain):
    def body(inner_ref, received_ref, gain_ref, out_ref):
        projected = inner_ref[...] + received_ref[...].astype(jnp.float32)
        out_ref[...] = norm_rows(projected, gain_ref[...]).astype(jnp.bfloat16)

    return call(body, shape_of(inner.shape), [VMEM] * 3)(inner, received, gain.reshape(1, -1))


def attend_project(place, queries, own, passed, out_weight, heads, quarters):
    span, width_heads = queries.shape
    size = width_heads // heads
    pair = 2 * size
    width = out_weight.shape[1]
    share = span // quarters
    blocks = len(passed)
    half = quarters // 2

    def body(place_ref, q_ref, own_ref, *refs):
        first_ref, direct_ref, relay_ref, last_ref = refs[:blocks]
        weight_ref, send_ref, keep_ref, acc, carry, att, proj, middle = refs[blocks:]
        kv_refs = (own_ref, first_ref, middle, last_ref)

        @pl.when(place_ref[0] == 2)
        def _():
            middle[...] = direct_ref[...]

        @pl.when(place_ref[0] == 3)
        def _():
            middle[...] = relay_ref[...]

        row = lax.broadcasted_iota(jnp.int32, (span, span), 0)
        column = lax.broadcasted_iota(jnp.int32, (span, span), 1)
        earlier = column < row
        after = jnp.where(row > column, 1.0, 0.0)
        sums = jnp.concatenate([after, jnp.ones((span, span), jnp.float32)], axis=1)
        sums = jnp.concatenate([sums, sums], axis=0).astype(jnp.bfloat16)
        low = lax.broadcasted_iota(jnp.int32, (span, pair), 1) < size

        def one_block(d):
            for h in range(heads):
                lanes = slice((h // 2) * pair, (h // 2 + 1) * pair)
                query = jnp.where(low if h % 2 == 0 else ~low, q_ref[:, lanes], 0.0).astype(jnp.bfloat16)
                key = kv_refs[d][:span, lanes]
                bias = kv_refs[d][span + h : span + h + 1, :span].astype(jnp.float32)
                z = lax.dot_general(
                    query, key, (((1,), (1,)), ((), ())), preferred_element_type=jnp.float32
                ) * size ** (-0.5) + bias
                rest = -(jnp.maximum(z, 0.0) + jnp.log1p(jnp.exp(-jnp.abs(z))))
                masked = jnp.where(earlier, rest, 0.0) if d == 0 else rest
                top = masked.astype(jnp.bfloat16)
                bottom = (masked - top.astype(jnp.float32)).astype(jnp.bfloat16)
                both = jnp.dot(
                    jnp.concatenate([top, bottom], axis=1), sums, preferred_element_type=jnp.float32
                )
                local = jnp.exp(z + rest + both[:, :span])
                if d == 0:
                    local = jnp.where(earlier, local, 0.0)
                value = kv_refs[d][:span, width_heads + lanes.start : width_heads + lanes.stop]
                part = jnp.dot(local.astype(jnp.bfloat16), value, preferred_element_type=jnp.float32)
                if d == 0:
                    carry[h] = both[:, span:]
                    total = part
                else:
                    before = carry[h]
                    total = jnp.exp(before) * part
                    carry[h] = before + both[:, span:]
                mine = low if h % 2 == 0 else ~low
                if d == 0 and h % 2 == 0:
                    acc[h // 2] = total
                elif d == 0:
                    acc[h // 2] = jnp.where(mine, total, acc[h // 2])
                else:
                    acc[h // 2] = acc[h // 2] + jnp.where(mine, total, 0.0)

        one_block(0)
        for d in range(1, blocks):
            pl.when(place_ref[0] >= d)(lambda d=d: one_block(d))
        for p in range(heads // 2):
            att[:, p * pair : (p + 1) * pair] = acc[p].astype(jnp.bfloat16)
        proj[...] = jnp.dot(att[...], weight_ref[...], preferred_element_type=jnp.float32)
        core = place_ref[1]
        for k in range(half):
            send_ref[k * share : (k + 1) * share, :] = proj[
                pl.ds((2 * k + 1 - core) * share, share), :
            ].astype(jnp.bfloat16)
            keep_ref[k * share : (k + 1) * share, :] = proj[pl.ds((2 * k + core) * share, share), :]

    return call(
        body,
        [shape_of((half * share, width)), shape_of((half * share, width), jnp.float32)],
        [SMEM, VMEM, VMEM] + [VMEM] * len(passed) + [VMEM],
        scratch=(
            pltpu.VMEM((heads // 2, span, pair), jnp.float32),
            pltpu.VMEM((heads, span, span), jnp.float32),
            pltpu.VMEM((span, width_heads), jnp.bfloat16),
            pltpu.VMEM((span, width), jnp.float32),
            pltpu.VMEM(own.shape, jnp.bfloat16),
        ),
        flops=4 * blocks * span * span * width_heads + 2 * span * width_heads * width,
    )(place, queries, own, *passed, out_weight)


def per_device(*arrays):
    return paired_step(*arrays)


def paired_step(
    queries,
    keys,
    values,
    stop_bias,
    out_weight,
    mix_gain,
    moe_input,
    ffn_gain,
    expert_ids,
    expert_scores,
    gate_weight,
    up_weight,
    down_weight,
):
    blocks = lax.axis_size("ep")
    shards = lax.axis_size("tp")
    group = lax.axis_index("grp")
    block = lax.axis_index("ep")
    shard = lax.axis_index("tp")
    place = jnp.stack([block, shard % 2, group, shard // 2]).astype(jnp.int32)
    heads = stop_bias.shape[1]

    def core(array):
        return lax.ppermute(array, "tp", [(i, i ^ 1) for i in range(shards)])

    def across(array):
        return lax.ppermute(array, "tp", [(i, i ^ 2) for i in range(shards)])

    def beside(array):
        return lax.ppermute(array, "grp", [(0, 1), (1, 0)])

    def turn(array, d):
        return lax.ppermute(array, "ep", [(i, (i + d) % blocks) for i in range(blocks)])

    def upward(array, d):
        return lax.ppermute(array, "ep", [(i, i + d) for i in range(blocks - d)])

    rows, top = expert_ids.shape
    capacity = 3 * rows * top // (2 * blocks)
    mine = (gate_weight[0], up_weight[0], down_weight[0])
    prepared = prepare(
        place, moe_input, ffn_gain, expert_ids.T, keys, values, stop_bias.T, mine, blocks, capacity
    )
    outbound, own, halves = prepared[:blocks], prepared[blocks], prepared[blocks + 1 :]

    arrived = [outbound[0]] + [turn(outbound[d], d) for d in range(1, blocks)]

    far = tuple(across(array) for array in halves)
    near = tuple(core(array) for array in mine)
    other = tuple(beside(array) for array in far)
    far_near = tuple(core(array) for array in far)
    other_near = tuple(core(array) for array in other)

    passed = [upward(own, 1), lax.ppermute(own, "ep", [(0, 2)])]
    passed += [lax.ppermute(array, "ep", [(2, 3)]) for array in passed]

    def whole(arrays):
        return [[array] for array in arrays]

    def chunked(arrays):
        return [arrays[0:2], arrays[2:4], arrays[4:6]]

    early = [k for k in range(blocks) if k % 2 == 0]
    late = [k for k in range(blocks) if k % 2 == 1]
    pieces = [
        [whole(mine), whole(near)],
        [chunked(far), chunked(far_near)],
        [chunked(other), chunked(other_near)],
    ]
    head = [arrived[k] for k in early]
    summed = expert_part(head, pieces[0], None, False)[0]
    summed = expert_part(head, pieces[1], summed, False)[0]
    done = expert_part(head, pieces[2], summed, True)
    done += expert_part([arrived[k] for k in late], pieces[0] + pieces[1] + pieces[2], None, True)
    produced = [done[(early + late).index(k)] for k in range(blocks)]
    returned = [produced[0]] + [turn(produced[d], -d) for d in range(1, blocks)]

    send, kept = attend_project(place, queries, own, passed, out_weight, heads, shards)
    outer, inner = pair_sum(place, kept, core(send))
    mixed = finish(inner, across(outer), mix_gain)
    experts_mixed = combine_rows(place, expert_ids.T, expert_scores.T, returned)
    return (mixed, experts_mixed)


def solution(mesh):
    sizes = mesh.shape
    paired = sizes["grp"] == 2 and sizes["tp"] == 4 and sizes["ep"] == sizes["tp"]
    return jax.shard_map(
        per_device if paired else per_device_wide,
        mesh=mesh,
        in_specs=(
            P(("grp", "ep"), "tp"),
            P(("grp", "ep"), "tp"),
            P(("grp", "ep"), "tp"),
            P(("grp", "ep"), "tp"),
            P("tp", None),
            P(),
            P(("grp", "ep", "tp"), None),
            P(),
            P(("grp", "ep", "tp"), None),
            P(("grp", "ep", "tp"), None),
            P("ep", None, "tp"),
            P("ep", None, "tp"),
            P("ep", "tp", None),
        ),
        out_specs=(P(("grp", "ep", "tp"), None), P(("grp", "ep", "tp"), None)),
        check_vma=False,
    )
```

```python
import jax
import jax.numpy as jnp
from jax import lax
from jax.experimental import pallas as pl
from jax.experimental.pallas import tpu as pltpu
from jax.sharding import PartitionSpec as P


def norm_rows(values, gain):
    values = values.astype(jnp.float32)
    scale = lax.rsqrt(jnp.mean(values * values, axis=-1, keepdims=True) + 1e-06)
    return values * scale * gain


def break_terms(query_heads, query_place, key_block, bias_block, first):
    span = key_block.shape[0]
    heads = query_heads.shape[1]
    key_heads = key_block.reshape(span, heads, -1)
    scores = jnp.einsum("qhd,khd->hqk", query_heads, key_heads, preferred_element_type=jnp.float32)
    scores = scores * query_heads.shape[2] ** (-0.5) + bias_block.astype(jnp.float32).T[:, None, :]
    key_place = first + jnp.arange(span)
    past = (key_place[None, :] < query_place[:, None])[None]
    rest = jnp.where(past, jax.nn.log_sigmoid(-scores), 0.0)
    later = lax.cumsum(rest, axis=2, reverse=True)
    return (scores, past, rest, later)


def block_part(scores, past, rest, later, value_block, heads):
    within = later - rest
    local = jnp.where(past, jnp.exp(jax.nn.log_sigmoid(scores) + within), 0.0).astype(jnp.bfloat16)
    span = value_block.shape[0]
    value_heads = value_block.reshape(span, heads, -1)
    part = jnp.einsum("hqk,khd->qhd", local, value_heads, preferred_element_type=jnp.float32)
    return part.reshape(part.shape[0], -1)


def keep(state):
    return state


def dispatch_plan(normed, expert_ids, experts, capacity):
    rows, top = expert_ids.shape
    flat_ids = expert_ids.reshape(rows * top)
    onehot = (flat_ids[:, None] == jnp.arange(experts)[None, :]).astype(jnp.int32)
    earlier = jnp.cumsum(onehot, axis=0) - onehot
    place = jnp.sum(earlier * onehot, axis=1)
    target = flat_ids * capacity + place
    source = (
        jnp.zeros((experts * capacity,), jnp.int32)
        .at[target]
        .set(jnp.arange(rows * top, dtype=jnp.int32) // top + 1)
    )
    padded = jnp.concatenate([jnp.zeros((1, normed.shape[1]), normed.dtype), normed], axis=0)
    return (padded[source].reshape(experts, capacity, normed.shape[1]), target)


def expert_hidden(piece, gate_weight, up_weight):
    flat = piece.reshape(-1, piece.shape[-1])
    gate = jnp.dot(flat, gate_weight[0], preferred_element_type=jnp.float32)
    upward = jnp.dot(flat, up_weight[0], preferred_element_type=jnp.float32)
    hidden = (jax.nn.silu(gate) * upward).astype(jnp.bfloat16)
    return hidden.reshape(piece.shape[0], piece.shape[1], -1)


def send_back(summed):
    return lax.all_to_all(
        summed.astype(jnp.bfloat16), "ep", split_axis=0, concat_axis=0, tiled=True
    )


def return_rows(hidden_all, down_weight, sources):
    flat = hidden_all.reshape(-1, hidden_all.shape[2])
    product = jnp.dot(flat, down_weight[0], preferred_element_type=jnp.float32)
    return send_back(
        lax.psum_scatter(
            product.reshape(sources * lax.axis_size("tp"), hidden_all.shape[1], -1).astype(
                jnp.bfloat16
            ),
            "tp",
            scatter_dimension=0,
            tiled=True,
        ).astype(jnp.float32)
    )


def per_device_wide(
    queries,
    keys,
    values,
    stop_bias,
    out_weight,
    mix_gain,
    moe_input,
    ffn_gain,
    expert_ids,
    expert_scores,
    gate_weight,
    up_weight,
    down_weight,
):
    span = queries.shape[0]
    heads = stop_bias.shape[1]
    width_heads = queries.shape[1]
    blocks = lax.axis_size("ep")
    own_first = lax.axis_index("ep") * span
    query_heads = queries.reshape(span, heads, -1)
    query_place = own_first + jnp.arange(span)

    def piece_rows(piece, index):
        return tuple((lax.dynamic_slice_in_dim(member, index * span, span, 0) for member in piece))

    start_state = (
        jnp.zeros((blocks, heads, span), jnp.float32),
        jnp.zeros((blocks, span, width_heads), jnp.float32),
    )
    piece = (
        lax.all_gather(keys, "ep", axis=0, tiled=True),
        lax.all_gather(values, "ep", axis=0, tiled=True),
        lax.all_gather(stop_bias, "ep", axis=0, tiled=True),
    )

    def one_block(index, state):
        key_block, value_block, bias_block = piece_rows(piece, index)
        first = index * span

        def compute(inner_state):
            totals, parts = inner_state
            scores, past, rest, later = break_terms(
                query_heads, query_place, key_block, bias_block, first
            )
            part = block_part(scores, past, rest, later, value_block, heads)
            number = first // span
            totals = lax.dynamic_update_index_in_dim(totals, later[:, :, 0], number, 0)
            parts = lax.dynamic_update_index_in_dim(parts, part, number, 0)
            return (totals, parts)

        return lax.cond(first <= own_first, compute, keep, state)

    totals, parts = lax.fori_loop(0, piece[0].shape[0] // span, one_block, start_state)
    carried = lax.cumsum(totals, axis=0, reverse=True) - totals
    factor = jnp.exp(carried).transpose(0, 2, 1)[:, :, :, None]
    attended = jnp.sum(factor * parts.reshape(blocks, span, heads, -1), axis=0).reshape(
        span, width_heads
    )
    attended = attended.astype(jnp.bfloat16)
    projected = lax.psum_scatter(
        jnp.dot(attended, out_weight, preferred_element_type=jnp.float32).astype(jnp.bfloat16),
        "tp",
        scatter_dimension=0,
        tiled=True,
    ).astype(jnp.float32)
    mixed = norm_rows(projected, mix_gain).astype(jnp.bfloat16)
    normed = norm_rows(moe_input, ffn_gain).astype(jnp.bfloat16)
    rows, top = expert_ids.shape
    experts = lax.axis_size("ep")
    capacity = 3 * rows * top // (2 * experts)
    weights = expert_scores / jnp.sum(expert_scores, axis=1, keepdims=True)
    outbound, target = dispatch_plan(normed, expert_ids, experts, capacity)
    arrived = lax.all_to_all(outbound, "ep", split_axis=0, concat_axis=0, tiled=True)
    hidden_all = expert_hidden(
        lax.all_gather(arrived, "tp", axis=0, tiled=True), gate_weight, up_weight
    )
    returned = return_rows(hidden_all, down_weight, arrived.shape[0])
    picked = returned.reshape(experts * capacity, -1)[target].reshape(rows, top, -1)
    experts_mixed = jnp.sum(picked.astype(jnp.float32) * weights[:, :, None], axis=1).astype(
        jnp.bfloat16
    )
    return (mixed, experts_mixed)


VMEM = pl.BlockSpec(memory_space=pltpu.VMEM)
SMEM = pl.BlockSpec(memory_space=pltpu.SMEM)
HBM = pl.BlockSpec(memory_space=pltpu.HBM)


def shape_of(shape, dtype=jnp.bfloat16):
    return jax.ShapeDtypeStruct(shape, dtype)


def call(body, outs, ins, scratch=(), flops=0, limit=24):
    return pl.pallas_call(
        body,
        out_shape=outs,
        in_specs=ins,
        out_specs=jax.tree.map(lambda _: VMEM, outs),
        scratch_shapes=scratch,
        compiler_params=pltpu.CompilerParams(vmem_limit_bytes=limit * 1024 * 1024),
        cost_estimate=pl.CostEstimate(flops=flops, transcendentals=0, bytes_accessed=0),
    )


def selections(place_ref, ids_ref, experts, capacity):
    top, rows = ids_ref.shape
    distance = lax.broadcasted_iota(jnp.int32, (8, rows), 0)
    expert = (place_ref[0] + distance) % experts
    hits = [ids_ref[k : k + 1, :] == expert for k in range(top)]
    chosen = jnp.zeros((8, rows), jnp.float32)
    for hit in hits:
        chosen = chosen + jnp.where(hit & (distance < experts), 1.0, 0.0)
    below = lax.broadcasted_iota(jnp.int32, (rows, rows), 0) < lax.broadcasted_iota(
        jnp.int32, (rows, rows), 1
    )
    rank = jnp.dot(
        chosen.astype(jnp.bfloat16),
        jnp.where(below, 1.0, 0.0).astype(jnp.bfloat16),
        preferred_element_type=jnp.float32,
    )
    slot = lax.broadcasted_iota(jnp.int32, (capacity, rows), 0).astype(jnp.float32)
    picks = []
    for d in range(experts):
        pick = (rank[d : d + 1, :] == slot) & (chosen[d : d + 1, :] > 0.5)
        picks.append(jnp.where(pick, 1.0, 0.0).astype(jnp.bfloat16))
    return hits, picks


def prepare(place, moe_input, ffn_gain, ids, keys, values, bias, weights, experts, capacity):
    rows, width = moe_input.shape
    span, heads_width = keys.shape
    heads = bias.shape[0]
    gate, upward, down = weights
    part = gate.shape[1] // 2
    deep = gate.shape[0] // 2
    thin = part // 2
    slim = part // 4

    def body(place_ref, gain_hbm, ids_hbm, bias_hbm, input_hbm, keys_hbm, values_hbm, *refs):
        gate_hbm, up_hbm, down_hbm = refs[:3]
        outs = refs[3 : 3 + experts]
        own_ref, gate_a, gate_b, up_a, up_b, down_a, down_b, down_c = refs[3 + experts : 11 + experts]
        input_v, gain_v, ids_v, bias_v, sems = refs[11 + experts :]
        begin = pl.multiple_of(place_ref[2] * part, part)
        beyond = pl.multiple_of((1 - place_ref[2]) * part, part)
        columns = pl.ds(begin, part)
        moves = [
            (ids_hbm, ids_v),
            (input_hbm, input_v),
            (gain_hbm, gain_v),
            (bias_hbm, bias_v),
            (gate_hbm.at[pl.ds(0, deep), columns], gate_a),
            (gate_hbm.at[pl.ds(deep, deep), columns], gate_b),
            (keys_hbm, own_ref.at[pl.ds(0, span), pl.ds(0, heads_width)]),
            (values_hbm, own_ref.at[pl.ds(0, span), pl.ds(heads_width, heads_width)]),
            (up_hbm.at[pl.ds(0, deep), columns], up_a),
            (up_hbm.at[pl.ds(deep, deep), columns], up_b),
            (down_hbm.at[pl.ds(begin, thin), :], down_a),
            (down_hbm.at[pl.ds(pl.multiple_of(begin + thin, slim), slim), :], down_b),
            (down_hbm.at[pl.ds(pl.multiple_of(begin + 3 * slim, slim), slim), :], down_c.at[pl.ds(0, slim), :]),
            (down_hbm.at[pl.ds(pl.multiple_of(beyond + 3 * slim, slim), slim), :], down_c.at[pl.ds(slim, slim), :]),
        ]
        copies = [
            pltpu.make_async_copy(source, target, sems.at[k])
            for k, (source, target) in enumerate(moves)
        ]
        for copy in copies:
            copy.start()
        own_ref[span:, :] = jnp.zeros((heads, 2 * heads_width), jnp.bfloat16)
        copies[0].wait()
        _, picks = selections(place_ref, ids_v, experts, capacity)
        copies[1].wait()
        copies[2].wait()
        normed = norm_rows(input_v[...], gain_v[...]).astype(jnp.bfloat16)
        for d in range(experts):
            outs[d][...] = jnp.dot(
                picks[d], normed, preferred_element_type=jnp.float32
            ).astype(jnp.bfloat16)
        copies[3].wait()
        own_ref[span:, :span] = bias_v[...]
        for copy in copies[4:]:
            copy.wait()

    outs = [shape_of((capacity, width))] * experts + [
        shape_of((span + heads, 2 * heads_width)),
        shape_of((deep, part)),
        shape_of((deep, part)),
        shape_of((deep, part)),
        shape_of((deep, part)),
        shape_of((thin, width)),
        shape_of((slim, width)),
        shape_of((thin, width)),
    ]
    return call(
        body,
        outs,
        [SMEM] + [HBM] * 9,
        scratch=(
            pltpu.VMEM((rows, width), jnp.bfloat16),
            pltpu.VMEM((1, width), jnp.float32),
            pltpu.VMEM(ids.shape, jnp.int32),
            pltpu.VMEM(bias.shape, jnp.bfloat16),
            pltpu.SemaphoreType.DMA((14,)),
        ),
        flops=2 * experts * capacity * rows * width,
    )(
        place,
        *(
            pltpu.with_memory_space_constraint(array, pltpu.HBM)
            for array in (
                ffn_gain.reshape(1, width),
                ids,
                bias,
                moe_input,
                keys,
                values,
                gate,
                upward,
                down,
            )
        ),
    )


def combine_plan(place, ids, scores, experts, capacity):
    rows = ids.shape[1]

    def body(place_ref, ids_ref, scores_ref, high_ref, low_ref):
        hits, picks = selections(place_ref, ids_ref, experts, capacity)
        shares = scores_ref[...]
        shares = shares / jnp.sum(shares, axis=0, keepdims=True)
        weight = jnp.zeros((8, rows), jnp.float32)
        for k, hit in enumerate(hits):
            weight = weight + jnp.where(hit, shares[k : k + 1, :], 0.0)
        for d in range(experts):
            exact = picks[d].astype(jnp.float32) * weight[d : d + 1, :]
            high = exact.astype(jnp.bfloat16)
            some = slice(d * capacity, (d + 1) * capacity)
            high_ref[some, :] = high
            low_ref[some, :] = (exact - high.astype(jnp.float32)).astype(jnp.bfloat16)

    outs = [shape_of((experts * capacity, rows))] * 2
    return call(body, outs, [SMEM, VMEM, VMEM])(place, ids, scores)


def combine_rows(high, low, returned):
    rows = high.shape[1]
    width = returned[0].shape[1]

    def body(high_ref, low_ref, *refs):
        outputs = jnp.concatenate([ref[...] for ref in refs[:-1]], axis=0)
        weights = jnp.concatenate([high_ref[...], low_ref[...]], axis=1)
        total = lax.dot_general(
            weights, outputs, (((0,), (0,)), ((), ())), preferred_element_type=jnp.float32
        )
        refs[-1][...] = (total[:rows] + total[rows:]).astype(jnp.bfloat16)

    return call(
        body, shape_of((rows, width)), [VMEM] * (2 + len(returned)),
        flops=4 * high.shape[0] * rows * width,
    )(high, low, *returned)


def expert_rows(rows_in, pieces):
    capacity, width = rows_in[0].shape
    count = len(rows_in)
    hidden = sum(piece[0][0][0].shape[1] for piece in pieces)
    flat = [chunk[0] for piece in pieces for kind in piece for chunk in kind]

    def body(*refs):
        weight_refs = refs[count : count + len(flat)]
        outs = refs[count + len(flat) :]
        rows = jnp.concatenate([ref[...] for ref in refs[:count]], axis=0)
        inner, down = [], []
        at = 0
        for piece in pieces:
            kinds = []
            for kind in piece:
                chunk = [
                    weight_refs[at + k][low:high, :] for k, (_, low, high) in enumerate(kind)
                ]
                kinds.append(chunk[0] if len(chunk) == 1 else jnp.concatenate(chunk, axis=0))
                at += len(kind)
            size = kinds[0].shape[1]
            both = jnp.concatenate(kinds[:2], axis=1)
            down.append(kinds[2])
            product = jnp.dot(rows, both, preferred_element_type=jnp.float32)
            gate, upward = product[:, :size], product[:, size:]
            inner.append((gate / (1.0 + jnp.exp(-gate)) * upward).astype(jnp.bfloat16))
        inner = jnp.concatenate(inner, axis=1)
        out = jnp.dot(inner, jnp.concatenate(down, axis=0), preferred_element_type=jnp.float32)
        for d in range(count):
            outs[d][...] = out[d * capacity : (d + 1) * capacity].astype(jnp.bfloat16)

    return call(
        body,
        [shape_of((capacity, width))] * count,
        [VMEM] * (count + len(flat)),
        flops=6 * count * capacity * width * hidden,
    )(*rows_in, *flat)


def pair_sum(place, kept, received):
    share = kept.shape[0] // 2

    def body(place_ref, kept_ref, received_ref, outer_ref, inner_ref):
        mine = place_ref[3]
        for out, half in ((outer_ref, 1 - mine), (inner_ref, mine)):
            some = pl.ds(pl.multiple_of(half * share, share), share)
            out[...] = (kept_ref[some, :] + received_ref[some, :].astype(jnp.float32)).astype(out.dtype)

    outs = [shape_of((share, kept.shape[1])), shape_of((share, kept.shape[1]), jnp.float32)]
    return call(body, outs, [SMEM, VMEM, VMEM])(place, kept, received)


def finish(inner, received, gain):
    def body(inner_ref, received_ref, gain_ref, out_ref):
        projected = inner_ref[...] + received_ref[...].astype(jnp.float32)
        out_ref[...] = norm_rows(projected, gain_ref[...]).astype(jnp.bfloat16)

    return call(body, shape_of(inner.shape), [VMEM] * 3)(
        inner, received, gain.reshape(1, -1)
    )


def attend_project(place, queries, own, passed, out_weight, heads, quarters):
    span, width_heads = queries.shape
    size = width_heads // heads
    pair = 2 * size
    width = out_weight.shape[1]
    share = span // quarters
    blocks = len(passed)
    half = quarters // 2

    def body(place_ref, q_ref, own_ref, *refs):
        first_ref, direct_ref, relay_ref, last_ref = refs[:blocks]
        weight_ref, send_ref, keep_ref, acc, carry, att, proj, middle = refs[blocks:]
        kv_refs = (own_ref, first_ref, middle, last_ref)

        @pl.when(place_ref[0] == 2)
        def _():
            middle[...] = direct_ref[...]

        @pl.when(place_ref[0] == 3)
        def _():
            middle[...] = relay_ref[...]

        row = lax.broadcasted_iota(jnp.int32, (span, span), 0)
        column = lax.broadcasted_iota(jnp.int32, (span, span), 1)
        earlier = column < row
        after = jnp.where(row > column, 1.0, 0.0)
        sums = jnp.concatenate([after, jnp.ones((span, span), jnp.float32)], axis=1)
        sums = jnp.concatenate([sums, sums], axis=0).astype(jnp.bfloat16)
        low = lax.broadcasted_iota(jnp.int32, (span, pair), 1) < size

        def one_block(d):
            for h in range(heads):
                lanes = slice((h // 2) * pair, (h // 2 + 1) * pair)
                query = jnp.where(low if h % 2 == 0 else ~low, q_ref[:, lanes], 0.0).astype(jnp.bfloat16)
                key = kv_refs[d][:span, lanes]
                bias = kv_refs[d][span + h : span + h + 1, :span].astype(jnp.float32)
                z = lax.dot_general(
                    query, key, (((1,), (1,)), ((), ())), preferred_element_type=jnp.float32
                ) * size ** (-0.5) + bias
                rest = -(jnp.maximum(z, 0.0) + jnp.log1p(jnp.exp(-jnp.abs(z))))
                masked = jnp.where(earlier, rest, 0.0) if d == 0 else rest
                top = masked.astype(jnp.bfloat16)
                bottom = (masked - top.astype(jnp.float32)).astype(jnp.bfloat16)
                both = jnp.dot(
                    jnp.concatenate([top, bottom], axis=1), sums, preferred_element_type=jnp.float32
                )
                local = jnp.exp(z + rest + both[:, :span])
                if d == 0:
                    local = jnp.where(earlier, local, 0.0)
                value = kv_refs[d][:span, width_heads + lanes.start : width_heads + lanes.stop]
                part = jnp.dot(local.astype(jnp.bfloat16), value, preferred_element_type=jnp.float32)
                if d == 0:
                    carry[h] = both[:, span:]
                    total = part
                else:
                    before = carry[h]
                    total = jnp.exp(before) * part
                    carry[h] = before + both[:, span:]
                mine = low if h % 2 == 0 else ~low
                if d == 0 and h % 2 == 0:
                    acc[h // 2] = total
                elif d == 0:
                    acc[h // 2] = jnp.where(mine, total, acc[h // 2])
                else:
                    acc[h // 2] = acc[h // 2] + jnp.where(mine, total, 0.0)

        one_block(0)
        for d in range(1, blocks):
            pl.when(place_ref[0] >= d)(lambda d=d: one_block(d))
        for p in range(heads // 2):
            att[:, p * pair : (p + 1) * pair] = acc[p].astype(jnp.bfloat16)
        proj[...] = jnp.dot(att[...], weight_ref[...], preferred_element_type=jnp.float32)
        core = place_ref[1]
        for k in range(half):
            send_ref[k * share : (k + 1) * share, :] = proj[
                pl.ds((2 * k + 1 - core) * share, share), :
            ].astype(jnp.bfloat16)
            keep_ref[k * share : (k + 1) * share, :] = proj[pl.ds((2 * k + core) * share, share), :]

    return call(
        body,
        [shape_of((half * share, width)), shape_of((half * share, width), jnp.float32)],
        [SMEM, VMEM, VMEM] + [VMEM] * len(passed) + [VMEM],
        scratch=(
            pltpu.VMEM((heads // 2, span, pair), jnp.float32),
            pltpu.VMEM((heads, span, span), jnp.float32),
            pltpu.VMEM((span, width_heads), jnp.bfloat16),
            pltpu.VMEM((span, width), jnp.float32),
            pltpu.VMEM(own.shape, jnp.bfloat16),
        ),
        flops=4 * blocks * span * span * width_heads + 2 * span * width_heads * width,
    )(place, queries, own, *passed, out_weight)


def per_device(*arrays):
    return paired_step(*arrays)


def paired_step(
    queries,
    keys,
    values,
    stop_bias,
    out_weight,
    mix_gain,
    moe_input,
    ffn_gain,
    expert_ids,
    expert_scores,
    gate_weight,
    up_weight,
    down_weight,
):
    blocks = lax.axis_size("ep")
    shards = lax.axis_size("tp")
    group = lax.axis_index("grp")
    block = lax.axis_index("ep")
    shard = lax.axis_index("tp")
    place = jnp.stack([block, shard % 2, group, shard // 2]).astype(jnp.int32)
    heads = stop_bias.shape[1]

    def core(array):
        return lax.ppermute(array, "tp", [(i, i ^ 1) for i in range(shards)])

    def across(array):
        return lax.ppermute(array, "tp", [(i, i ^ 2) for i in range(shards)])

    def beside(array):
        return lax.ppermute(array, "grp", [(0, 1), (1, 0)])

    def turn(array, d):
        return lax.ppermute(array, "ep", [(i, (i + d) % blocks) for i in range(blocks)])

    def upward(array, d):
        return lax.ppermute(array, "ep", [(i, i + d) for i in range(blocks - d)])

    rows, top = expert_ids.shape
    capacity = 3 * rows * top // (2 * blocks)
    mine = (gate_weight[0], up_weight[0], down_weight[0])
    prepared = prepare(
        place, moe_input, ffn_gain, expert_ids.T, keys, values, stop_bias.T, mine, blocks, capacity
    )
    outbound, own, halves = prepared[:blocks], prepared[blocks], prepared[blocks + 1 :]

    arrived = [outbound[0]] + [turn(outbound[d], d) for d in range(1, blocks)]

    far = tuple(across(array) for array in halves)
    near = tuple(core(array) for array in mine)
    other = tuple(beside(array) for array in far[:-1])
    far_near = tuple(core(array) for array in far)
    other_near = tuple(core(array) for array in other)

    passed = [upward(own, 1), lax.ppermute(own, "ep", [(0, 2)])]
    passed += [lax.ppermute(array, "ep", [(2, 3)]) for array in passed]

    def chunk(array, low=0, high=None):
        return (array, low, array.shape[0] if high is None else high)

    def whole(arrays):
        return [[chunk(array)] for array in arrays]

    def chunked(arrays, last, which):
        slim = last.shape[0] // 2
        kinds = [[chunk(array) for array in some] for some in (arrays[0:2], arrays[2:4], arrays[4:6])]
        kinds[2].append(chunk(last, which * slim, (which + 1) * slim))
        return kinds

    pieces = [
        whole(mine),
        whole(near),
        chunked(far, far[6], 0),
        chunked(far_near, far_near[6], 0),
        chunked(other, far[6], 1),
        chunked(other_near, far_near[6], 1),
    ]
    order = (2, 0, 1, 3)
    done = expert_rows([arrived[k] for k in order[:1]], pieces)
    done += expert_rows([arrived[k] for k in order[1:]], pieces)
    produced = [done[order.index(k)] for k in range(blocks)]
    returned = [produced[0]] + [turn(produced[d], -d) for d in range(1, blocks)]

    send, kept = attend_project(place, queries, own, passed, out_weight, heads, shards)
    outer, inner = pair_sum(place, kept, core(send))
    mixed = finish(inner, across(outer), mix_gain)
    high, low = combine_plan(place, expert_ids.T, expert_scores.T, blocks, capacity)
    experts_mixed = combine_rows(high, low, returned)
    return (mixed, experts_mixed)


def solution(mesh):
    sizes = mesh.shape
    paired = sizes["grp"] == 2 and sizes["tp"] == 4 and sizes["ep"] == sizes["tp"]
    return jax.shard_map(
        per_device if paired else per_device_wide,
        mesh=mesh,
        in_specs=(
            P(("grp", "ep"), "tp"),
            P(("grp", "ep"), "tp"),
            P(("grp", "ep"), "tp"),
            P(("grp", "ep"), "tp"),
            P("tp", None),
            P(),
            P(("grp", "ep", "tp"), None),
            P(),
            P(("grp", "ep", "tp"), None),
            P(("grp", "ep", "tp"), None),
            P("ep", None, "tp"),
            P("ep", None, "tp"),
            P("ep", "tp", None),
        ),
        out_specs=(P(("grp", "ep", "tp"), None), P(("grp", "ep", "tp"), None)),
        check_vma=False,
    )
```

```python
import jax
import jax.numpy as jnp
from jax import lax
from jax.experimental import pallas as pl
from jax.experimental.pallas import tpu as pltpu
from jax.sharding import PartitionSpec as P


def norm_rows(values, gain):
    values = values.astype(jnp.float32)
    scale = lax.rsqrt(jnp.mean(values * values, axis=-1, keepdims=True) + 1e-06)
    return values * scale * gain


def break_terms(query_heads, query_place, key_block, bias_block, first):
    span = key_block.shape[0]
    heads = query_heads.shape[1]
    key_heads = key_block.reshape(span, heads, -1)
    scores = jnp.einsum("qhd,khd->hqk", query_heads, key_heads, preferred_element_type=jnp.float32)
    scores = scores * query_heads.shape[2] ** (-0.5) + bias_block.astype(jnp.float32).T[:, None, :]
    key_place = first + jnp.arange(span)
    past = (key_place[None, :] < query_place[:, None])[None]
    rest = jnp.where(past, jax.nn.log_sigmoid(-scores), 0.0)
    later = lax.cumsum(rest, axis=2, reverse=True)
    return (scores, past, rest, later)


def block_part(scores, past, rest, later, value_block, heads):
    within = later - rest
    local = jnp.where(past, jnp.exp(jax.nn.log_sigmoid(scores) + within), 0.0).astype(jnp.bfloat16)
    span = value_block.shape[0]
    value_heads = value_block.reshape(span, heads, -1)
    part = jnp.einsum("hqk,khd->qhd", local, value_heads, preferred_element_type=jnp.float32)
    return part.reshape(part.shape[0], -1)


def keep(state):
    return state


def dispatch_plan(normed, expert_ids, experts, capacity):
    rows, top = expert_ids.shape
    flat_ids = expert_ids.reshape(rows * top)
    onehot = (flat_ids[:, None] == jnp.arange(experts)[None, :]).astype(jnp.int32)
    earlier = jnp.cumsum(onehot, axis=0) - onehot
    place = jnp.sum(earlier * onehot, axis=1)
    target = flat_ids * capacity + place
    source = (
        jnp.zeros((experts * capacity,), jnp.int32)
        .at[target]
        .set(jnp.arange(rows * top, dtype=jnp.int32) // top + 1)
    )
    padded = jnp.concatenate([jnp.zeros((1, normed.shape[1]), normed.dtype), normed], axis=0)
    return (padded[source].reshape(experts, capacity, normed.shape[1]), target)


def expert_hidden(piece, gate_weight, up_weight):
    flat = piece.reshape(-1, piece.shape[-1])
    gate = jnp.dot(flat, gate_weight[0], preferred_element_type=jnp.float32)
    upward = jnp.dot(flat, up_weight[0], preferred_element_type=jnp.float32)
    hidden = (jax.nn.silu(gate) * upward).astype(jnp.bfloat16)
    return hidden.reshape(piece.shape[0], piece.shape[1], -1)


def send_back(summed):
    return lax.all_to_all(
        summed.astype(jnp.bfloat16), "ep", split_axis=0, concat_axis=0, tiled=True
    )


def return_rows(hidden_all, down_weight, sources):
    flat = hidden_all.reshape(-1, hidden_all.shape[2])
    product = jnp.dot(flat, down_weight[0], preferred_element_type=jnp.float32)
    return send_back(
        lax.psum_scatter(
            product.reshape(sources * lax.axis_size("tp"), hidden_all.shape[1], -1).astype(
                jnp.bfloat16
            ),
            "tp",
            scatter_dimension=0,
            tiled=True,
        ).astype(jnp.float32)
    )


def per_device_wide(
    queries,
    keys,
    values,
    stop_bias,
    out_weight,
    mix_gain,
    moe_input,
    ffn_gain,
    expert_ids,
    expert_scores,
    gate_weight,
    up_weight,
    down_weight,
):
    span = queries.shape[0]
    heads = stop_bias.shape[1]
    width_heads = queries.shape[1]
    blocks = lax.axis_size("ep")
    own_first = lax.axis_index("ep") * span
    query_heads = queries.reshape(span, heads, -1)
    query_place = own_first + jnp.arange(span)

    def piece_rows(piece, index):
        return tuple((lax.dynamic_slice_in_dim(member, index * span, span, 0) for member in piece))

    start_state = (
        jnp.zeros((blocks, heads, span), jnp.float32),
        jnp.zeros((blocks, span, width_heads), jnp.float32),
    )
    piece = (
        lax.all_gather(keys, "ep", axis=0, tiled=True),
        lax.all_gather(values, "ep", axis=0, tiled=True),
        lax.all_gather(stop_bias, "ep", axis=0, tiled=True),
    )

    def one_block(index, state):
        key_block, value_block, bias_block = piece_rows(piece, index)
        first = index * span

        def compute(inner_state):
            totals, parts = inner_state
            scores, past, rest, later = break_terms(
                query_heads, query_place, key_block, bias_block, first
            )
            part = block_part(scores, past, rest, later, value_block, heads)
            number = first // span
            totals = lax.dynamic_update_index_in_dim(totals, later[:, :, 0], number, 0)
            parts = lax.dynamic_update_index_in_dim(parts, part, number, 0)
            return (totals, parts)

        return lax.cond(first <= own_first, compute, keep, state)

    totals, parts = lax.fori_loop(0, piece[0].shape[0] // span, one_block, start_state)
    carried = lax.cumsum(totals, axis=0, reverse=True) - totals
    factor = jnp.exp(carried).transpose(0, 2, 1)[:, :, :, None]
    attended = jnp.sum(factor * parts.reshape(blocks, span, heads, -1), axis=0).reshape(
        span, width_heads
    )
    attended = attended.astype(jnp.bfloat16)
    projected = lax.psum_scatter(
        jnp.dot(attended, out_weight, preferred_element_type=jnp.float32).astype(jnp.bfloat16),
        "tp",
        scatter_dimension=0,
        tiled=True,
    ).astype(jnp.float32)
    mixed = norm_rows(projected, mix_gain).astype(jnp.bfloat16)
    normed = norm_rows(moe_input, ffn_gain).astype(jnp.bfloat16)
    rows, top = expert_ids.shape
    experts = lax.axis_size("ep")
    capacity = 3 * rows * top // (2 * experts)
    weights = expert_scores / jnp.sum(expert_scores, axis=1, keepdims=True)
    outbound, target = dispatch_plan(normed, expert_ids, experts, capacity)
    arrived = lax.all_to_all(outbound, "ep", split_axis=0, concat_axis=0, tiled=True)
    hidden_all = expert_hidden(
        lax.all_gather(arrived, "tp", axis=0, tiled=True), gate_weight, up_weight
    )
    returned = return_rows(hidden_all, down_weight, arrived.shape[0])
    picked = returned.reshape(experts * capacity, -1)[target].reshape(rows, top, -1)
    experts_mixed = jnp.sum(picked.astype(jnp.float32) * weights[:, :, None], axis=1).astype(
        jnp.bfloat16
    )
    return (mixed, experts_mixed)


VMEM = pl.BlockSpec(memory_space=pltpu.VMEM)
SMEM = pl.BlockSpec(memory_space=pltpu.SMEM)
HBM = pl.BlockSpec(memory_space=pltpu.HBM)


def shape_of(shape, dtype=jnp.bfloat16):
    return jax.ShapeDtypeStruct(shape, dtype)


def call(body, outs, ins, scratch=(), flops=0, limit=24):
    return pl.pallas_call(
        body,
        out_shape=outs,
        in_specs=ins,
        out_specs=jax.tree.map(lambda _: VMEM, outs),
        scratch_shapes=scratch,
        compiler_params=pltpu.CompilerParams(vmem_limit_bytes=limit * 1024 * 1024),
        cost_estimate=pl.CostEstimate(flops=flops, transcendentals=0, bytes_accessed=0),
    )


def selections(place_ref, ids_ref, experts, capacity):
    top, rows = ids_ref.shape
    distance = lax.broadcasted_iota(jnp.int32, (8, rows), 0)
    expert = (place_ref[0] + distance) % experts
    hits = [ids_ref[k : k + 1, :] == expert for k in range(top)]
    chosen = jnp.zeros((8, rows), jnp.float32)
    for hit in hits:
        chosen = chosen + jnp.where(hit & (distance < experts), 1.0, 0.0)
    below = lax.broadcasted_iota(jnp.int32, (rows, rows), 0) < lax.broadcasted_iota(
        jnp.int32, (rows, rows), 1
    )
    rank = jnp.dot(
        chosen.astype(jnp.bfloat16),
        jnp.where(below, 1.0, 0.0).astype(jnp.bfloat16),
        preferred_element_type=jnp.float32,
    )
    slot = lax.broadcasted_iota(jnp.int32, (capacity, rows), 0).astype(jnp.float32)
    picks = []
    for d in range(experts):
        pick = (rank[d : d + 1, :] == slot) & (chosen[d : d + 1, :] > 0.5)
        picks.append(jnp.where(pick, 1.0, 0.0).astype(jnp.bfloat16))
    return hits, picks


def in_hbm(*arrays):
    return [pltpu.with_memory_space_constraint(array, pltpu.HBM) for array in arrays]


def start_all(moves, sems):
    copies = [
        pltpu.make_async_copy(source, target, sems.at[k]) for k, (source, target) in enumerate(moves)
    ]
    for copy in copies:
        copy.start()
    return copies


def pack(place, keys, values, bias, gate):
    span, heads_width = keys.shape
    heads = bias.shape[0]
    part = gate.shape[1] // 2
    deep = gate.shape[0] // 2

    def body(place_ref, bias_hbm, keys_hbm, values_hbm, gate_hbm, own_ref, gate_a, bias_v, sems):
        columns = pl.ds(pl.multiple_of(place_ref[2] * part, part), part)
        copies = start_all(
            [
                (bias_hbm, bias_v),
                (gate_hbm.at[pl.ds(0, deep), columns], gate_a),
                (keys_hbm, own_ref.at[pl.ds(0, span), pl.ds(0, heads_width)]),
                (values_hbm, own_ref.at[pl.ds(0, span), pl.ds(heads_width, heads_width)]),
            ],
            sems,
        )
        own_ref[span:, :] = jnp.zeros((heads, 2 * heads_width), jnp.bfloat16)
        copies[0].wait()
        own_ref[span:, :span] = bias_v[...]
        for copy in copies[1:]:
            copy.wait()

    return call(
        body,
        [shape_of((span + heads, 2 * heads_width)), shape_of((deep, part))],
        [SMEM] + [HBM] * 4,
        scratch=(pltpu.VMEM(bias.shape, jnp.bfloat16), pltpu.SemaphoreType.DMA((4,))),
    )(place, *in_hbm(bias, keys, values, gate))


def route(place, moe_input, ffn_gain, ids, weights, experts, capacity):
    rows, width = moe_input.shape
    gate, upward, down = weights
    part = gate.shape[1] // 2
    deep = gate.shape[0] // 2
    thin = part // 2
    slim = part // 4

    def body(place_ref, gain_hbm, ids_hbm, input_hbm, gate_hbm, up_hbm, down_hbm, *refs):
        outs = refs[:experts]
        gate_b, up_a, up_b, down_a, down_b, down_c, input_v, gain_v, ids_v, sems = refs[experts:]
        begin = pl.multiple_of(place_ref[2] * part, part)
        beyond = pl.multiple_of((1 - place_ref[2]) * part, part)
        columns = pl.ds(begin, part)

        def some(first, size):
            return down_hbm.at[pl.ds(pl.multiple_of(first, slim), size), :]

        copies = start_all(
            [
                (ids_hbm, ids_v),
                (input_hbm, input_v),
                (gain_hbm, gain_v),
                (gate_hbm.at[pl.ds(deep, deep), columns], gate_b),
                (up_hbm.at[pl.ds(0, deep), columns], up_a),
                (up_hbm.at[pl.ds(deep, deep), columns], up_b),
                (some(begin, thin), down_a),
                (some(begin + thin, slim), down_b),
                (some(begin + 3 * slim, slim), down_c.at[pl.ds(0, slim), :]),
                (some(beyond + 3 * slim, slim), down_c.at[pl.ds(slim, slim), :]),
            ],
            sems,
        )
        copies[0].wait()
        _, picks = selections(place_ref, ids_v, experts, capacity)
        copies[1].wait()
        copies[2].wait()
        normed = norm_rows(input_v[...], gain_v[...]).astype(jnp.bfloat16)
        for d in range(experts):
            outs[d][...] = jnp.dot(
                picks[d], normed, preferred_element_type=jnp.float32
            ).astype(jnp.bfloat16)
        for copy in copies[3:]:
            copy.wait()

    outs = [shape_of((capacity, width))] * experts + [
        shape_of((deep, part)),
        shape_of((deep, part)),
        shape_of((deep, part)),
        shape_of((thin, width)),
        shape_of((slim, width)),
        shape_of((thin, width)),
    ]
    return call(
        body,
        outs,
        [SMEM] + [HBM] * 6,
        scratch=(
            pltpu.VMEM((rows, width), jnp.bfloat16),
            pltpu.VMEM((1, width), jnp.float32),
            pltpu.VMEM(ids.shape, jnp.int32),
            pltpu.SemaphoreType.DMA((10,)),
        ),
        flops=2 * experts * capacity * rows * width,
    )(place, *in_hbm(ffn_gain.reshape(1, width), ids, moe_input, gate, upward, down))


def combine_plan(place, ids, scores, experts, capacity):
    rows = ids.shape[1]

    def body(place_ref, ids_ref, scores_ref, high_ref, low_ref):
        hits, picks = selections(place_ref, ids_ref, experts, capacity)
        shares = scores_ref[...]
        shares = shares / jnp.sum(shares, axis=0, keepdims=True)
        weight = jnp.zeros((8, rows), jnp.float32)
        for k, hit in enumerate(hits):
            weight = weight + jnp.where(hit, shares[k : k + 1, :], 0.0)
        for d in range(experts):
            exact = picks[d].astype(jnp.float32) * weight[d : d + 1, :]
            high = exact.astype(jnp.bfloat16)
            some = slice(d * capacity, (d + 1) * capacity)
            high_ref[some, :] = high
            low_ref[some, :] = (exact - high.astype(jnp.float32)).astype(jnp.bfloat16)

    outs = [shape_of((experts * capacity, rows))] * 2
    return call(body, outs, [SMEM, VMEM, VMEM])(place, ids, scores)


def combine_rows(high, low, returned):
    rows = high.shape[1]
    width = returned[0].shape[1]

    def body(high_ref, low_ref, *refs):
        outputs = jnp.concatenate([ref[...] for ref in refs[:-1]], axis=0)
        weights = jnp.concatenate([high_ref[...], low_ref[...]], axis=1)
        total = lax.dot_general(
            weights, outputs, (((0,), (0,)), ((), ())), preferred_element_type=jnp.float32
        )
        refs[-1][...] = (total[:rows] + total[rows:]).astype(jnp.bfloat16)

    return call(
        body, shape_of((rows, width)), [VMEM] * (2 + len(returned)),
        flops=4 * high.shape[0] * rows * width,
    )(high, low, *returned)


def expert_rows(rows_in, pieces):
    capacity, width = rows_in[0].shape
    count = len(rows_in)
    hidden = sum(piece[0][0][0].shape[1] for piece in pieces)
    flat = [chunk[0] for piece in pieces for kind in piece for chunk in kind]

    def body(*refs):
        weight_refs = refs[count : count + len(flat)]
        outs = refs[count + len(flat) :]
        rows = jnp.concatenate([ref[...] for ref in refs[:count]], axis=0)
        inner, down = [], []
        at = 0
        for piece in pieces:
            kinds = []
            for kind in piece:
                chunk = [
                    weight_refs[at + k][low:high, :] for k, (_, low, high) in enumerate(kind)
                ]
                kinds.append(chunk[0] if len(chunk) == 1 else jnp.concatenate(chunk, axis=0))
                at += len(kind)
            size = kinds[0].shape[1]
            both = jnp.concatenate(kinds[:2], axis=1)
            down.append(kinds[2])
            product = jnp.dot(rows, both, preferred_element_type=jnp.float32)
            gate, upward = product[:, :size], product[:, size:]
            inner.append((gate / (1.0 + jnp.exp(-gate)) * upward).astype(jnp.bfloat16))
        inner = jnp.concatenate(inner, axis=1)
        out = jnp.dot(inner, jnp.concatenate(down, axis=0), preferred_element_type=jnp.float32)
        for d in range(count):
            outs[d][...] = out[d * capacity : (d + 1) * capacity].astype(jnp.bfloat16)

    return call(
        body,
        [shape_of((capacity, width))] * count,
        [VMEM] * (count + len(flat)),
        flops=6 * count * capacity * width * hidden,
    )(*rows_in, *flat)


def pair_sum(place, kept, received):
    share = kept.shape[0] // 2

    def body(place_ref, kept_ref, received_ref, outer_ref, inner_ref):
        mine = place_ref[3]
        for out, half in ((outer_ref, 1 - mine), (inner_ref, mine)):
            some = pl.ds(pl.multiple_of(half * share, share), share)
            out[...] = (kept_ref[some, :] + received_ref[some, :].astype(jnp.float32)).astype(out.dtype)

    outs = [shape_of((share, kept.shape[1])), shape_of((share, kept.shape[1]), jnp.float32)]
    return call(body, outs, [SMEM, VMEM, VMEM])(place, kept, received)


def finish(inner, received, gain):
    def body(inner_ref, received_ref, gain_ref, out_ref):
        projected = inner_ref[...] + received_ref[...].astype(jnp.float32)
        out_ref[...] = norm_rows(projected, gain_ref[...]).astype(jnp.bfloat16)

    return call(body, shape_of(inner.shape), [VMEM] * 3)(
        inner, received, gain.reshape(1, -1)
    )


def attend_project(place, queries, own, passed, out_weight, heads, quarters):
    span, width_heads = queries.shape
    size = width_heads // heads
    pair = 2 * size
    width = out_weight.shape[1]
    share = span // quarters
    blocks = len(passed)
    half = quarters // 2

    def body(place_ref, q_ref, own_ref, *refs):
        first_ref, direct_ref, relay_ref, last_ref = refs[:blocks]
        weight_ref, send_ref, keep_ref, acc, carry, att, proj, middle = refs[blocks:]
        kv_refs = (own_ref, first_ref, middle, last_ref)

        @pl.when(place_ref[0] == 2)
        def _():
            middle[...] = direct_ref[...]

        @pl.when(place_ref[0] == 3)
        def _():
            middle[...] = relay_ref[...]

        row = lax.broadcasted_iota(jnp.int32, (span, span), 0)
        column = lax.broadcasted_iota(jnp.int32, (span, span), 1)
        earlier = column < row
        after = jnp.where(row > column, 1.0, 0.0)
        sums = jnp.concatenate([after, jnp.ones((span, span), jnp.float32)], axis=1)
        sums = jnp.concatenate([sums, sums], axis=0).astype(jnp.bfloat16)
        low = lax.broadcasted_iota(jnp.int32, (span, pair), 1) < size

        def one_block(d):
            for h in range(heads):
                lanes = slice((h // 2) * pair, (h // 2 + 1) * pair)
                query = jnp.where(low if h % 2 == 0 else ~low, q_ref[:, lanes], 0.0).astype(jnp.bfloat16)
                key = kv_refs[d][:span, lanes]
                bias = kv_refs[d][span + h : span + h + 1, :span].astype(jnp.float32)
                z = lax.dot_general(
                    query, key, (((1,), (1,)), ((), ())), preferred_element_type=jnp.float32
                ) * size ** (-0.5) + bias
                rest = -(jnp.maximum(z, 0.0) + jnp.log1p(jnp.exp(-jnp.abs(z))))
                masked = jnp.where(earlier, rest, 0.0) if d == 0 else rest
                top = masked.astype(jnp.bfloat16)
                bottom = (masked - top.astype(jnp.float32)).astype(jnp.bfloat16)
                both = jnp.dot(
                    jnp.concatenate([top, bottom], axis=1), sums, preferred_element_type=jnp.float32
                )
                local = jnp.exp(z + rest + both[:, :span])
                if d == 0:
                    local = jnp.where(earlier, local, 0.0)
                value = kv_refs[d][:span, width_heads + lanes.start : width_heads + lanes.stop]
                part = jnp.dot(local.astype(jnp.bfloat16), value, preferred_element_type=jnp.float32)
                if d == 0:
                    carry[h] = both[:, span:]
                    total = part
                else:
                    before = carry[h]
                    total = jnp.exp(before) * part
                    carry[h] = before + both[:, span:]
                mine = low if h % 2 == 0 else ~low
                if d == 0 and h % 2 == 0:
                    acc[h // 2] = total
                elif d == 0:
                    acc[h // 2] = jnp.where(mine, total, acc[h // 2])
                else:
                    acc[h // 2] = acc[h // 2] + jnp.where(mine, total, 0.0)

        one_block(0)
        for d in range(1, blocks):
            pl.when(place_ref[0] >= d)(lambda d=d: one_block(d))
        for p in range(heads // 2):
            att[:, p * pair : (p + 1) * pair] = acc[p].astype(jnp.bfloat16)
        proj[...] = jnp.dot(att[...], weight_ref[...], preferred_element_type=jnp.float32)
        core = place_ref[1]
        for k in range(half):
            send_ref[k * share : (k + 1) * share, :] = proj[
                pl.ds((2 * k + 1 - core) * share, share), :
            ].astype(jnp.bfloat16)
            keep_ref[k * share : (k + 1) * share, :] = proj[pl.ds((2 * k + core) * share, share), :]

    return call(
        body,
        [shape_of((half * share, width)), shape_of((half * share, width), jnp.float32)],
        [SMEM, VMEM, VMEM] + [VMEM] * len(passed) + [VMEM],
        scratch=(
            pltpu.VMEM((heads // 2, span, pair), jnp.float32),
            pltpu.VMEM((heads, span, span), jnp.float32),
            pltpu.VMEM((span, width_heads), jnp.bfloat16),
            pltpu.VMEM((span, width), jnp.float32),
            pltpu.VMEM(own.shape, jnp.bfloat16),
        ),
        flops=4 * blocks * span * span * width_heads + 2 * span * width_heads * width,
    )(place, queries, own, *passed, out_weight)


def per_device(*arrays):
    return paired_step(*arrays)


def paired_step(
    queries,
    keys,
    values,
    stop_bias,
    out_weight,
    mix_gain,
    moe_input,
    ffn_gain,
    expert_ids,
    expert_scores,
    gate_weight,
    up_weight,
    down_weight,
):
    blocks = lax.axis_size("ep")
    shards = lax.axis_size("tp")
    group = lax.axis_index("grp")
    block = lax.axis_index("ep")
    shard = lax.axis_index("tp")
    place = jnp.stack([block, shard % 2, group, shard // 2]).astype(jnp.int32)
    heads = stop_bias.shape[1]

    def core(array):
        return lax.ppermute(array, "tp", [(i, i ^ 1) for i in range(shards)])

    def across(array):
        return lax.ppermute(array, "tp", [(i, i ^ 2) for i in range(shards)])

    def beside(array):
        return lax.ppermute(array, "grp", [(0, 1), (1, 0)])

    def turn(array, d):
        return lax.ppermute(array, "ep", [(i, (i + d) % blocks) for i in range(blocks)])

    def upward(array, d):
        return lax.ppermute(array, "ep", [(i, i + d) for i in range(blocks - d)])

    rows, top = expert_ids.shape
    capacity = 3 * rows * top // (2 * blocks)
    mine = (gate_weight[0], up_weight[0], down_weight[0])
    own, first_half = pack(place, keys, values, stop_bias.T, mine[0])
    routed = route(place, moe_input, ffn_gain, expert_ids.T, mine, blocks, capacity)
    outbound, halves = routed[:blocks], [first_half, *routed[blocks:]]

    arrived = [outbound[0]] + [turn(outbound[d], d) for d in range(1, blocks)]

    far = tuple(across(array) for array in halves)
    near = tuple(core(array) for array in mine)
    other = tuple(beside(array) for array in far[:-1])
    far_near = tuple(core(array) for array in far)
    other_near = tuple(core(array) for array in other)

    passed = [upward(own, 1), lax.ppermute(own, "ep", [(0, 2)])]
    passed += [lax.ppermute(array, "ep", [(2, 3)]) for array in passed]

    def chunk(array, low=0, high=None):
        return (array, low, array.shape[0] if high is None else high)

    def whole(arrays):
        return [[chunk(array)] for array in arrays]

    def chunked(arrays, last, which):
        slim = last.shape[0] // 2
        kinds = [[chunk(array) for array in some] for some in (arrays[0:2], arrays[2:4], arrays[4:6])]
        kinds[2].append(chunk(last, which * slim, (which + 1) * slim))
        return kinds

    pieces = [
        whole(mine),
        whole(near),
        chunked(far, far[6], 0),
        chunked(far_near, far_near[6], 0),
        chunked(other, far[6], 1),
        chunked(other_near, far_near[6], 1),
    ]
    order = (2, 0, 1, 3)
    done = expert_rows([arrived[k] for k in order[:1]], pieces)
    done += expert_rows([arrived[k] for k in order[1:]], pieces)
    produced = [done[order.index(k)] for k in range(blocks)]
    returned = [produced[0]] + [turn(produced[d], -d) for d in range(1, blocks)]

    send, kept = attend_project(place, queries, own, passed, out_weight, heads, shards)
    outer, inner = pair_sum(place, kept, core(send))
    mixed = finish(inner, across(outer), mix_gain)
    high, low = combine_plan(place, expert_ids.T, expert_scores.T, blocks, capacity)
    experts_mixed = combine_rows(high, low, returned)
    return (mixed, experts_mixed)


def solution(mesh):
    sizes = mesh.shape
    paired = sizes["grp"] == 2 and sizes["tp"] == 4 and sizes["ep"] == sizes["tp"]
    return jax.shard_map(
        per_device if paired else per_device_wide,
        mesh=mesh,
        in_specs=(
            P(("grp", "ep"), "tp"),
            P(("grp", "ep"), "tp"),
            P(("grp", "ep"), "tp"),
            P(("grp", "ep"), "tp"),
            P("tp", None),
            P(),
            P(("grp", "ep", "tp"), None),
            P(),
            P(("grp", "ep", "tp"), None),
            P(("grp", "ep", "tp"), None),
            P("ep", None, "tp"),
            P("ep", None, "tp"),
            P("ep", "tp", None),
        ),
        out_specs=(P(("grp", "ep", "tp"), None), P(("grp", "ep", "tp"), None)),
        check_vma=False,
    )
```

```python
import jax
import jax.numpy as jnp
from jax import lax
from jax.experimental import pallas as pl
from jax.experimental.pallas import tpu as pltpu
from jax.sharding import PartitionSpec as P


def norm_rows(values, gain):
    values = values.astype(jnp.float32)
    scale = lax.rsqrt(jnp.mean(values * values, axis=-1, keepdims=True) + 1e-06)
    return values * scale * gain


def break_terms(query_heads, query_place, key_block, bias_block, first):
    span = key_block.shape[0]
    heads = query_heads.shape[1]
    key_heads = key_block.reshape(span, heads, -1)
    scores = jnp.einsum("qhd,khd->hqk", query_heads, key_heads, preferred_element_type=jnp.float32)
    scores = scores * query_heads.shape[2] ** (-0.5) + bias_block.astype(jnp.float32).T[:, None, :]
    key_place = first + jnp.arange(span)
    past = (key_place[None, :] < query_place[:, None])[None]
    rest = jnp.where(past, jax.nn.log_sigmoid(-scores), 0.0)
    later = lax.cumsum(rest, axis=2, reverse=True)
    return (scores, past, rest, later)


def block_part(scores, past, rest, later, value_block, heads):
    within = later - rest
    local = jnp.where(past, jnp.exp(jax.nn.log_sigmoid(scores) + within), 0.0).astype(jnp.bfloat16)
    span = value_block.shape[0]
    value_heads = value_block.reshape(span, heads, -1)
    part = jnp.einsum("hqk,khd->qhd", local, value_heads, preferred_element_type=jnp.float32)
    return part.reshape(part.shape[0], -1)


def keep(state):
    return state


def dispatch_plan(normed, expert_ids, experts, capacity):
    rows, top = expert_ids.shape
    flat_ids = expert_ids.reshape(rows * top)
    onehot = (flat_ids[:, None] == jnp.arange(experts)[None, :]).astype(jnp.int32)
    earlier = jnp.cumsum(onehot, axis=0) - onehot
    place = jnp.sum(earlier * onehot, axis=1)
    target = flat_ids * capacity + place
    source = (
        jnp.zeros((experts * capacity,), jnp.int32)
        .at[target]
        .set(jnp.arange(rows * top, dtype=jnp.int32) // top + 1)
    )
    padded = jnp.concatenate([jnp.zeros((1, normed.shape[1]), normed.dtype), normed], axis=0)
    return (padded[source].reshape(experts, capacity, normed.shape[1]), target)


def expert_hidden(piece, gate_weight, up_weight):
    flat = piece.reshape(-1, piece.shape[-1])
    gate = jnp.dot(flat, gate_weight[0], preferred_element_type=jnp.float32)
    upward = jnp.dot(flat, up_weight[0], preferred_element_type=jnp.float32)
    hidden = (jax.nn.silu(gate) * upward).astype(jnp.bfloat16)
    return hidden.reshape(piece.shape[0], piece.shape[1], -1)


def send_back(summed):
    return lax.all_to_all(
        summed.astype(jnp.bfloat16), "ep", split_axis=0, concat_axis=0, tiled=True
    )


def return_rows(hidden_all, down_weight, sources):
    flat = hidden_all.reshape(-1, hidden_all.shape[2])
    product = jnp.dot(flat, down_weight[0], preferred_element_type=jnp.float32)
    return send_back(
        lax.psum_scatter(
            product.reshape(sources * lax.axis_size("tp"), hidden_all.shape[1], -1).astype(
                jnp.bfloat16
            ),
            "tp",
            scatter_dimension=0,
            tiled=True,
        ).astype(jnp.float32)
    )


def per_device_wide(
    queries,
    keys,
    values,
    stop_bias,
    out_weight,
    mix_gain,
    moe_input,
    ffn_gain,
    expert_ids,
    expert_scores,
    gate_weight,
    up_weight,
    down_weight,
):
    span = queries.shape[0]
    heads = stop_bias.shape[1]
    width_heads = queries.shape[1]
    blocks = lax.axis_size("ep")
    own_first = lax.axis_index("ep") * span
    query_heads = queries.reshape(span, heads, -1)
    query_place = own_first + jnp.arange(span)

    def piece_rows(piece, index):
        return tuple((lax.dynamic_slice_in_dim(member, index * span, span, 0) for member in piece))

    start_state = (
        jnp.zeros((blocks, heads, span), jnp.float32),
        jnp.zeros((blocks, span, width_heads), jnp.float32),
    )
    piece = (
        lax.all_gather(keys, "ep", axis=0, tiled=True),
        lax.all_gather(values, "ep", axis=0, tiled=True),
        lax.all_gather(stop_bias, "ep", axis=0, tiled=True),
    )

    def one_block(index, state):
        key_block, value_block, bias_block = piece_rows(piece, index)
        first = index * span

        def compute(inner_state):
            totals, parts = inner_state
            scores, past, rest, later = break_terms(
                query_heads, query_place, key_block, bias_block, first
            )
            part = block_part(scores, past, rest, later, value_block, heads)
            number = first // span
            totals = lax.dynamic_update_index_in_dim(totals, later[:, :, 0], number, 0)
            parts = lax.dynamic_update_index_in_dim(parts, part, number, 0)
            return (totals, parts)

        return lax.cond(first <= own_first, compute, keep, state)

    totals, parts = lax.fori_loop(0, piece[0].shape[0] // span, one_block, start_state)
    carried = lax.cumsum(totals, axis=0, reverse=True) - totals
    factor = jnp.exp(carried).transpose(0, 2, 1)[:, :, :, None]
    attended = jnp.sum(factor * parts.reshape(blocks, span, heads, -1), axis=0).reshape(
        span, width_heads
    )
    attended = attended.astype(jnp.bfloat16)
    projected = lax.psum_scatter(
        jnp.dot(attended, out_weight, preferred_element_type=jnp.float32).astype(jnp.bfloat16),
        "tp",
        scatter_dimension=0,
        tiled=True,
    ).astype(jnp.float32)
    mixed = norm_rows(projected, mix_gain).astype(jnp.bfloat16)
    normed = norm_rows(moe_input, ffn_gain).astype(jnp.bfloat16)
    rows, top = expert_ids.shape
    experts = lax.axis_size("ep")
    capacity = 3 * rows * top // (2 * experts)
    weights = expert_scores / jnp.sum(expert_scores, axis=1, keepdims=True)
    outbound, target = dispatch_plan(normed, expert_ids, experts, capacity)
    arrived = lax.all_to_all(outbound, "ep", split_axis=0, concat_axis=0, tiled=True)
    hidden_all = expert_hidden(
        lax.all_gather(arrived, "tp", axis=0, tiled=True), gate_weight, up_weight
    )
    returned = return_rows(hidden_all, down_weight, arrived.shape[0])
    picked = returned.reshape(experts * capacity, -1)[target].reshape(rows, top, -1)
    experts_mixed = jnp.sum(picked.astype(jnp.float32) * weights[:, :, None], axis=1).astype(
        jnp.bfloat16
    )
    return (mixed, experts_mixed)


VMEM = pl.BlockSpec(memory_space=pltpu.VMEM)
SMEM = pl.BlockSpec(memory_space=pltpu.SMEM)
HBM = pl.BlockSpec(memory_space=pltpu.HBM)


def shape_of(shape, dtype=jnp.bfloat16):
    return jax.ShapeDtypeStruct(shape, dtype)


def call(body, outs, ins, scratch=(), flops=0, limit=24):
    return pl.pallas_call(
        body,
        out_shape=outs,
        in_specs=ins,
        out_specs=jax.tree.map(lambda _: VMEM, outs),
        scratch_shapes=scratch,
        compiler_params=pltpu.CompilerParams(vmem_limit_bytes=limit * 1024 * 1024),
        cost_estimate=pl.CostEstimate(flops=flops, transcendentals=0, bytes_accessed=0),
    )


def selections(place_ref, ids_ref, experts, capacity):
    top, rows = ids_ref.shape
    distance = lax.broadcasted_iota(jnp.int32, (8, rows), 0)
    expert = (place_ref[0] + distance) % experts
    hits = [ids_ref[k : k + 1, :] == expert for k in range(top)]
    chosen = jnp.zeros((8, rows), jnp.float32)
    for hit in hits:
        chosen = chosen + jnp.where(hit & (distance < experts), 1.0, 0.0)
    below = lax.broadcasted_iota(jnp.int32, (rows, rows), 0) < lax.broadcasted_iota(
        jnp.int32, (rows, rows), 1
    )
    rank = jnp.dot(
        chosen.astype(jnp.bfloat16),
        jnp.where(below, 1.0, 0.0).astype(jnp.bfloat16),
        preferred_element_type=jnp.float32,
    )
    slot = lax.broadcasted_iota(jnp.int32, (capacity, rows), 0).astype(jnp.float32)
    picks = []
    for d in range(experts):
        pick = (rank[d : d + 1, :] == slot) & (chosen[d : d + 1, :] > 0.5)
        picks.append(jnp.where(pick, 1.0, 0.0).astype(jnp.bfloat16))
    return hits, picks


def in_hbm(*arrays):
    return [pltpu.with_memory_space_constraint(array, pltpu.HBM) for array in arrays]


def start_all(moves, sems):
    copies = [
        pltpu.make_async_copy(source, target, sems.at[k]) for k, (source, target) in enumerate(moves)
    ]
    for copy in copies:
        copy.start()
    return copies


def pack(place, keys, values, bias, gate):
    span, heads_width = keys.shape
    heads = bias.shape[0]
    part = gate.shape[1] // 2
    deep = gate.shape[0] // 2

    def body(place_ref, bias_hbm, keys_hbm, values_hbm, gate_hbm, own_ref, gate_a, bias_v, sems):
        columns = pl.ds(pl.multiple_of(place_ref[2] * part, part), part)
        copies = start_all(
            [
                (bias_hbm, bias_v),
                (gate_hbm.at[pl.ds(0, deep), columns], gate_a),
                (keys_hbm, own_ref.at[pl.ds(0, span), pl.ds(0, heads_width)]),
                (values_hbm, own_ref.at[pl.ds(0, span), pl.ds(heads_width, heads_width)]),
            ],
            sems,
        )
        own_ref[span:, :] = jnp.zeros((heads, 2 * heads_width), jnp.bfloat16)
        copies[0].wait()
        own_ref[span:, :span] = bias_v[...]
        for copy in copies[1:]:
            copy.wait()

    return call(
        body,
        [shape_of((span + heads, 2 * heads_width)), shape_of((deep, part))],
        [SMEM] + [HBM] * 4,
        scratch=(pltpu.VMEM(bias.shape, jnp.bfloat16), pltpu.SemaphoreType.DMA((4,))),
    )(place, *in_hbm(bias, keys, values, gate))


def route(place, moe_input, ffn_gain, ids, weights, experts, capacity):
    rows, width = moe_input.shape
    gate, upward, down = weights
    part = gate.shape[1] // 2
    deep = gate.shape[0] // 2
    thin = part // 2

    def body(place_ref, gain_hbm, ids_hbm, input_hbm, gate_hbm, up_hbm, down_hbm, *refs):
        outs = refs[:experts]
        gate_b, up_a, up_b, down_a, down_b, down_c, input_v, gain_v, ids_v, sems = refs[experts:]
        begin = pl.multiple_of(place_ref[2] * part, part)
        beyond = pl.multiple_of((1 - place_ref[2]) * part, part)
        columns = pl.ds(begin, part)

        def some(first, size):
            return down_hbm.at[pl.ds(pl.multiple_of(first, thin), size), :]

        copies = start_all(
            [
                (ids_hbm, ids_v),
                (input_hbm, input_v),
                (gain_hbm, gain_v),
                (gate_hbm.at[pl.ds(deep, deep), columns], gate_b),
                (up_hbm.at[pl.ds(0, deep), columns], up_a),
                (up_hbm.at[pl.ds(deep, deep), columns], up_b),
                (some(begin, thin), down_a),
                (some(begin + thin, thin), down_b),
                (some(beyond + thin, thin), down_c),
            ],
            sems,
        )
        copies[0].wait()
        _, picks = selections(place_ref, ids_v, experts, capacity)
        copies[1].wait()
        copies[2].wait()
        normed = norm_rows(input_v[...], gain_v[...]).astype(jnp.bfloat16)
        for d in range(experts):
            outs[d][...] = jnp.dot(
                picks[d], normed, preferred_element_type=jnp.float32
            ).astype(jnp.bfloat16)
        for copy in copies[3:]:
            copy.wait()

    outs = [shape_of((capacity, width))] * experts + [
        shape_of((deep, part)),
        shape_of((deep, part)),
        shape_of((deep, part)),
        shape_of((thin, width)),
        shape_of((thin, width)),
        shape_of((thin, width)),
    ]
    return call(
        body,
        outs,
        [SMEM] + [HBM] * 6,
        scratch=(
            pltpu.VMEM((rows, width), jnp.bfloat16),
            pltpu.VMEM((1, width), jnp.float32),
            pltpu.VMEM(ids.shape, jnp.int32),
            pltpu.SemaphoreType.DMA((9,)),
        ),
        flops=2 * experts * capacity * rows * width,
    )(place, *in_hbm(ffn_gain.reshape(1, width), ids, moe_input, gate, upward, down))


def combine_plan(place, ids, scores, experts, capacity):
    rows = ids.shape[1]

    def body(place_ref, ids_ref, scores_ref, high_ref, low_ref):
        hits, picks = selections(place_ref, ids_ref, experts, capacity)
        shares = scores_ref[...]
        shares = shares / jnp.sum(shares, axis=0, keepdims=True)
        weight = jnp.zeros((8, rows), jnp.float32)
        for k, hit in enumerate(hits):
            weight = weight + jnp.where(hit, shares[k : k + 1, :], 0.0)
        for d in range(experts):
            exact = picks[d].astype(jnp.float32) * weight[d : d + 1, :]
            high = exact.astype(jnp.bfloat16)
            some = slice(d * capacity, (d + 1) * capacity)
            high_ref[some, :] = high
            low_ref[some, :] = (exact - high.astype(jnp.float32)).astype(jnp.bfloat16)

    outs = [shape_of((experts * capacity, rows))] * 2
    return call(body, outs, [SMEM, VMEM, VMEM])(place, ids, scores)


def combine_rows(high, low, returned):
    rows = high.shape[1]
    width = returned[0].shape[1]

    def body(high_ref, low_ref, *refs):
        outputs = jnp.concatenate([ref[...] for ref in refs[:-1]], axis=0)
        weights = jnp.concatenate([high_ref[...], low_ref[...]], axis=1)
        total = lax.dot_general(
            weights, outputs, (((0,), (0,)), ((), ())), preferred_element_type=jnp.float32
        )
        refs[-1][...] = (total[:rows] + total[rows:]).astype(jnp.bfloat16)

    return call(
        body, shape_of((rows, width)), [VMEM] * (2 + len(returned)),
        flops=4 * high.shape[0] * rows * width,
    )(high, low, *returned)


def expert_rows(rows_in, pieces):
    capacity, width = rows_in[0].shape
    count = len(rows_in)
    hidden = sum(piece[0][0].shape[1] for piece in pieces)
    flat = [chunk for piece in pieces for kind in piece for chunk in kind]

    def body(*refs):
        weight_refs = refs[count : count + len(flat)]
        outs = refs[count + len(flat) :]
        rows = jnp.concatenate([ref[...] for ref in refs[:count]], axis=0)
        inner, down = [], []
        at = 0
        for piece in pieces:
            kinds = []
            for kind in piece:
                chunk = [ref[...] for ref in weight_refs[at : at + len(kind)]]
                kinds.append(chunk[0] if len(chunk) == 1 else jnp.concatenate(chunk, axis=0))
                at += len(kind)
            size = kinds[0].shape[1]
            both = jnp.concatenate(kinds[:2], axis=1)
            down.append(kinds[2])
            product = jnp.dot(rows, both, preferred_element_type=jnp.float32)
            gate, upward = product[:, :size], product[:, size:]
            inner.append((gate / (1.0 + jnp.exp(-gate)) * upward).astype(jnp.bfloat16))
        inner = jnp.concatenate(inner, axis=1)
        out = jnp.dot(inner, jnp.concatenate(down, axis=0), preferred_element_type=jnp.float32)
        for d in range(count):
            outs[d][...] = out[d * capacity : (d + 1) * capacity].astype(jnp.bfloat16)

    return call(
        body,
        [shape_of((capacity, width))] * count,
        [VMEM] * (count + len(flat)),
        flops=6 * count * capacity * width * hidden,
    )(*rows_in, *flat)


def pair_sum(place, kept, received):
    share = kept.shape[0] // 2

    def body(place_ref, kept_ref, received_ref, outer_ref, inner_ref):
        mine = place_ref[3]
        for out, half in ((outer_ref, 1 - mine), (inner_ref, mine)):
            some = pl.ds(pl.multiple_of(half * share, share), share)
            out[...] = (kept_ref[some, :] + received_ref[some, :].astype(jnp.float32)).astype(out.dtype)

    outs = [shape_of((share, kept.shape[1])), shape_of((share, kept.shape[1]), jnp.float32)]
    return call(body, outs, [SMEM, VMEM, VMEM])(place, kept, received)


def finish(inner, received, gain):
    def body(inner_ref, received_ref, gain_ref, out_ref):
        projected = inner_ref[...] + received_ref[...].astype(jnp.float32)
        out_ref[...] = norm_rows(projected, gain_ref[...]).astype(jnp.bfloat16)

    return call(body, shape_of(inner.shape), [VMEM] * 3)(inner, received, gain.reshape(1, -1))


def attend_project(place, queries, own, passed, out_weight, heads, quarters):
    span, width_heads = queries.shape
    size = width_heads // heads
    pair = 2 * size
    width = out_weight.shape[1]
    share = span // quarters
    blocks = len(passed)
    half = quarters // 2

    def body(place_ref, q_ref, own_ref, *refs):
        first_ref, direct_ref, relay_ref, last_ref = refs[:blocks]
        weight_ref, send_ref, keep_ref, acc, carry, att, proj, middle = refs[blocks:]
        kv_refs = (own_ref, first_ref, middle, last_ref)

        @pl.when(place_ref[0] == 2)
        def _():
            middle[...] = direct_ref[...]

        @pl.when(place_ref[0] == 3)
        def _():
            middle[...] = relay_ref[...]

        row = lax.broadcasted_iota(jnp.int32, (span, span), 0)
        column = lax.broadcasted_iota(jnp.int32, (span, span), 1)
        earlier = column < row
        after = jnp.where(row > column, 1.0, 0.0)
        sums = jnp.concatenate([after, jnp.ones((span, span), jnp.float32)], axis=1)
        sums = jnp.concatenate([sums, sums], axis=0).astype(jnp.bfloat16)
        low = lax.broadcasted_iota(jnp.int32, (span, pair), 1) < size

        def one_block(d):
            for h in range(heads):
                lanes = slice((h // 2) * pair, (h // 2 + 1) * pair)
                query = jnp.where(low if h % 2 == 0 else ~low, q_ref[:, lanes], 0.0).astype(jnp.bfloat16)
                key = kv_refs[d][:span, lanes]
                bias = kv_refs[d][span + h : span + h + 1, :span].astype(jnp.float32)
                z = lax.dot_general(
                    query, key, (((1,), (1,)), ((), ())), preferred_element_type=jnp.float32
                ) * size ** (-0.5) + bias
                rest = -(jnp.maximum(z, 0.0) + jnp.log1p(jnp.exp(-jnp.abs(z))))
                masked = jnp.where(earlier, rest, 0.0) if d == 0 else rest
                top = masked.astype(jnp.bfloat16)
                bottom = (masked - top.astype(jnp.float32)).astype(jnp.bfloat16)
                both = jnp.dot(
                    jnp.concatenate([top, bottom], axis=1), sums, preferred_element_type=jnp.float32
                )
                local = jnp.exp(z + rest + both[:, :span])
                if d == 0:
                    local = jnp.where(earlier, local, 0.0)
                value = kv_refs[d][:span, width_heads + lanes.start : width_heads + lanes.stop]
                part = jnp.dot(local.astype(jnp.bfloat16), value, preferred_element_type=jnp.float32)
                if d == 0:
                    carry[h] = both[:, span:]
                    total = part
                else:
                    before = carry[h]
                    total = jnp.exp(before) * part
                    carry[h] = before + both[:, span:]
                mine = low if h % 2 == 0 else ~low
                if d == 0 and h % 2 == 0:
                    acc[h // 2] = total
                elif d == 0:
                    acc[h // 2] = jnp.where(mine, total, acc[h // 2])
                else:
                    acc[h // 2] = acc[h // 2] + jnp.where(mine, total, 0.0)

        one_block(0)
        for d in range(1, blocks):
            pl.when(place_ref[0] >= d)(lambda d=d: one_block(d))
        for p in range(heads // 2):
            att[:, p * pair : (p + 1) * pair] = acc[p].astype(jnp.bfloat16)
        proj[...] = jnp.dot(att[...], weight_ref[...], preferred_element_type=jnp.float32)
        core = place_ref[1]
        for k in range(half):
            send_ref[k * share : (k + 1) * share, :] = proj[
                pl.ds((2 * k + 1 - core) * share, share), :
            ].astype(jnp.bfloat16)
            keep_ref[k * share : (k + 1) * share, :] = proj[pl.ds((2 * k + core) * share, share), :]

    return call(
        body,
        [shape_of((half * share, width)), shape_of((half * share, width), jnp.float32)],
        [SMEM, VMEM, VMEM] + [VMEM] * len(passed) + [VMEM],
        scratch=(
            pltpu.VMEM((heads // 2, span, pair), jnp.float32),
            pltpu.VMEM((heads, span, span), jnp.float32),
            pltpu.VMEM((span, width_heads), jnp.bfloat16),
            pltpu.VMEM((span, width), jnp.float32),
            pltpu.VMEM(own.shape, jnp.bfloat16),
        ),
        flops=4 * blocks * span * span * width_heads + 2 * span * width_heads * width,
    )(place, queries, own, *passed, out_weight)


def per_device(*arrays):
    return paired_step(*arrays)


def paired_step(
    queries,
    keys,
    values,
    stop_bias,
    out_weight,
    mix_gain,
    moe_input,
    ffn_gain,
    expert_ids,
    expert_scores,
    gate_weight,
    up_weight,
    down_weight,
):
    blocks = lax.axis_size("ep")
    shards = lax.axis_size("tp")
    group = lax.axis_index("grp")
    block = lax.axis_index("ep")
    shard = lax.axis_index("tp")
    place = jnp.stack([block, shard % 2, group, shard // 2]).astype(jnp.int32)
    heads = stop_bias.shape[1]

    def core(array):
        return lax.ppermute(array, "tp", [(i, i ^ 1) for i in range(shards)])

    def across(array):
        return lax.ppermute(array, "tp", [(i, i ^ 2) for i in range(shards)])

    def beside(array):
        return lax.ppermute(array, "grp", [(0, 1), (1, 0)])

    def turn(array, d):
        return lax.ppermute(array, "ep", [(i, (i + d) % blocks) for i in range(blocks)])

    def upward(array, d):
        return lax.ppermute(array, "ep", [(i, i + d) for i in range(blocks - d)])

    rows, top = expert_ids.shape
    capacity = 3 * rows * top // (2 * blocks)
    mine = (gate_weight[0], up_weight[0], down_weight[0])
    own, first_half = pack(place, keys, values, stop_bias.T, mine[0])
    routed = route(place, moe_input, ffn_gain, expert_ids.T, mine, blocks, capacity)
    outbound, halves = routed[:blocks], [first_half, *routed[blocks:]]

    arrived = [outbound[0]] + [turn(outbound[d], d) for d in range(1, blocks)]

    far = tuple(across(array) for array in halves)
    near = tuple(core(array) for array in mine)
    other = tuple(beside(array) for array in far[:5])
    far_near = tuple(core(array) for array in far)
    other_near = tuple(core(array) for array in other)

    passed = [upward(own, 1), lax.ppermute(own, "ep", [(0, 2)])]
    passed += [lax.ppermute(array, "ep", [(2, 3)]) for array in passed]

    def whole(arrays):
        return [[array] for array in arrays]

    def chunked(arrays, last):
        return [arrays[0:2], arrays[2:4], [arrays[4], last]]

    pieces = [
        whole(mine),
        whole(near),
        chunked(far, far[5]),
        chunked(far_near, far_near[5]),
        chunked(other, far[6]),
        chunked(other_near, far_near[6]),
    ]
    order = (2, 0, 1, 3)
    done = expert_rows([arrived[k] for k in order[:1]], pieces)
    done += expert_rows([arrived[k] for k in order[1:]], pieces)
    produced = [done[order.index(k)] for k in range(blocks)]
    returned = [produced[0]] + [turn(produced[d], -d) for d in range(1, blocks)]

    send, kept = attend_project(place, queries, own, passed, out_weight, heads, shards)
    outer, inner = pair_sum(place, kept, core(send))
    mixed = finish(inner, across(outer), mix_gain)
    high, low = combine_plan(place, expert_ids.T, expert_scores.T, blocks, capacity)
    experts_mixed = combine_rows(high, low, returned)
    return (mixed, experts_mixed)


def solution(mesh):
    sizes = mesh.shape
    paired = sizes["grp"] == 2 and sizes["tp"] == 4 and sizes["ep"] == sizes["tp"]
    return jax.shard_map(
        per_device if paired else per_device_wide,
        mesh=mesh,
        in_specs=(
            P(("grp", "ep"), "tp"),
            P(("grp", "ep"), "tp"),
            P(("grp", "ep"), "tp"),
            P(("grp", "ep"), "tp"),
            P("tp", None),
            P(),
            P(("grp", "ep", "tp"), None),
            P(),
            P(("grp", "ep", "tp"), None),
            P(("grp", "ep", "tp"), None),
            P("ep", None, "tp"),
            P("ep", None, "tp"),
            P("ep", "tp", None),
        ),
        out_specs=(P(("grp", "ep", "tp"), None), P(("grp", "ep", "tp"), None)),
        check_vma=False,
    )
```

```python
import jax
import jax.numpy as jnp
from jax import lax
from jax.experimental import pallas as pl
from jax.experimental.pallas import tpu as pltpu
from jax.sharding import PartitionSpec as P


def norm_rows(values, gain):
    values = values.astype(jnp.float32)
    scale = lax.rsqrt(jnp.mean(values * values, axis=-1, keepdims=True) + 1e-06)
    return values * scale * gain


def break_terms(query_heads, query_place, key_block, bias_block, first):
    span = key_block.shape[0]
    heads = query_heads.shape[1]
    key_heads = key_block.reshape(span, heads, -1)
    scores = jnp.einsum("qhd,khd->hqk", query_heads, key_heads, preferred_element_type=jnp.float32)
    scores = scores * query_heads.shape[2] ** (-0.5) + bias_block.astype(jnp.float32).T[:, None, :]
    key_place = first + jnp.arange(span)
    past = (key_place[None, :] < query_place[:, None])[None]
    rest = jnp.where(past, jax.nn.log_sigmoid(-scores), 0.0)
    later = lax.cumsum(rest, axis=2, reverse=True)
    return (scores, past, rest, later)


def block_part(scores, past, rest, later, value_block, heads):
    within = later - rest
    local = jnp.where(past, jnp.exp(jax.nn.log_sigmoid(scores) + within), 0.0).astype(jnp.bfloat16)
    span = value_block.shape[0]
    value_heads = value_block.reshape(span, heads, -1)
    part = jnp.einsum("hqk,khd->qhd", local, value_heads, preferred_element_type=jnp.float32)
    return part.reshape(part.shape[0], -1)


def keep(state):
    return state


def dispatch_plan(normed, expert_ids, experts, capacity):
    rows, top = expert_ids.shape
    flat_ids = expert_ids.reshape(rows * top)
    onehot = (flat_ids[:, None] == jnp.arange(experts)[None, :]).astype(jnp.int32)
    earlier = jnp.cumsum(onehot, axis=0) - onehot
    place = jnp.sum(earlier * onehot, axis=1)
    target = flat_ids * capacity + place
    source = (
        jnp.zeros((experts * capacity,), jnp.int32)
        .at[target]
        .set(jnp.arange(rows * top, dtype=jnp.int32) // top + 1)
    )
    padded = jnp.concatenate([jnp.zeros((1, normed.shape[1]), normed.dtype), normed], axis=0)
    return (padded[source].reshape(experts, capacity, normed.shape[1]), target)


def expert_hidden(piece, gate_weight, up_weight):
    flat = piece.reshape(-1, piece.shape[-1])
    gate = jnp.dot(flat, gate_weight[0], preferred_element_type=jnp.float32)
    upward = jnp.dot(flat, up_weight[0], preferred_element_type=jnp.float32)
    hidden = (jax.nn.silu(gate) * upward).astype(jnp.bfloat16)
    return hidden.reshape(piece.shape[0], piece.shape[1], -1)


def send_back(summed):
    return lax.all_to_all(
        summed.astype(jnp.bfloat16), "ep", split_axis=0, concat_axis=0, tiled=True
    )


def return_rows(hidden_all, down_weight, sources):
    flat = hidden_all.reshape(-1, hidden_all.shape[2])
    product = jnp.dot(flat, down_weight[0], preferred_element_type=jnp.float32)
    return send_back(
        lax.psum_scatter(
            product.reshape(sources * lax.axis_size("tp"), hidden_all.shape[1], -1).astype(
                jnp.bfloat16
            ),
            "tp",
            scatter_dimension=0,
            tiled=True,
        ).astype(jnp.float32)
    )


def per_device_wide(
    queries,
    keys,
    values,
    stop_bias,
    out_weight,
    mix_gain,
    moe_input,
    ffn_gain,
    expert_ids,
    expert_scores,
    gate_weight,
    up_weight,
    down_weight,
):
    span = queries.shape[0]
    heads = stop_bias.shape[1]
    width_heads = queries.shape[1]
    blocks = lax.axis_size("ep")
    own_first = lax.axis_index("ep") * span
    query_heads = queries.reshape(span, heads, -1)
    query_place = own_first + jnp.arange(span)

    def piece_rows(piece, index):
        return tuple((lax.dynamic_slice_in_dim(member, index * span, span, 0) for member in piece))

    start_state = (
        jnp.zeros((blocks, heads, span), jnp.float32),
        jnp.zeros((blocks, span, width_heads), jnp.float32),
    )
    piece = (
        lax.all_gather(keys, "ep", axis=0, tiled=True),
        lax.all_gather(values, "ep", axis=0, tiled=True),
        lax.all_gather(stop_bias, "ep", axis=0, tiled=True),
    )

    def one_block(index, state):
        key_block, value_block, bias_block = piece_rows(piece, index)
        first = index * span

        def compute(inner_state):
            totals, parts = inner_state
            scores, past, rest, later = break_terms(
                query_heads, query_place, key_block, bias_block, first
            )
            part = block_part(scores, past, rest, later, value_block, heads)
            number = first // span
            totals = lax.dynamic_update_index_in_dim(totals, later[:, :, 0], number, 0)
            parts = lax.dynamic_update_index_in_dim(parts, part, number, 0)
            return (totals, parts)

        return lax.cond(first <= own_first, compute, keep, state)

    totals, parts = lax.fori_loop(0, piece[0].shape[0] // span, one_block, start_state)
    carried = lax.cumsum(totals, axis=0, reverse=True) - totals
    factor = jnp.exp(carried).transpose(0, 2, 1)[:, :, :, None]
    attended = jnp.sum(factor * parts.reshape(blocks, span, heads, -1), axis=0).reshape(
        span, width_heads
    )
    attended = attended.astype(jnp.bfloat16)
    projected = lax.psum_scatter(
        jnp.dot(attended, out_weight, preferred_element_type=jnp.float32).astype(jnp.bfloat16),
        "tp",
        scatter_dimension=0,
        tiled=True,
    ).astype(jnp.float32)
    mixed = norm_rows(projected, mix_gain).astype(jnp.bfloat16)
    normed = norm_rows(moe_input, ffn_gain).astype(jnp.bfloat16)
    rows, top = expert_ids.shape
    experts = lax.axis_size("ep")
    capacity = 3 * rows * top // (2 * experts)
    weights = expert_scores / jnp.sum(expert_scores, axis=1, keepdims=True)
    outbound, target = dispatch_plan(normed, expert_ids, experts, capacity)
    arrived = lax.all_to_all(outbound, "ep", split_axis=0, concat_axis=0, tiled=True)
    hidden_all = expert_hidden(
        lax.all_gather(arrived, "tp", axis=0, tiled=True), gate_weight, up_weight
    )
    returned = return_rows(hidden_all, down_weight, arrived.shape[0])
    picked = returned.reshape(experts * capacity, -1)[target].reshape(rows, top, -1)
    experts_mixed = jnp.sum(picked.astype(jnp.float32) * weights[:, :, None], axis=1).astype(
        jnp.bfloat16
    )
    return (mixed, experts_mixed)


VMEM = pl.BlockSpec(memory_space=pltpu.VMEM)
SMEM = pl.BlockSpec(memory_space=pltpu.SMEM)
HBM = pl.BlockSpec(memory_space=pltpu.HBM)


def shape_of(shape, dtype=jnp.bfloat16):
    return jax.ShapeDtypeStruct(shape, dtype)


def call(body, outs, ins, scratch=(), flops=0, limit=24):
    return pl.pallas_call(
        body,
        out_shape=outs,
        in_specs=ins,
        out_specs=jax.tree.map(lambda _: VMEM, outs),
        scratch_shapes=scratch,
        compiler_params=pltpu.CompilerParams(vmem_limit_bytes=limit * 1024 * 1024),
        cost_estimate=pl.CostEstimate(flops=flops, transcendentals=0, bytes_accessed=0),
    )


def selections(place_ref, ids_ref, experts, capacity):
    top, rows = ids_ref.shape
    distance = lax.broadcasted_iota(jnp.int32, (8, rows), 0)
    expert = (place_ref[0] + distance) % experts
    hits = [ids_ref[k : k + 1, :] == expert for k in range(top)]
    chosen = jnp.zeros((8, rows), jnp.float32)
    for hit in hits:
        chosen = chosen + jnp.where(hit & (distance < experts), 1.0, 0.0)
    below = lax.broadcasted_iota(jnp.int32, (rows, rows), 0) < lax.broadcasted_iota(
        jnp.int32, (rows, rows), 1
    )
    rank = jnp.dot(
        chosen.astype(jnp.bfloat16),
        jnp.where(below, 1.0, 0.0).astype(jnp.bfloat16),
        preferred_element_type=jnp.float32,
    )
    slot = lax.broadcasted_iota(jnp.int32, (capacity, rows), 0).astype(jnp.float32)
    picks = []
    for d in range(experts):
        pick = (rank[d : d + 1, :] == slot) & (chosen[d : d + 1, :] > 0.5)
        picks.append(jnp.where(pick, 1.0, 0.0).astype(jnp.bfloat16))
    return hits, picks


def in_hbm(*arrays):
    return [pltpu.with_memory_space_constraint(array, pltpu.HBM) for array in arrays]


def start_all(moves, sems):
    copies = [
        pltpu.make_async_copy(source, target, sems.at[k]) for k, (source, target) in enumerate(moves)
    ]
    for copy in copies:
        copy.start()
    return copies


def pack(place, keys, values, bias, gate):
    span, heads_width = keys.shape
    heads = bias.shape[0]
    part = gate.shape[1] // 2
    deep = gate.shape[0] // 2

    def body(place_ref, bias_hbm, keys_hbm, values_hbm, gate_hbm, own_ref, gate_a, bias_v, sems):
        columns = pl.ds(pl.multiple_of(place_ref[2] * part, part), part)
        copies = start_all(
            [
                (bias_hbm, bias_v),
                (gate_hbm.at[pl.ds(0, deep), columns], gate_a),
                (keys_hbm, own_ref.at[pl.ds(0, span), pl.ds(0, heads_width)]),
                (values_hbm, own_ref.at[pl.ds(0, span), pl.ds(heads_width, heads_width)]),
            ],
            sems,
        )
        own_ref[span:, :] = jnp.zeros((heads, 2 * heads_width), jnp.bfloat16)
        copies[0].wait()
        own_ref[span:, :span] = bias_v[...]
        for copy in copies[1:]:
            copy.wait()

    return call(
        body,
        [shape_of((span + heads, 2 * heads_width)), shape_of((deep, part))],
        [SMEM] + [HBM] * 4,
        scratch=(pltpu.VMEM(bias.shape, jnp.bfloat16), pltpu.SemaphoreType.DMA((4,))),
    )(place, *in_hbm(bias, keys, values, gate))


def route(place, moe_input, ffn_gain, ids, weights, experts, capacity):
    rows, width = moe_input.shape
    gate, upward, down = weights
    part = gate.shape[1] // 2
    deep = gate.shape[0] // 2
    thin = part // 2

    def body(place_ref, gain_hbm, ids_hbm, input_hbm, gate_hbm, up_hbm, down_hbm, *refs):
        outs = refs[:experts]
        gate_b, up_a, up_b, down_a, down_b, down_c, input_v, gain_v, ids_v, sems = refs[experts:]
        begin = pl.multiple_of(place_ref[2] * part, part)
        beyond = pl.multiple_of((1 - place_ref[2]) * part, part)
        columns = pl.ds(begin, part)

        def some(first, size):
            return down_hbm.at[pl.ds(pl.multiple_of(first, thin), size), :]

        copies = start_all(
            [
                (ids_hbm, ids_v),
                (input_hbm, input_v),
                (gain_hbm, gain_v),
                (gate_hbm.at[pl.ds(deep, deep), columns], gate_b),
                (up_hbm.at[pl.ds(0, deep), columns], up_a),
                (up_hbm.at[pl.ds(deep, deep), columns], up_b),
                (some(begin, thin), down_a),
                (some(begin + thin, thin), down_b),
                (some(beyond + thin, thin), down_c),
            ],
            sems,
        )
        copies[0].wait()
        _, picks = selections(place_ref, ids_v, experts, capacity)
        copies[1].wait()
        copies[2].wait()
        normed = norm_rows(input_v[...], gain_v[...]).astype(jnp.bfloat16)
        for d in range(experts):
            outs[d][...] = jnp.dot(
                picks[d], normed, preferred_element_type=jnp.float32
            ).astype(jnp.bfloat16)
        for copy in copies[3:]:
            copy.wait()

    outs = [shape_of((capacity, width))] * experts + [
        shape_of((deep, part)),
        shape_of((deep, part)),
        shape_of((deep, part)),
        shape_of((thin, width)),
        shape_of((thin, width)),
        shape_of((thin, width)),
    ]
    return call(
        body,
        outs,
        [SMEM] + [HBM] * 6,
        scratch=(
            pltpu.VMEM((rows, width), jnp.bfloat16),
            pltpu.VMEM((1, width), jnp.float32),
            pltpu.VMEM(ids.shape, jnp.int32),
            pltpu.SemaphoreType.DMA((9,)),
        ),
        flops=2 * experts * capacity * rows * width,
    )(place, *in_hbm(ffn_gain.reshape(1, width), ids, moe_input, gate, upward, down))


def combine_plan(place, ids, scores, experts, capacity):
    rows = ids.shape[1]

    def body(place_ref, ids_ref, scores_ref, high_ref, low_ref):
        hits, picks = selections(place_ref, ids_ref, experts, capacity)
        shares = scores_ref[...]
        shares = shares / jnp.sum(shares, axis=0, keepdims=True)
        weight = jnp.zeros((8, rows), jnp.float32)
        for k, hit in enumerate(hits):
            weight = weight + jnp.where(hit, shares[k : k + 1, :], 0.0)
        for d in range(experts):
            exact = picks[d].astype(jnp.float32) * weight[d : d + 1, :]
            high = exact.astype(jnp.bfloat16)
            some = slice(d * capacity, (d + 1) * capacity)
            high_ref[some, :] = high
            low_ref[some, :] = (exact - high.astype(jnp.float32)).astype(jnp.bfloat16)

    outs = [shape_of((experts * capacity, rows))] * 2
    return call(body, outs, [SMEM, VMEM, VMEM])(place, ids, scores)


def combine_rows(high, low, returned, chosen, before):
    rows = high.shape[1]
    capacity, width = returned[0].shape

    def body(high_ref, low_ref, *refs):
        outputs = jnp.concatenate([ref[...] for ref in refs[: len(chosen)]], axis=0)
        both = jnp.concatenate([high_ref[...], low_ref[...]], axis=1)
        weights = jnp.concatenate([both[d * capacity : (d + 1) * capacity] for d in chosen], axis=0)
        total = lax.dot_general(
            weights, outputs, (((0,), (0,)), ((), ())), preferred_element_type=jnp.float32
        )
        total = total[:rows] + total[rows:]
        if before is not None:
            total = total + refs[len(chosen)][...]
        refs[-1][...] = total.astype(refs[-1].dtype)

    extra = [] if before is None else [before]
    return call(
        body,
        shape_of((rows, width), jnp.float32 if before is None else jnp.bfloat16),
        [VMEM] * (2 + len(chosen) + len(extra)),
        flops=4 * len(chosen) * capacity * rows * width,
    )(high, low, *(returned[d] for d in chosen), *extra)


def expert_rows(rows_in, pieces):
    capacity, width = rows_in[0].shape
    count = len(rows_in)
    hidden = sum(piece[0][0].shape[1] for piece in pieces)
    flat = [chunk for piece in pieces for kind in piece for chunk in kind]

    def body(*refs):
        weight_refs = refs[count : count + len(flat)]
        outs = refs[count + len(flat) :]
        rows = jnp.concatenate([ref[...] for ref in refs[:count]], axis=0)
        inner, down = [], []
        at = 0
        for piece in pieces:
            kinds = []
            for kind in piece:
                chunk = [ref[...] for ref in weight_refs[at : at + len(kind)]]
                kinds.append(chunk[0] if len(chunk) == 1 else jnp.concatenate(chunk, axis=0))
                at += len(kind)
            size = kinds[0].shape[1]
            both = jnp.concatenate(kinds[:2], axis=1)
            down.append(kinds[2])
            product = jnp.dot(rows, both, preferred_element_type=jnp.float32)
            gate, upward = product[:, :size], product[:, size:]
            inner.append((gate / (1.0 + jnp.exp(-gate)) * upward).astype(jnp.bfloat16))
        inner = jnp.concatenate(inner, axis=1)
        out = jnp.dot(inner, jnp.concatenate(down, axis=0), preferred_element_type=jnp.float32)
        for d in range(count):
            outs[d][...] = out[d * capacity : (d + 1) * capacity].astype(jnp.bfloat16)

    return call(
        body,
        [shape_of((capacity, width))] * count,
        [VMEM] * (count + len(flat)),
        flops=6 * count * capacity * width * hidden,
    )(*rows_in, *flat)


def pair_sum(place, kept, received):
    share = kept.shape[0] // 2

    def body(place_ref, kept_ref, received_ref, outer_ref, inner_ref):
        mine = place_ref[3]
        for out, half in ((outer_ref, 1 - mine), (inner_ref, mine)):
            some = pl.ds(pl.multiple_of(half * share, share), share)
            out[...] = (kept_ref[some, :] + received_ref[some, :].astype(jnp.float32)).astype(out.dtype)

    outs = [shape_of((share, kept.shape[1])), shape_of((share, kept.shape[1]), jnp.float32)]
    return call(body, outs, [SMEM, VMEM, VMEM])(place, kept, received)


def finish(inner, received, gain):
    def body(inner_ref, received_ref, gain_ref, out_ref):
        projected = inner_ref[...] + received_ref[...].astype(jnp.float32)
        out_ref[...] = norm_rows(projected, gain_ref[...]).astype(jnp.bfloat16)

    return call(body, shape_of(inner.shape), [VMEM] * 3)(inner, received, gain.reshape(1, -1))


def attend_project(place, queries, own, passed, out_weight, heads, quarters):
    span, width_heads = queries.shape
    size = width_heads // heads
    pair = 2 * size
    width = out_weight.shape[1]
    share = span // quarters
    blocks = len(passed)
    half = quarters // 2

    def body(place_ref, q_ref, own_ref, *refs):
        first_ref, direct_ref, relay_ref, last_ref = refs[:blocks]
        weight_ref, send_ref, keep_ref, acc, carry, att, proj, middle = refs[blocks:]
        kv_refs = (own_ref, first_ref, middle, last_ref)

        @pl.when(place_ref[0] == 2)
        def _():
            middle[...] = direct_ref[...]

        @pl.when(place_ref[0] == 3)
        def _():
            middle[...] = relay_ref[...]

        row = lax.broadcasted_iota(jnp.int32, (span, span), 0)
        column = lax.broadcasted_iota(jnp.int32, (span, span), 1)
        earlier = column < row
        after = jnp.where(row > column, 1.0, 0.0)
        sums = jnp.concatenate([after, jnp.ones((span, span), jnp.float32)], axis=1)
        sums = jnp.concatenate([sums, sums], axis=0).astype(jnp.bfloat16)
        low = lax.broadcasted_iota(jnp.int32, (span, pair), 1) < size

        def one_block(d):
            for h in range(heads):
                lanes = slice((h // 2) * pair, (h // 2 + 1) * pair)
                query = jnp.where(low if h % 2 == 0 else ~low, q_ref[:, lanes], 0.0).astype(jnp.bfloat16)
                key = kv_refs[d][:span, lanes]
                bias = kv_refs[d][span + h : span + h + 1, :span].astype(jnp.float32)
                z = lax.dot_general(
                    query, key, (((1,), (1,)), ((), ())), preferred_element_type=jnp.float32
                ) * size ** (-0.5) + bias
                rest = -(jnp.maximum(z, 0.0) + jnp.log1p(jnp.exp(-jnp.abs(z))))
                masked = jnp.where(earlier, rest, 0.0) if d == 0 else rest
                top = masked.astype(jnp.bfloat16)
                bottom = (masked - top.astype(jnp.float32)).astype(jnp.bfloat16)
                both = jnp.dot(
                    jnp.concatenate([top, bottom], axis=1), sums, preferred_element_type=jnp.float32
                )
                local = jnp.exp(z + rest + both[:, :span])
                if d == 0:
                    local = jnp.where(earlier, local, 0.0)
                value = kv_refs[d][:span, width_heads + lanes.start : width_heads + lanes.stop]
                part = jnp.dot(local.astype(jnp.bfloat16), value, preferred_element_type=jnp.float32)
                if d == 0:
                    carry[h] = both[:, span:]
                    total = part
                else:
                    before = carry[h]
                    total = jnp.exp(before) * part
                    carry[h] = before + both[:, span:]
                mine = low if h % 2 == 0 else ~low
                if d == 0 and h % 2 == 0:
                    acc[h // 2] = total
                elif d == 0:
                    acc[h // 2] = jnp.where(mine, total, acc[h // 2])
                else:
                    acc[h // 2] = acc[h // 2] + jnp.where(mine, total, 0.0)

        one_block(0)
        for d in range(1, blocks):
            pl.when(place_ref[0] >= d)(lambda d=d: one_block(d))
        for p in range(heads // 2):
            att[:, p * pair : (p + 1) * pair] = acc[p].astype(jnp.bfloat16)
        proj[...] = jnp.dot(att[...], weight_ref[...], preferred_element_type=jnp.float32)
        core = place_ref[1]
        for k in range(half):
            send_ref[k * share : (k + 1) * share, :] = proj[
                pl.ds((2 * k + 1 - core) * share, share), :
            ].astype(jnp.bfloat16)
            keep_ref[k * share : (k + 1) * share, :] = proj[pl.ds((2 * k + core) * share, share), :]

    return call(
        body,
        [shape_of((half * share, width)), shape_of((half * share, width), jnp.float32)],
        [SMEM, VMEM, VMEM] + [VMEM] * len(passed) + [VMEM],
        scratch=(
            pltpu.VMEM((heads // 2, span, pair), jnp.float32),
            pltpu.VMEM((heads, span, span), jnp.float32),
            pltpu.VMEM((span, width_heads), jnp.bfloat16),
            pltpu.VMEM((span, width), jnp.float32),
            pltpu.VMEM(own.shape, jnp.bfloat16),
        ),
        flops=4 * blocks * span * span * width_heads + 2 * span * width_heads * width,
    )(place, queries, own, *passed, out_weight)


def per_device(*arrays):
    return paired_step(*arrays)


def paired_step(
    queries,
    keys,
    values,
    stop_bias,
    out_weight,
    mix_gain,
    moe_input,
    ffn_gain,
    expert_ids,
    expert_scores,
    gate_weight,
    up_weight,
    down_weight,
):
    blocks = lax.axis_size("ep")
    shards = lax.axis_size("tp")
    group = lax.axis_index("grp")
    block = lax.axis_index("ep")
    shard = lax.axis_index("tp")
    place = jnp.stack([block, shard % 2, group, shard // 2]).astype(jnp.int32)
    heads = stop_bias.shape[1]

    def core(array):
        return lax.ppermute(array, "tp", [(i, i ^ 1) for i in range(shards)])

    def across(array):
        return lax.ppermute(array, "tp", [(i, i ^ 2) for i in range(shards)])

    def beside(array):
        return lax.ppermute(array, "grp", [(0, 1), (1, 0)])

    def turn(array, d):
        return lax.ppermute(array, "ep", [(i, (i + d) % blocks) for i in range(blocks)])

    def upward(array, d):
        return lax.ppermute(array, "ep", [(i, i + d) for i in range(blocks - d)])

    rows, top = expert_ids.shape
    capacity = 3 * rows * top // (2 * blocks)
    mine = (gate_weight[0], up_weight[0], down_weight[0])
    own, first_half = pack(place, keys, values, stop_bias.T, mine[0])
    routed = route(place, moe_input, ffn_gain, expert_ids.T, mine, blocks, capacity)
    outbound, halves = routed[:blocks], [first_half, *routed[blocks:]]

    arrived = [outbound[0]] + [turn(outbound[d], d) for d in range(1, blocks)]

    far = tuple(across(array) for array in halves)
    near = tuple(core(array) for array in mine)
    other = tuple(beside(array) for array in far[:5])
    far_near = tuple(core(array) for array in far)
    other_near = tuple(core(array) for array in other)

    passed = [upward(own, 1), lax.ppermute(own, "ep", [(0, 2)])]
    passed += [lax.ppermute(array, "ep", [(2, 3)]) for array in passed]

    def whole(arrays):
        return [[array] for array in arrays]

    def chunked(arrays, last):
        return [arrays[0:2], arrays[2:4], [arrays[4], last]]

    pieces = [
        whole(mine),
        whole(near),
        chunked(far, far[5]),
        chunked(far_near, far_near[5]),
        chunked(other, far[6]),
        chunked(other_near, far_near[6]),
    ]
    order = (2, 0, 1, 3)
    done = expert_rows([arrived[k] for k in order[:1]], pieces)
    done += expert_rows([arrived[k] for k in order[1:]], pieces)
    produced = [done[order.index(k)] for k in range(blocks)]
    returned = [produced[0]] + [turn(produced[d], -d) for d in range(1, blocks)]

    send, kept = attend_project(place, queries, own, passed, out_weight, heads, shards)
    outer, inner = pair_sum(place, kept, core(send))
    mixed = finish(inner, across(outer), mix_gain)
    high, low = combine_plan(place, expert_ids.T, expert_scores.T, blocks, capacity)
    partial = combine_rows(high, low, returned, (0, 2), None)
    experts_mixed = combine_rows(high, low, returned, (1, 3), partial)
    return (mixed, experts_mixed)


def solution(mesh):
    sizes = mesh.shape
    paired = sizes["grp"] == 2 and sizes["tp"] == 4 and sizes["ep"] == sizes["tp"]
    return jax.shard_map(
        per_device if paired else per_device_wide,
        mesh=mesh,
        in_specs=(
            P(("grp", "ep"), "tp"),
            P(("grp", "ep"), "tp"),
            P(("grp", "ep"), "tp"),
            P(("grp", "ep"), "tp"),
            P("tp", None),
            P(),
            P(("grp", "ep", "tp"), None),
            P(),
            P(("grp", "ep", "tp"), None),
            P(("grp", "ep", "tp"), None),
            P("ep", None, "tp"),
            P("ep", None, "tp"),
            P("ep", "tp", None),
        ),
        out_specs=(P(("grp", "ep", "tp"), None), P(("grp", "ep", "tp"), None)),
        check_vma=False,
    )
```
